32 devices in a mesh: sp: 16 (over z, y, x), tp: 2 (over core).
Axes of the slice: x: 2, y: 2, z: 4, core: 2. Of those that a mesh axis runs over, the one named last changes fastest.
Arguments:
- mixer_in: bfloat16 [8192, 1024], P('sp', 'tp'), may hold values from -6 to 6
- residual: bfloat16 [8192, 2048], P(('sp', 'tp')), may hold values from -6 to 6
- decay_real: float32 [64, 64], P('tp'), may hold values from -2 to 0, as said below
- decay_imag: float32 [64, 64], P('tp'), may hold values from 1 to 200
- log_step: float32 [64], P('tp'), may hold values from -3.9 to -2.5
- in_real: float32 [64, 64, 16], P('tp'), may hold values from -1 to 1
- in_imag: float32 [64, 64, 16], P('tp'), may hold values from -1 to 1
- output_real: float32 [64, 16, 64], P('tp'), may hold values from -0.5 to 0.5
- output_imaginary: float32 [64, 16, 64], P('tp'), may hold values from -0.5 to 0.5
- skip: float32 [1024], P('tp'), may hold values from -4 to 4
- out_proj: bfloat16 [1024, 2048], P('tp'), may hold values from -0.1875 to 0.1875
- norm_gain: float32 [2048], replicated, may hold values from 0.1 to 1.9
- w_gate: bfloat16 [2048, 5632], P('sp', 'tp'), may hold values from -0.125 to 0.125
- w_up: bfloat16 [2048, 5632], P('sp', 'tp'), may hold values from -0.125 to 0.125
- w_down: bfloat16 [5632, 2048], P('tp', 'sp'), may hold values from -0.078125 to 0.078125
Outputs:
- output: bfloat16 [8192, 2048], P(('sp', 'tp'))
The draws below stay inside these ranges and needn't reach their ends.
Inputs may be any that keep to these rules, and one draw needn't show every extreme that they name: `decay_real`: every entry is negative.
All inputs are finite; a program needn't handle non-finite values.
Results may differ from the reference program's by a relative error of at most 0.02.
Values may be sent and summed in bfloat16 or wider, within the bound.
A program may use at most 128 MiB of HBM per device.

```python
import jax
import jax.numpy as jnp
from jax import lax

D = 2048
CH = 1024
GROUP = 16
STATE = 64
FF = 5632
TOK_DEV = 512
GROUPS = 64
TOKENS = 8192
CH_DEV = 512
FF_DEV = 2816
N_SP = 16


def draw_decay_real(key, part):
    slow_key, rate_key = jax.random.split(jax.random.fold_in(key, 11))
    slow = jax.random.bernoulli(slow_key, 0.5, (GROUPS, 1))
    mixing = jax.random.uniform(rate_key, (GROUPS, STATE), jnp.float32)
    slow_rate = 5.0 / TOKENS * jnp.exp(mixing * jnp.log(5.0))
    fast_rate = 0.6 * jnp.exp(mixing * jnp.log(2.0))
    return -jnp.where(slow, slow_rate, fast_rate)


def level_of(own_key, extent, shards, low, high):
    level = 1.0
    for position, parts in shards:
        heights = jax.random.uniform(jax.random.fold_in(jax.random.fold_in(own_key, 6), position), (parts,), jnp.float32, low / len(shards), high / len(shards))
        level = level * jnp.repeat(jnp.exp(heights), extent[position] // parts).reshape((-1,) + (1,) * (len(extent) - 1 - position))
    return level


def normal_values(key, shape, scale, bound, cuts=(), dtype=jnp.bfloat16):
    loudness = level_of(key, shape, cuts, -0.22, 0.18) if cuts else 1.0
    entries = jax.random.normal(key, shape, jnp.float32) * scale * loudness
    return jnp.minimum(jnp.maximum(entries, -bound), bound).astype(dtype)


def setup_inputs(seed: int = 0) -> dict:
    key_list = jax.random.split(jax.random.key(seed), 16)
    return {
        "mixer_in": normal_values(key_list[0], (TOKENS, CH), 1.0, 6.0, ((0, 16), (1, 2))),
        "residual": normal_values(key_list[1], (TOKENS, D), 1.0, 6.0, ((0, 32),)),
        "decay_real": draw_decay_real(jax.random.fold_in(key_list[15], 71), 0),
        "decay_imag": jnp.clip(1.0 + 199.0 * jax.random.uniform(key_list[3], (GROUPS, STATE), jnp.float32) ** level_of(key_list[3], (GROUPS, STATE), ((0, 2),), -0.2, 0.2), 1.0, 200.0),
        "log_step": jnp.clip(-3.9 + 1.4000001 * jax.random.uniform(key_list[4], (GROUPS,), jnp.float32) ** level_of(key_list[4], (GROUPS,), ((0, 2),), -0.2, 0.2), -3.9, -2.5),
        "in_real": normal_values(key_list[5], (GROUPS, STATE, GROUP), (2 * GROUP) ** -0.5, 1.0, ((0, 2),), jnp.float32),
        "in_imag": normal_values(key_list[6], (GROUPS, STATE, GROUP), (2 * GROUP) ** -0.5, 1.0, ((0, 2),), jnp.float32),
        "output_real": normal_values(key_list[7], (GROUPS, GROUP, STATE), (2 * STATE) ** -0.5, 0.5, ((0, 2),), jnp.float32),
        "output_imaginary": normal_values(key_list[8], (GROUPS, GROUP, STATE), (2 * STATE) ** -0.5, 0.5, ((0, 2),), jnp.float32),
        "skip": normal_values(key_list[9], (CH,), 1.0, 4.0, ((0, 2),), jnp.float32),
        "out_proj": normal_values(key_list[10], (CH, D), CH ** -0.5, 0.1875, ((0, 2),)),
        "norm_gain": jnp.clip(1.0 + 0.18 * jax.random.normal(key_list[11], (D,), jnp.float32), 0.1, 1.9),
        "w_gate": normal_values(key_list[12], (D, FF), D ** -0.5, 0.125, ((0, 16), (1, 2))),
        "w_up": normal_values(key_list[13], (D, FF), D ** -0.5, 0.125, ((0, 16), (1, 2))),
        "w_down": normal_values(key_list[14], (FF, D), FF ** -0.5, 0.078125, ((0, 2), (1, 16))),
    }


def discrete(decay_real, decay_imag, log_step, in_real, in_imag):
    step_size = jnp.exp(log_step)[:, None]
    magnitude = jnp.exp(decay_real * step_size)
    angle = decay_imag * step_size
    power_re = magnitude * jnp.cos(angle)
    power_im = magnitude * jnp.sin(angle)
    denom = decay_real * decay_real + decay_imag * decay_imag
    ratio_re = ((power_re - 1.0) * decay_real + power_im * decay_imag) / denom
    ratio_im = (power_im * decay_real - (power_re - 1.0) * decay_imag) / denom
    drive_re = ratio_re[..., None] * in_real - ratio_im[..., None] * in_imag
    drive_im = ratio_re[..., None] * in_imag + ratio_im[..., None] * in_real
    return (power_re, power_im, drive_re, drive_im)

def combine(earlier, later):
    ar1, ai1, br1, bi1 = earlier
    ar2, ai2, br2, bi2 = later
    return (ar2 * ar1 - ai2 * ai1, ar2 * ai1 + ai2 * ar1, ar2 * br1 - ai2 * bi1 + br2, ar2 * bi1 + ai2 * br1 + bi2)

def block_sum(left, right, width):
    summed = jnp.zeros((left.shape[0], right.shape[1]), jnp.float32)
    for index in range(left.shape[1] // width):
        partial_value = jnp.dot(left[:, index * width:(index + 1) * width], right[index * width:(index + 1) * width], preferred_element_type=jnp.float32).astype(jnp.bfloat16)
        summed = summed + lax.optimization_barrier(partial_value).astype(jnp.float32)
    return summed.astype(jnp.bfloat16)

def reference(mixer_in, residual, decay_real, decay_imag, log_step, in_real, in_imag, output_real, output_imaginary, skip, out_proj, norm_gain, w_gate, w_up, w_down):
    highest_precision = lax.Precision.HIGHEST
    power_re, power_im, bar_re, bar_im = discrete(decay_real, decay_imag, log_step, in_real, in_imag)
    groups, states = decay_real.shape
    signal = mixer_in.astype(jnp.float32).reshape(N_SP, TOK_DEV, groups, GROUP)
    group_skip_gain = skip.reshape(groups, GROUP)

    def advance(carry, block_range):
        hold_re, hold_im = carry
        drive_re = jnp.einsum('tgc,gpc->tgp', block_range, bar_re, precision=highest_precision)
        drive_im = jnp.einsum('tgc,gpc->tgp', block_range, bar_im, precision=highest_precision)
        a_re = jnp.broadcast_to(power_re[None], drive_re.shape)
        a_im = jnp.broadcast_to(power_im[None], drive_re.shape)
        pw_re, pw_im, state_real, state_imaginary = lax.associative_scan(combine, (a_re, a_im, drive_re, drive_im), axis=0)
        state_real = state_real + pw_re * hold_re[None] - pw_im * hold_im[None]
        state_imaginary = state_imaginary + pw_re * hold_im[None] + pw_im * hold_re[None]
        mixed_before_norm = jnp.einsum('uzl,zhl->uzh', state_real, output_real, precision=highest_precision) - jnp.einsum('uzl,zhl->uzh', state_imaginary, output_imaginary, precision=highest_precision) + group_skip_gain[None] * block_range
        return ((state_real[-1], state_imaginary[-1]), mixed_before_norm.reshape(TOK_DEV, groups * GROUP))
    zero_state = jnp.zeros((groups, states), jnp.float32)
    _, mixed_all = lax.scan(advance, (zero_state, zero_state), signal)
    activated = jax.nn.gelu(mixed_all).astype(jnp.bfloat16)
    res_blocks = residual.reshape(N_SP, TOK_DEV, residual.shape[1])

    def finish(pair):
        act_rows, res_rows = pair
        mixed = block_sum(act_rows, out_proj, CH_DEV)
        carried = res_rows.astype(jnp.float32) + mixed.astype(jnp.float32)
        scale = lax.rsqrt(lax.optimization_barrier(jnp.mean(carried * carried, axis=-1, keepdims=True)) + 1e-06)
        normed = (carried * scale * norm_gain).astype(jnp.bfloat16)
        gate = jnp.dot(normed, w_gate, preferred_element_type=jnp.float32)
        up = jnp.dot(normed, w_up, preferred_element_type=jnp.float32)
        hidden = (jax.nn.silu(gate) * up).astype(jnp.bfloat16)
        down = block_sum(hidden, w_down, FF_DEV)
        return (carried + 0.5 * down.astype(jnp.float32)).astype(jnp.bfloat16)
    result = lax.map(finish, (activated, res_blocks))
    return result.reshape(TOKENS, residual.shape[1])
```

```python
import functools

import jax
import jax.numpy as jnp
from jax import lax
from jax.experimental import pallas as pl
from jax.experimental.pallas import tpu as pltpu
from jax.sharding import Mesh
from jax.sharding import PartitionSpec as P

F32 = jnp.float32
BF16 = jnp.bfloat16
SP = ("h", "u", "m", "v")
PEERS = ("u", "v")
GATHER = 8
CHUNKS = 8
MESH = pl.DeviceIdType.MESH


def discrete(decay_real, decay_imag, log_step, in_real, in_imag):
    step_size = jnp.exp(log_step)[:, None]
    magnitude = jnp.exp(decay_real * step_size)
    angle = decay_imag * step_size
    power_re = magnitude * jnp.cos(angle)
    power_im = magnitude * jnp.sin(angle)
    denom = decay_real * decay_real + decay_imag * decay_imag
    ratio_re = ((power_re - 1.0) * decay_real + power_im * decay_imag) / denom
    ratio_im = (power_im * decay_real - (power_re - 1.0) * decay_imag) / denom
    drive_re = ratio_re[..., None] * in_real - ratio_im[..., None] * in_imag
    drive_im = ratio_re[..., None] * in_imag + ratio_im[..., None] * in_real
    return (power_re, power_im, drive_re, drive_im)


def cmul(ar, ai, br, bi):
    return ar * br - ai * bi, ar * bi + ai * br


def cpow(ar, ai, count):
    result = None
    while count:
        if count & 1:
            result = (ar, ai) if result is None else cmul(*result, ar, ai)
        count >>= 1
        if count:
            ar, ai = cmul(ar, ai, ar, ai)
    return result


def iota(shape, dim):
    return lax.broadcasted_iota(jnp.int32, shape, dim)


def tiled(block, copies, across, down):
    rows, columns = block.shape
    wide = (columns, columns * copies)
    pick = (iota(wide, 0) == lax.rem(iota(wide, 1), columns)).astype(BF16)
    full = jnp.dot(block, pick, preferred_element_type=F32)
    keep = lax.div(iota(full.shape, 0), down) == lax.div(iota(full.shape, 1), across)
    return jnp.where(keep, full, 0.0).astype(BF16)


def layer(sizes, fused, x_ref, b_ref, c_ref, a_ref, k_ref, wo_ref, res_ref, gain_ref, *rest):
    quarters, rest = rest[:3], rest[3:]
    if fused:
        out_ref, *rest = rest
        hidden, partners, peers, *rest = rest
    weights, (rows_ref, carried_ref), rest = rest[:3], rest[3:5], rest[5:]
    (work, read_in, read_out, ends, total, gathered, act, share, others,
     send_sem, recv_sem, local_sem) = rest
    blocks, rows, cb = x_ref.shape
    sb = a_ref.shape[2]
    depth = quarters[0].shape[2]
    width = wo_ref.shape[1]
    span = rows // CHUNKS
    nh, nm, tp = sizes["h"], sizes["m"], sizes["tp"]
    n = nh * 4 * nm
    h, u, m, v, core = (lax.axis_index(name) for name in (*SP, "tp"))
    index = lambda h, u, m, v: ((h * 2 + u) * nm + m) * 2 + v
    me = index(h, u, m, v)
    peer = lambda k: (1 - u if k & 2 else u, 1 - v if k & 1 else v)
    counter = iter(range(send_sem.shape[0]))

    def send(src, dst, device):
        slot = next(counter)
        copy = pltpu.make_async_remote_copy(
            src_ref=src, dst_ref=dst, send_sem=send_sem.at[slot], recv_sem=recv_sem.at[slot],
            device_id=device, device_id_type=MESH,
        )
        copy.start()
        return copy

    def place(ref, position):
        if depth % 128:
            return ref.at[position]
        return ref.at[:, pl.ds(pl.multiple_of(position * depth, depth), depth)]

    barrier = pltpu.get_barrier_semaphore()
    others_sp = []
    for k in range(1, n):
        to = lax.rem(me + k, n)
        there = (lax.div(to, 4 * nm), lax.rem(lax.div(to, 2 * nm), 2),
                 lax.rem(lax.div(to, 2), nm), lax.rem(to, 2), core)
        others_sp.append(there)
        pl.semaphore_signal(barrier, inc=1, device_id=there, device_id_type=MESH)
    for t in range(1, tp):
        pl.semaphore_signal(
            barrier, inc=1, device_id=(h, u, m, v, lax.rem(core + t, tp)), device_id_type=MESH
        )
    pl.semaphore_wait(barrier, n - 1 + tp - 1)

    sent = []
    first = {}
    over_h = {}
    over_m = {}

    def spread_h(w, k, src, position):
        for r in range(1, nh):
            pu, pv = peer(k)
            copy = send(src, place(weights[w], position), (lax.rem(h + r, nh), u, m, v, core))
            over_h[w, k, r] = copy

    def spread_m(w, k, r, src, position):
        for s in range(1, nm):
            over_m[w, k, r, s] = send(
                src, place(weights[w], position), (h, u, lax.rem(m + s, nm), v, core)
            )

    own = u * 2 + v
    for w in range(3):
        for k in (3, 1, 2):
            pu, pv = peer(k)
            first[w, k] = send(
                quarters[w].at[pu * 2 + pv], place(weights[w], me), (h, pu, m, pv, core)
            )
    locals_ = []
    for w in range(3):
        spread_h(w, 0, quarters[w].at[own], me)
        spread_m(w, 0, 0, quarters[w].at[own], me)
        copy = pltpu.make_async_copy(quarters[w].at[own], place(weights[w], me), local_sem.at[w])
        copy.start()
        locals_.append(copy)

    def scan(b, start, keep):
        work[...] = jnp.dot(x_ref[b], read_in[b], preferred_element_type=F32)
        br = jnp.broadcast_to(a_ref[b, 0:1, :], (CHUNKS, sb))
        bi = jnp.broadcast_to(a_ref[b, 1:2, :], (CHUNKS, sb))

        def step(i, state):
            at = pl.ds(pl.multiple_of(i * CHUNKS, CHUNKS), CHUNKS)
            nr, ni = cmul(br, bi, *state)
            nr, ni = nr + work[at, :sb], ni + work[at, sb:]
            if keep:
                work[at, :sb] = nr
                work[at, sb:] = ni
            return nr, ni

        return lax.fori_loop(0, span, step, start, unroll=8)

    @pl.loop(0, blocks)
    def _(b):
        states = b_ref.shape[3]
        for half in range(2):
            read_in[b, :, half * sb:(half + 1) * sb] = tiled(
                b_ref[b, half], GATHER, states, cb // GATHER
            )
            read_out[b, half * sb:(half + 1) * sb, :] = tiled(
                c_ref[b, half], GATHER, cb // GATHER, states
            )
        zero = jnp.zeros((CHUNKS, sb), F32)
        sr, si = scan(b, (zero, zero), False)
        ends[b, :, :sb] = sr
        ends[b, :, sb:] = si
        lr, li = cpow(a_ref[b, 0:1, :], a_ref[b, 1:2, :], span)
        er, ei = sr[0:1], si[0:1]
        for chunk in range(1, CHUNKS):
            er, ei = cmul(lr, li, er, ei)
            er, ei = er + sr[chunk:chunk + 1], ei + si[chunk:chunk + 1]
        total[b, :, :sb] = er
        total[b, :, sb:] = ei

    states_out = [send(total, gathered.at[me], there) for there in others_sp]
    gathered[me] = total[...]
    for copy in states_out:
        copy.wait_recv()

    @pl.loop(0, blocks)
    def _(b):
        lr, li = cpow(a_ref[b, 0:1, :], a_ref[b, 1:2, :], span)
        tr, ti = cpow(lr, li, CHUNKS)
        hr = jnp.zeros((1, sb), F32)
        hi = hr
        for device in range(n - 1):
            nr, ni = cmul(tr, ti, hr, hi)
            nr = nr + gathered[device, b, :, :sb]
            ni = ni + gathered[device, b, :, sb:]
            hr, hi = jnp.where(device < me, nr, hr), jnp.where(device < me, ni, hi)
        starts_r, starts_i = [hr], [hi]
        for chunk in range(CHUNKS - 1):
            nr, ni = cmul(lr, li, hr, hi)
            hr = nr + ends[b, chunk:chunk + 1, :sb]
            hi = ni + ends[b, chunk:chunk + 1, sb:]
            starts_r.append(hr)
            starts_i.append(hi)
        scan(b, (jnp.concatenate(starts_r, axis=0), jnp.concatenate(starts_i, axis=0)), True)
        mixed = jnp.dot(work[...].astype(BF16), read_out[b], preferred_element_type=F32)
        mixed = mixed + k_ref[b] * x_ref[b].astype(F32)
        mixed = jax.nn.gelu(mixed).astype(BF16)
        square = (rows, rows)
        source = lax.rem(iota(square, 0), span) * CHUNKS + lax.div(iota(square, 0), span)
        turn = (iota(square, 1) == source).astype(BF16)
        act[:, pl.ds(pl.multiple_of(b * cb, cb), cb)] = jnp.dot(
            turn, mixed, preferred_element_type=F32
        ).astype(BF16)

    keep_rows = rows // tp
    tile = min(512, width)
    mixed_copies = []
    for t in (*range(1, tp), 0):
        to = lax.rem(core + t, tp)

        @pl.loop(0, width // tile)
        def _(j):
            at = pl.ds(pl.multiple_of(j * tile, tile), tile)
            share[t, :, at] = jnp.dot(
                act[pl.ds(pl.multiple_of(to * keep_rows, keep_rows), keep_rows), :],
                wo_ref[:, at], preferred_element_type=F32,
            ).astype(BF16)

        if t:
            mixed_copies.append(send(share.at[t], others.at[t - 1], (h, u, m, v, to)))

    for w in range(3):
        for k in (1, 2, 3):
            first[w, k].wait_recv()
            pu, pv = peer(k)
            position = index(h, pu, m, pv)
            spread_h(w, k, place(weights[w], position), position)
            spread_m(w, k, 0, place(weights[w], position), position)

    for copy in mixed_copies:
        copy.wait_recv()
    line = min(32, keep_rows)

    @pl.loop(0, keep_rows // line)
    def _(i):
        at = pl.ds(pl.multiple_of(i * line, line), line)
        mixed = share[0, at, :].astype(F32)
        for t in range(1, tp):
            mixed = mixed + others[t - 1, at, :].astype(F32)
        carried = res_ref[at, :].astype(F32) + mixed.astype(BF16).astype(F32)
        scale = lax.rsqrt(jnp.mean(carried * carried, axis=-1, keepdims=True) + 1e-06)
        carried_ref[at, :] = carried
        rows_ref[0, 0, at, :] = (carried * scale * gain_ref[...]).astype(BF16)

    row_copies = {}
    for k in (3, 1, 2):
        pu, pv = peer(k)
        row_copies[k] = send(rows_ref.at[0, 0], rows_ref.at[0, k], (h, pu, m, pv, core))
    last = []
    for t in range(1, tp):
        last.append(send(rows_ref.at[0, 0], rows_ref.at[t, 0], (h, u, m, v, lax.rem(core + t, tp))))

    def pass_m(w, k):
        pu, pv = peer(k)
        for r in range(1, nh):
            over_h[w, k, r].wait_recv()
            position = index(lax.rem(h - r + nh, nh), pu, m, pv)
            spread_m(w, k, r, place(weights[w], position), position)

    for w in range(3):
        for k in range(4):
            pass_m(w, k)
        if w == 1:
            for k in (1, 2, 3):
                row_copies[k].wait_recv()
                for t in range(1, tp):
                    last.append(send(
                        rows_ref.at[0, k], rows_ref.at[t, k], (h, u, m, v, lax.rem(core + t, tp))
                    ))
    sent = [*first.values(), *over_h.values(), *over_m.values(), *states_out, *mixed_copies]
    row_sends = [*row_copies.values(), *last]
    for (w, *_), copy in over_m.items():
        if w < 2 or not fused:
            copy.wait_recv()
    for copy in last:
        copy.wait_recv()
    for copy in locals_:
        copy.wait()
    if fused:
        sent += back(
            sizes, send, peer, (h, u, m, v, core), weights, rows_ref, carried_ref, out_ref,
            hidden, partners, peers, row_sends, [c for (w, *_), c in over_m.items() if w == 2],
        )
    else:
        sent += row_sends
    for copy in sent:
        copy.wait_send()


def back(sizes, send, peer, here, weights, rows_ref, carried_ref, out_ref, hidden, partners,
         peers, row_sends, down_copies):
    tp = sizes["tp"]
    h, u, m, v, core = here
    _, _, keep_rows, width = rows_ref.shape
    across = (((1,), (1,)), ((), ()))

    @pl.loop(0, 4 * tp)
    def _(i):
        t, k = lax.div(i, 4), lax.rem(i, 4)
        block = rows_ref[t, k]
        gate = lax.dot_general(block, weights[0][...], across, preferred_element_type=F32)
        up = lax.dot_general(block, weights[1][...], across, preferred_element_type=F32)
        hidden[i] = (jax.nn.silu(gate) * up).astype(BF16)

    for copy in (*down_copies,):
        copy.wait_recv()
    for copy in row_sends:
        copy.wait_send()

    tile = min(512, width)
    line = min(32, keep_rows)
    sent = []
    peer_copies = []
    from_core = {}

    def reduce(k):
        for copy in from_core[k]:
            copy.wait_recv()

        @pl.loop(0, keep_rows // line)
        def _(i):
            at = pl.ds(pl.multiple_of(i * line, line), line)
            total = rows_ref[0, k, at, :].astype(F32)
            for t in range(1, tp):
                total = total + partners[k, t - 1, at, :].astype(F32)
            rows_ref[0, k, at, :] = total.astype(BF16)

        if k:
            pu, pv = peer(k)
            peer_copies.append(send(rows_ref.at[0, k], peers.at[k - 1], (h, pu, m, pv, core)))

    order = (3, 1, 2, 0)
    for step, k in enumerate(order):
        from_core[k] = []
        for t in (*range(1, tp), 0):
            @pl.loop(0, width // tile)
            def _(j):
                at = pl.ds(pl.multiple_of(j * tile, tile), tile)
                rows_ref[t, k, :, at] = jnp.dot(
                    hidden[t * 4 + k], weights[2][:, at], preferred_element_type=F32
                ).astype(BF16)

            if t:
                from_core[k].append(send(
                    rows_ref.at[t, k], partners.at[k, t - 1],
                    (h, u, m, v, lax.rem(core + tp - t, tp)),
                ))
        reduce(k)
        sent += from_core[k]
    for copy in peer_copies:
        copy.wait_recv()

    @pl.loop(0, keep_rows // line)
    def _(i):
        at = pl.ds(pl.multiple_of(i * line, line), line)
        total = rows_ref[0, 0, at, :].astype(F32)
        for k in range(1, 4):
            total = total + peers[k - 1, at, :].astype(F32)
        total = total.astype(BF16).astype(F32)
        out_ref[at, :] = (carried_ref[at, :] + 0.5 * total).astype(BF16)

    return sent + peer_copies


def streamed(sizes, scopes, x_ref, b_ref, c_ref, a_ref, k_ref, wo_ref, res_ref, gain_ref, gate_ref,
             up_ref, down_ref, out_ref, *rest):
    quarters, weights, rest = (gate_ref, up_ref, down_ref), rest[:3], rest[3:]
    (extra, rows_ref, carried_ref, gates, hidden, partners, firsts, seconds, work, read_in,
     read_out, ends, total, gathered, act, share, others, send_sem, recv_sem, local_sem) = rest
    blocks, rows, cb = x_ref.shape
    sb = a_ref.shape[2]
    depth = gate_ref.shape[2]
    width = wo_ref.shape[1]
    keep_rows = rows // 2
    span = rows // CHUNKS
    nh, nm = sizes["h"], sizes["m"]
    n = nh * 4 * nm
    h, u, m, v, core = (lax.axis_index(name) for name in (*SP, "tp"))
    oh, ou, om, ov = 1 - h, 1 - u, 1 - m, 1 - v
    index = lambda h, u, m, v: ((h * 2 + u) * nm + m) * 2 + v
    me = index(h, u, m, v)
    inner = u != h
    to_x, to_z, to_y = (h, u, m, ov, core), (h, ou, m, v, core), (h, u, om, v, core)
    to_c, to_b, to_t = (oh, u, m, v, core), (oh, ou, m, v, core), (h, u, m, v, 1 - core)
    plane = [(a, b, c) for a in (h, oh) for b in (u, ou) for c in (v, ov)]
    across = (((1,), (1,)), ((), ()))
    slots, everywhere, inside, moves = {}, [], [], []
    counter = iter(range(send_sem.shape[0]))

    def slot(name):
        return slots.setdefault(name, len(slots))

    def describe(src, dst, device, name, number):
        return pltpu.make_async_remote_copy(
            src_ref=src, dst_ref=dst, send_sem=send_sem.at[number],
            recv_sem=recv_sem.at[slot(name)], device_id=device, device_id_type=MESH,
        )

    def send(src, dst, device, name, kept=everywhere):
        number = next(counter)
        copy = describe(src, dst, device, name, number)
        copy.start()
        kept.append((name, number) if kept is inside else copy)

    def arrive(dst, device, name):
        describe(dst, dst, device, name, 0).wait_recv()

    def place(w, position):
        return weights[w].at[:, pl.ds(pl.multiple_of(position * depth, depth), depth)]

    def spot(w, j, row=m):
        a, b, c = plane[j]
        return place(w, index(a, b, row, c))

    def mine(w, b, c):
        return quarters[w].at[b * 2 + c]

    def own(w):
        return mine(w, u, v)

    def send_x(w, s):
        if s:
            send(mine(w, ou, ov), extra.at[w], to_x, ("xo", w))
        else:
            send(mine(w, u, ov), spot(w, 0), to_x, ("xu", w))

    def send_z(w, s):
        send(extra.at[w] if s else mine(w, ou, v), spot(w, s), to_z, ("z", w, s))

    def send_c(w, s):
        send(spot(w, 1) if s else own(w), spot(w, s), to_c, ("cs", w, s))

    def send_b(w, s):
        send(extra.at[w] if s else mine(w, ou, v), spot(w, s), to_b, ("co", w, s), inside)

    def relay(w, s):
        send(spot(w, 2 + s), spot(w, 2 + s), to_c, ("co", w, s), inside)

    def send_y(w, j):
        send(own(w) if j == 0 else spot(w, j), spot(w, j), to_y, ("y", w, j))

    def wait_x(w, s):
        if s:
            arrive(extra.at[w], to_x, ("xo", w))
        else:
            arrive(spot(w, 1), to_x, ("xu", w))

    def wait_z(w, s):
        arrive(spot(w, 2 + s), to_z, ("z", w, s))

    def wait_cs(w, s):
        arrive(spot(w, 4 + s), to_c, ("cs", w, s))

    def wait_co(w, s):
        arrive(spot(w, 6 + s), to_c, ("co", w, s))

    def wait_y(w, j):
        arrive(spot(w, j, om), to_y, ("y", w, j))

    barrier = pltpu.get_barrier_semaphore()
    others_sp = []
    for k in range(1, n):
        to = lax.rem(me + k, n)
        there = (lax.div(to, 4 * nm), lax.rem(lax.div(to, 2 * nm), 2),
                 lax.rem(lax.div(to, 2), nm), lax.rem(to, 2), core)
        others_sp.append(there)
        pl.semaphore_signal(barrier, inc=1, device_id=there, device_id_type=MESH)
    pl.semaphore_signal(barrier, inc=1, device_id=to_t, device_id_type=MESH)
    with jax.named_scope("A_barrier"):
        pl.semaphore_wait(barrier, n)

    send_x(0, 0)
    send_z(0, 0)
    send_y(0, 0)

    @pl.when(inner)
    def _():
        send_b(0, 0)

    local = []
    for w in range(3):
        copy = pltpu.make_async_copy(own(w), spot(w, 0), local_sem.at[w])
        copy.start()
        local.append(copy)

    def scan(b, start, keep):
        work[...] = jnp.dot(x_ref[b], read_in[b], preferred_element_type=F32)
        br = jnp.broadcast_to(a_ref[b, 0:1, :], (CHUNKS, sb))
        bi = jnp.broadcast_to(a_ref[b, 1:2, :], (CHUNKS, sb))

        def step(i, state):
            at = pl.ds(pl.multiple_of(i * CHUNKS, CHUNKS), CHUNKS)
            nr, ni = cmul(br, bi, *state)
            nr, ni = nr + work[at, :sb], ni + work[at, sb:]
            if keep:
                work[at, :sb] = nr
                work[at, sb:] = ni
            return nr, ni

        return lax.fori_loop(0, span, step, start, unroll=8)

    with jax.named_scope("B_scan1"):
        @pl.loop(0, blocks)
        def _(b):
            states = b_ref.shape[3]
            for half in range(2):
                read_in[b, :, half * sb:(half + 1) * sb] = tiled(
                    b_ref[b, half], GATHER, states, cb // GATHER
                )
                read_out[b, half * sb:(half + 1) * sb, :] = tiled(
                    c_ref[b, half], GATHER, cb // GATHER, states
                )
            zero = jnp.zeros((CHUNKS, sb), F32)
            sr, si = scan(b, (zero, zero), False)
            ends[b, :, :sb] = sr
            ends[b, :, sb:] = si
            lr, li = cpow(a_ref[b, 0:1, :], a_ref[b, 1:2, :], span)
            er, ei = sr[0:1], si[0:1]
            for chunk in range(1, CHUNKS):
                er, ei = cmul(lr, li, er, ei)
                er, ei = er + sr[chunk:chunk + 1], ei + si[chunk:chunk + 1]
            total[b, :, :sb] = er
            total[b, :, sb:] = ei

    for k, there in enumerate(others_sp):
        send(total, gathered.at[me], there, ("s", k))
    gathered[me] = total[...]

    send_x(0, 1)
    send_c(0, 0)
    for w in (1, 2):
        for s in range(2):
            send_x(w, s)
    with jax.named_scope("C_x0"):
        wait_x(0, 0)
    send_c(0, 1)
    send_y(0, 1)
    with jax.named_scope("C_states"):
        for k in range(n - 1):
            arrive(gathered.at[lax.rem(me + n - 1 - k, n)], others_sp[k], ("s", k))

    square = (rows, rows)
    source = lax.rem(iota(square, 0), span) * CHUNKS + lax.div(iota(square, 0), span)

    with jax.named_scope("D_scan2"):
        @pl.loop(0, blocks)
        def _(b):
            lr, li = cpow(a_ref[b, 0:1, :], a_ref[b, 1:2, :], span)
            tr, ti = cpow(lr, li, CHUNKS)
            hr = jnp.zeros((1, sb), F32)
            hi = hr
            for device in range(n - 1):
                nr, ni = cmul(tr, ti, hr, hi)
                nr = nr + gathered[device, b, :, :sb]
                ni = ni + gathered[device, b, :, sb:]
                hr, hi = jnp.where(device < me, nr, hr), jnp.where(device < me, ni, hi)
            starts_r, starts_i = [hr], [hi]
            for chunk in range(CHUNKS - 1):
                nr, ni = cmul(lr, li, hr, hi)
                hr = nr + ends[b, chunk:chunk + 1, :sb]
                hi = ni + ends[b, chunk:chunk + 1, sb:]
                starts_r.append(hr)
                starts_i.append(hi)
            scan(b, (jnp.concatenate(starts_r, axis=0), jnp.concatenate(starts_i, axis=0)), True)
            mixed = jnp.dot(work[...].astype(BF16), read_out[b], preferred_element_type=F32)
            mixed = mixed + k_ref[b] * x_ref[b].astype(F32)
            mixed = jax.nn.gelu(mixed).astype(BF16)
            turn = (iota(square, 1) == source).astype(BF16)
            act[:, pl.ds(pl.multiple_of(b * cb, cb), cb)] = jnp.dot(
                turn, mixed, preferred_element_type=F32
            ).astype(BF16)

    with jax.named_scope("D_x1"):
        wait_x(0, 1)
    send_z(0, 1)

    @pl.when(inner)
    def _():
        send_b(0, 1)

    tile = min(512, width)
    with jax.named_scope("E_outproj"):
        for t in (1, 0):
            to = core if t == 0 else 1 - core

            @pl.loop(0, width // tile)
            def _(j):
                at = pl.ds(pl.multiple_of(j * tile, tile), tile)
                share[t, :, at] = jnp.dot(
                    act[pl.ds(pl.multiple_of(to * keep_rows, keep_rows), keep_rows), :],
                    wo_ref[:, at], preferred_element_type=F32,
                ).astype(BF16)

            if t:
                send(share.at[1], others, to_t, ("mix",))

    with jax.named_scope("G_mix"):
        arrive(others, to_t, ("mix",))
    line = min(32, keep_rows)
    with jax.named_scope("H_norm"):
        @pl.loop(0, keep_rows // line)
        def _(i):
            at = pl.ds(pl.multiple_of(i * line, line), line)
            mixed = share[0, at, :].astype(F32) + others[at, :].astype(F32)
            carried = res_ref[at, :].astype(F32) + mixed.astype(BF16).astype(F32)
            scale = lax.rsqrt(jnp.mean(carried * carried, axis=-1, keepdims=True) + 1e-06)
            carried_ref[at, :] = carried
            rows_ref[0, 0, at, :] = (carried * scale * gain_ref[...]).astype(BF16)

    send(rows_ref.at[0, 0], rows_ref.at[0, 1], to_x, ("r", 1), moves)
    send(rows_ref.at[0, 0], rows_ref.at[0, 2], to_z, ("r", 2), moves)
    send(rows_ref.at[0, 0], rows_ref.at[1, 0], to_t, ("t", 0), moves)

    def share_core(k):
        send(rows_ref.at[0, k], rows_ref.at[1, k], to_t, ("t", k), moves)

    def wait_core(k):
        arrive(rows_ref.at[1, k], to_t, ("t", k))

    def own_blocks(w):
        send_z(w, 0)
        send_c(w, 0)
        send_y(w, 0)

        @pl.when(inner)
        def _():
            send_b(w, 0)

        wait_x(w, 0)
        send_c(w, 1)
        send_y(w, 1)
        wait_x(w, 1)
        send_z(w, 1)

        @pl.when(inner)
        def _():
            send_b(w, 1)

    def pass_z(w):
        for s in range(2):
            with jax.named_scope(f"z{w}{s}"):
                wait_z(w, s)

            @pl.when(inner)
            def _():
                relay(w, s)

            send_y(w, 2 + s)

    def pass_c(w):
        for s in range(2):
            with jax.named_scope(f"cs{w}{s}"):
                wait_cs(w, s)
            send_y(w, 4 + s)

    def pass_o(w):
        for s in range(2):
            with jax.named_scope(f"co{w}{s}"):
                wait_co(w, s)
            send_y(w, 6 + s)

    def gate_part(t, k):
        with jax.named_scope(f"gate{t}{k}"):
            gates[4 * t + k] = lax.dot_general(
                rows_ref[t, k], weights[0][...], across, preferred_element_type=F32
            )

    def up_part(t, k):
        with jax.named_scope(f"up{t}{k}"):
            up = lax.dot_general(
                rows_ref[t, k], weights[1][...], across, preferred_element_type=F32
            )
            hidden[pl.ds((4 * t + k) * keep_rows, keep_rows), :] = (
                jax.nn.silu(gates[4 * t + k]) * up
            ).astype(BF16)

    half = keep_rows // 2
    with jax.named_scope("own1"):
        own_blocks(1)
    pass_z(0)
    pass_c(0)
    pass_o(0)
    with jax.named_scope("r1"):
        arrive(rows_ref.at[0, 1], to_x, ("r", 1))
    send(rows_ref.at[0, 1, pl.ds(0, half)], rows_ref.at[0, 3, pl.ds(0, half)], to_z,
         ("r", 3, 0), moves)
    share_core(1)
    with jax.named_scope("r2"):
        arrive(rows_ref.at[0, 2], to_z, ("r", 2))
    send(rows_ref.at[0, 2, pl.ds(half, half)], rows_ref.at[0, 3, pl.ds(half, half)], to_x,
         ("r", 3, 1), moves)
    share_core(2)
    for copy in local:
        copy.wait()
    with jax.named_scope("y0"):
        for j in range(8):
            wait_y(0, j)
    wait_core(0)
    gate_part(0, 0)
    gate_part(1, 0)
    pass_z(1)
    with jax.named_scope("own2"):
        own_blocks(2)
    gate_part(0, 1)
    wait_core(1)
    gate_part(1, 1)
    pass_c(1)
    gate_part(0, 2)
    wait_core(2)
    gate_part(1, 2)
    pass_o(1)
    with jax.named_scope("r3"):
        arrive(rows_ref.at[0, 3, pl.ds(0, half)], to_z, ("r", 3, 0))
        arrive(rows_ref.at[0, 3, pl.ds(half, half)], to_x, ("r", 3, 1))
    share_core(3)
    gate_part(0, 3)
    pass_z(2)
    with jax.named_scope("t3"):
        wait_core(3)
    gate_part(1, 3)
    with jax.named_scope("y1"):
        for j in range(8):
            wait_y(1, j)
    for t, k in ((0, 0), (1, 0), (0, 1)):
        up_part(t, k)
    pass_c(2)
    for t, k in ((1, 1), (0, 2), (1, 2)):
        up_part(t, k)
    pass_o(2)
    for t, k in ((0, 3), (1, 3)):
        up_part(t, k)
    with jax.named_scope("moves"):
        for copy in moves:
            copy.wait_send()

    across_u = width // 8
    chunks = [(a, b, c) for a in (h, oh) for c in (m, om) for b in range(2)]

    def columns(j):
        a, b, c = chunks[j]
        return pl.ds(pl.multiple_of(index(a, b, c, 0) * depth, across_u), across_u)

    def down(j):
        at = columns(j)
        for t in (1, 0):
            result = jnp.dot(
                hidden[4 * t * keep_rows:4 * (t + 1) * keep_rows, :], weights[2][:, at],
                preferred_element_type=F32,
            ).astype(BF16)
            for k in range(4):
                rows_ref[t, k, :, at] = result[k * keep_rows:(k + 1) * keep_rows]
            if t:
                send(rows_ref.at[1, :, :, at], partners.at[j], to_t, ("p", j))

    def add(target, j, other):
        at = columns(j)

        @pl.loop(0, keep_rows // line)
        def _(i):
            lines = pl.ds(pl.multiple_of(i * line, line), line)
            rows_ref[0, target, lines, at] = (
                rows_ref[0, target, lines, at].astype(F32) + other[lines, :].astype(F32)
            ).astype(BF16)

    def pair(j):
        at = columns(j)
        near, far = (1, 2) if j % 2 == 0 else (2, 1)
        device = to_x if j % 2 == 0 else to_z
        arrive(partners.at[j], to_t, ("p", j))
        for place_in, k in enumerate((3, near)):
            add(k, j, partners.at[j, k])
            send(rows_ref.at[0, k, :, at], firsts.at[j, place_in], device, ("f", j, place_in))
        add(far, j, partners.at[j, far])
        add(0, j, partners.at[j, 0])

    def combine(j):
        at = columns(j)
        far = 2 if j % 2 == 0 else 1
        device, other = (to_x, to_z) if j % 2 == 0 else (to_z, to_x)
        arrive(firsts.at[j, 0], device, ("f", j, 0))
        add(far, j, firsts.at[j, 0])
        send(rows_ref.at[0, far, :, at], seconds.at[j], other, ("g", j))
        arrive(firsts.at[j, 1], device, ("f", j, 1))
        add(0, j, firsts.at[j, 1])

    def finish(j):
        at = columns(j)
        arrive(seconds.at[j], to_z if j % 2 == 0 else to_x, ("g", j))

        @pl.loop(0, keep_rows // line)
        def _(i):
            lines = pl.ds(pl.multiple_of(i * line, line), line)
            summed = rows_ref[0, 0, lines, at].astype(F32) + seconds[j, lines, :].astype(F32)
            summed = summed.astype(BF16).astype(F32)
            out_ref[lines, at] = (carried_ref[lines, at] + 0.5 * summed).astype(BF16)

    lag = (1, 3, 5)
    for step in range(8 + lag[2]):
        if step < 8:
            if step == 2:
                with jax.named_scope("y2a"):
                    for j in range(4):
                        wait_y(2, j)
            if step == 6:
                with jax.named_scope("y2b"):
                    for j in range(4, 8):
                        wait_y(2, j)
            with jax.named_scope(f"down{step}"):
                down(step)
        if 0 <= step - lag[0] < 8:
            with jax.named_scope(f"pair{step - lag[0]}"):
                pair(step - lag[0])
        if 0 <= step - lag[1] < 8:
            with jax.named_scope(f"comb{step - lag[1]}"):
                combine(step - lag[1])
        if 0 <= step - lag[2] < 8:
            with jax.named_scope(f"fin{step - lag[2]}"):
                finish(step - lag[2])
    for copy in everywhere:
        copy.wait_send()

    @pl.when(inner)
    def _():
        for name, number in inside:
            describe(extra.at[0], extra.at[0], to_c, name, number).wait_send()


def shift(value, axis, count, by):
    return lax.ppermute(value, axis, [(i, (i + by) % count) for i in range(count)])


def flip(value, axes, count, k):
    return lax.ppermute(value, axes, [(i, i ^ k) for i in range(count)])


def on_device(sizes, mixer_in, residual, decay_real, decay_imag, log_step, in_real, in_imag,
              output_real, output_imaginary, skip, out_proj, norm_gain, w_gate, w_up, w_down):
    tp, nh, nm = sizes["tp"], sizes["h"], sizes["m"]
    n = nh * 4 * nm
    rows, channels = mixer_in.shape
    keep_rows, width = residual.shape
    depth, hidden_units = w_gate.shape
    part = hidden_units // 4
    groups, states = decay_real.shape
    blocks = groups // GATHER
    cb, sb = channels // blocks, GATHER * states
    power_re, power_im, bar_re, bar_im = discrete(
        decay_real, decay_imag, log_step, in_real, in_imag
    )
    rows_first = lambda t: jnp.transpose(t, (0, 2, 1)).reshape(blocks, -1, t.shape[1])
    read_in = jnp.stack([rows_first(bar_re), rows_first(bar_im)], axis=1).astype(BF16)
    read_out = jnp.stack(
        [rows_first(output_real), -rows_first(output_imaginary)], axis=1
    ).astype(BF16)
    power = jnp.stack([power_re.reshape(blocks, sb), power_im.reshape(blocks, sb)], axis=1)
    x = mixer_in.reshape(CHUNKS, rows // CHUNKS, blocks, cb).transpose(2, 1, 0, 3)
    x = x.reshape(blocks, rows, cb)
    vmem = pl.BlockSpec(memory_space=pltpu.VMEM)
    operands = (x, read_in, read_out, power, skip.reshape(blocks, 1, cb), out_proj, residual,
                norm_gain.reshape(1, width), w_gate.T.reshape(4, part, depth),
                w_up.T.reshape(4, part, depth), w_down.reshape(4, part, depth))
    if depth % 128 == 0 and (tp, nh, nm) == (2, 2, 2):
        cut = width // 8
        return pl.pallas_call(
            functools.partial(streamed, sizes, None),
            in_specs=[vmem] * 11,
            out_specs=vmem,
            out_shape=jax.ShapeDtypeStruct((keep_rows, width), BF16),
            scratch_shapes=[
                *[pltpu.VMEM((part, n * depth), BF16)] * 3,
                pltpu.VMEM((3, part, depth), BF16),
                pltpu.VMEM((2, 4, keep_rows, width), BF16),
                pltpu.VMEM((keep_rows, width), F32),
                pltpu.VMEM((8, keep_rows, part), F32),
                pltpu.VMEM((8 * keep_rows, part), BF16),
                pltpu.VMEM((8, 4, keep_rows, cut), BF16),
                pltpu.VMEM((8, 2, keep_rows, cut), BF16),
                pltpu.VMEM((8, keep_rows, cut), BF16),
                pltpu.VMEM((rows, 2 * sb), F32),
                pltpu.VMEM((blocks, cb, 2 * sb), BF16),
                pltpu.VMEM((blocks, 2 * sb, cb), BF16),
                pltpu.VMEM((blocks, CHUNKS, 2 * sb), F32),
                pltpu.VMEM((blocks, 1, 2 * sb), F32),
                pltpu.VMEM((n, blocks, 1, 2 * sb), F32),
                pltpu.VMEM((rows, channels), BF16),
                pltpu.VMEM((2, keep_rows, width), BF16),
                pltpu.VMEM((keep_rows, width), BF16),
                pltpu.SemaphoreType.DMA((160,)),
                pltpu.SemaphoreType.DMA((160,)),
                pltpu.SemaphoreType.DMA((3,)),
            ],
            compiler_params=pltpu.CompilerParams(
                collective_id=0, has_side_effects=True, vmem_limit_bytes=62 * 2**20
            ),
            name="streamed",
        )(*operands)
    copies = 3 * (3 + 4 * (nh - 1) + 4 * nh * (nm - 1)) + (n - 1) + (tp - 1) + 3 + 4 * (tp - 1)
    laid = (part, n * depth) if depth % 128 == 0 else (n, part, depth)
    between = [(laid, BF16)] * 3 + [
        ((tp, 4, keep_rows, width), BF16), ((keep_rows, width), F32),
    ]
    fused = depth % 128 == 0
    if fused:
        copies += 4 * (tp - 1) + 3
        out_shape = [jax.ShapeDtypeStruct((keep_rows, width), BF16)]
        extra = [
            pltpu.VMEM((4 * tp, keep_rows, part), BF16),
            pltpu.VMEM((4, tp - 1, keep_rows, width), BF16),
            pltpu.VMEM((3, keep_rows, width), BF16),
            *(pltpu.VMEM(*item) for item in between),
        ]
    else:
        out_shape = [jax.ShapeDtypeStruct(*item) for item in between]
        extra = []
    results = pl.pallas_call(
        functools.partial(layer, sizes, fused),
        in_specs=[vmem] * 11,
        out_specs=[vmem] * len(out_shape),
        out_shape=out_shape,
        scratch_shapes=[
            *extra,
            pltpu.VMEM((rows, 2 * sb), F32),
            pltpu.VMEM((blocks, cb, 2 * sb), BF16),
            pltpu.VMEM((blocks, 2 * sb, cb), BF16),
            pltpu.VMEM((blocks, CHUNKS, 2 * sb), F32),
            pltpu.VMEM((blocks, 1, 2 * sb), F32),
            pltpu.VMEM((n, blocks, 1, 2 * sb), F32),
            pltpu.VMEM((rows, channels), BF16),
            pltpu.VMEM((tp, keep_rows, width), BF16),
            pltpu.VMEM((tp - 1, keep_rows, width), BF16),
            pltpu.SemaphoreType.DMA((copies,)),
            pltpu.SemaphoreType.DMA((copies,)),
            pltpu.SemaphoreType.DMA((3,)),
        ],
        compiler_params=pltpu.CompilerParams(
            collective_id=0, has_side_effects=True, vmem_limit_bytes=62 * 2**20
        ),
        name="layer",
    )(*operands)
    if fused:
        return results[0]
    full_gate, full_up, full_down, rows_all, carried = results
    if len(laid) == 3:
        full_gate, full_up, full_down = (
            t.transpose(1, 0, 2).reshape(part, width) for t in (full_gate, full_up, full_down)
        )

    flat = rows_all.reshape(-1, width)
    across = (((1,), (1,)), ((), ()))
    gate = lax.dot_general(flat, full_gate, across, preferred_element_type=F32)
    up = lax.dot_general(flat, full_up, across, preferred_element_type=F32)
    hidden = (jax.nn.silu(gate) * up).astype(BF16)
    down = jnp.dot(hidden, full_down, preferred_element_type=F32).astype(BF16)
    down = down.reshape(rows_all.shape)
    summed = down[0].astype(F32)
    for t in range(1, tp):
        summed = summed + shift(down[t], "tp", tp, -t).astype(F32)
    summed = summed.astype(BF16)
    total = summed[0].astype(F32)
    for k in range(1, 4):
        total = total + flip(summed[k], PEERS, 4, k).astype(F32)
    total = total.astype(BF16)
    return (carried + 0.5 * total.astype(F32)).astype(BF16)


def solution(mesh):
    sp, tp = mesh.shape["sp"], mesh.shape["tp"]
    sizes = {"h": sp // 8, "u": 2, "m": 2, "v": 2, "tp": tp}
    cut = Mesh(mesh.devices.reshape(tuple(sizes.values())), tuple(sizes))
    return jax.shard_map(
        functools.partial(on_device, sizes),
        mesh=cut,
        in_specs=(
            P(SP, "tp"),
            P((*SP, "tp"), None),
            P("tp", None),
            P("tp", None),
            P("tp"),
            P("tp", None, None),
            P("tp", None, None),
            P("tp", None, None),
            P("tp", None, None),
            P("tp"),
            P("tp", None),
            P(),
            P(SP, "tp"),
            P(SP, "tp"),
            P("tp", SP),
        ),
        out_specs=P((*SP, "tp"), None),
        check_vma=False,
    )
```

```python
import functools

import jax
import jax.numpy as jnp
from jax import lax
from jax.experimental import pallas as pl
from jax.experimental.pallas import tpu as pltpu
from jax.sharding import Mesh
from jax.sharding import PartitionSpec as P

F32 = jnp.float32
BF16 = jnp.bfloat16
SP = ("h", "u", "m", "v")
PEERS = ("u", "v")
GATHER = 8
CHUNKS = 8
MESH = pl.DeviceIdType.MESH


def discrete(decay_real, decay_imag, log_step, in_real, in_imag):
    step_size = jnp.exp(log_step)[:, None]
    magnitude = jnp.exp(decay_real * step_size)
    angle = decay_imag * step_size
    power_re = magnitude * jnp.cos(angle)
    power_im = magnitude * jnp.sin(angle)
    denom = decay_real * decay_real + decay_imag * decay_imag
    ratio_re = ((power_re - 1.0) * decay_real + power_im * decay_imag) / denom
    ratio_im = (power_im * decay_real - (power_re - 1.0) * decay_imag) / denom
    drive_re = ratio_re[..., None] * in_real - ratio_im[..., None] * in_imag
    drive_im = ratio_re[..., None] * in_imag + ratio_im[..., None] * in_real
    return (power_re, power_im, drive_re, drive_im)


def cmul(ar, ai, br, bi):
    return ar * br - ai * bi, ar * bi + ai * br


def cpow(ar, ai, count):
    result = None
    while count:
        if count & 1:
            result = (ar, ai) if result is None else cmul(*result, ar, ai)
        count >>= 1
        if count:
            ar, ai = cmul(ar, ai, ar, ai)
    return result


def iota(shape, dim):
    return lax.broadcasted_iota(jnp.int32, shape, dim)


def tiled(block, copies, across, down):
    rows, columns = block.shape
    wide = (columns, columns * copies)
    pick = (iota(wide, 0) == lax.rem(iota(wide, 1), columns)).astype(BF16)
    full = jnp.dot(block, pick, preferred_element_type=F32)
    keep = lax.div(iota(full.shape, 0), down) == lax.div(iota(full.shape, 1), across)
    return jnp.where(keep, full, 0.0).astype(BF16)


def layer(sizes, fused, x_ref, b_ref, c_ref, a_ref, k_ref, wo_ref, res_ref, gain_ref, *rest):
    quarters, rest = rest[:3], rest[3:]
    if fused:
        out_ref, *rest = rest
        hidden, partners, peers, *rest = rest
    weights, (rows_ref, carried_ref), rest = rest[:3], rest[3:5], rest[5:]
    (work, read_in, read_out, ends, total, gathered, act, share, others,
     send_sem, recv_sem, local_sem) = rest
    blocks, rows, cb = x_ref.shape
    sb = a_ref.shape[2]
    depth = quarters[0].shape[2]
    width = wo_ref.shape[1]
    span = rows // CHUNKS
    nh, nm, tp = sizes["h"], sizes["m"], sizes["tp"]
    n = nh * 4 * nm
    h, u, m, v, core = (lax.axis_index(name) for name in (*SP, "tp"))
    index = lambda h, u, m, v: ((h * 2 + u) * nm + m) * 2 + v
    me = index(h, u, m, v)
    peer = lambda k: (1 - u if k & 2 else u, 1 - v if k & 1 else v)
    counter = iter(range(send_sem.shape[0]))

    def send(src, dst, device):
        slot = next(counter)
        copy = pltpu.make_async_remote_copy(
            src_ref=src, dst_ref=dst, send_sem=send_sem.at[slot], recv_sem=recv_sem.at[slot],
            device_id=device, device_id_type=MESH,
        )
        copy.start()
        return copy

    def place(ref, position):
        if depth % 128:
            return ref.at[position]
        return ref.at[:, pl.ds(pl.multiple_of(position * depth, depth), depth)]

    barrier = pltpu.get_barrier_semaphore()
    others_sp = []
    for k in range(1, n):
        to = lax.rem(me + k, n)
        there = (lax.div(to, 4 * nm), lax.rem(lax.div(to, 2 * nm), 2),
                 lax.rem(lax.div(to, 2), nm), lax.rem(to, 2), core)
        others_sp.append(there)
        pl.semaphore_signal(barrier, inc=1, device_id=there, device_id_type=MESH)
    for t in range(1, tp):
        pl.semaphore_signal(
            barrier, inc=1, device_id=(h, u, m, v, lax.rem(core + t, tp)), device_id_type=MESH
        )
    pl.semaphore_wait(barrier, n - 1 + tp - 1)

    sent = []
    first = {}
    over_h = {}
    over_m = {}

    def spread_h(w, k, src, position):
        for r in range(1, nh):
            pu, pv = peer(k)
            copy = send(src, place(weights[w], position), (lax.rem(h + r, nh), u, m, v, core))
            over_h[w, k, r] = copy

    def spread_m(w, k, r, src, position):
        for s in range(1, nm):
            over_m[w, k, r, s] = send(
                src, place(weights[w], position), (h, u, lax.rem(m + s, nm), v, core)
            )

    own = u * 2 + v
    for w in range(3):
        for k in (3, 1, 2):
            pu, pv = peer(k)
            first[w, k] = send(
                quarters[w].at[pu * 2 + pv], place(weights[w], me), (h, pu, m, pv, core)
            )
    locals_ = []
    for w in range(3):
        spread_h(w, 0, quarters[w].at[own], me)
        spread_m(w, 0, 0, quarters[w].at[own], me)
        copy = pltpu.make_async_copy(quarters[w].at[own], place(weights[w], me), local_sem.at[w])
        copy.start()
        locals_.append(copy)

    def scan(b, start, keep):
        work[...] = jnp.dot(x_ref[b], read_in[b], preferred_element_type=F32)
        br = jnp.broadcast_to(a_ref[b, 0:1, :], (CHUNKS, sb))
        bi = jnp.broadcast_to(a_ref[b, 1:2, :], (CHUNKS, sb))

        def step(i, state):
            at = pl.ds(pl.multiple_of(i * CHUNKS, CHUNKS), CHUNKS)
            nr, ni = cmul(br, bi, *state)
            nr, ni = nr + work[at, :sb], ni + work[at, sb:]
            if keep:
                work[at, :sb] = nr
                work[at, sb:] = ni
            return nr, ni

        return lax.fori_loop(0, span, step, start, unroll=8)

    @pl.loop(0, blocks)
    def _(b):
        states = b_ref.shape[3]
        for half in range(2):
            read_in[b, :, half * sb:(half + 1) * sb] = tiled(
                b_ref[b, half], GATHER, states, cb // GATHER
            )
            read_out[b, half * sb:(half + 1) * sb, :] = tiled(
                c_ref[b, half], GATHER, cb // GATHER, states
            )
        zero = jnp.zeros((CHUNKS, sb), F32)
        sr, si = scan(b, (zero, zero), False)
        ends[b, :, :sb] = sr
        ends[b, :, sb:] = si
        lr, li = cpow(a_ref[b, 0:1, :], a_ref[b, 1:2, :], span)
        er, ei = sr[0:1], si[0:1]
        for chunk in range(1, CHUNKS):
            er, ei = cmul(lr, li, er, ei)
            er, ei = er + sr[chunk:chunk + 1], ei + si[chunk:chunk + 1]
        total[b, :, :sb] = er
        total[b, :, sb:] = ei

    states_out = [send(total, gathered.at[me], there) for there in others_sp]
    gathered[me] = total[...]
    for copy in states_out:
        copy.wait_recv()

    @pl.loop(0, blocks)
    def _(b):
        lr, li = cpow(a_ref[b, 0:1, :], a_ref[b, 1:2, :], span)
        tr, ti = cpow(lr, li, CHUNKS)
        hr = jnp.zeros((1, sb), F32)
        hi = hr
        for device in range(n - 1):
            nr, ni = cmul(tr, ti, hr, hi)
            nr = nr + gathered[device, b, :, :sb]
            ni = ni + gathered[device, b, :, sb:]
            hr, hi = jnp.where(device < me, nr, hr), jnp.where(device < me, ni, hi)
        starts_r, starts_i = [hr], [hi]
        for chunk in range(CHUNKS - 1):
            nr, ni = cmul(lr, li, hr, hi)
            hr = nr + ends[b, chunk:chunk + 1, :sb]
            hi = ni + ends[b, chunk:chunk + 1, sb:]
            starts_r.append(hr)
            starts_i.append(hi)
        scan(b, (jnp.concatenate(starts_r, axis=0), jnp.concatenate(starts_i, axis=0)), True)
        mixed = jnp.dot(work[...].astype(BF16), read_out[b], preferred_element_type=F32)
        mixed = mixed + k_ref[b] * x_ref[b].astype(F32)
        mixed = jax.nn.gelu(mixed).astype(BF16)
        square = (rows, rows)
        source = lax.rem(iota(square, 0), span) * CHUNKS + lax.div(iota(square, 0), span)
        turn = (iota(square, 1) == source).astype(BF16)
        act[:, pl.ds(pl.multiple_of(b * cb, cb), cb)] = jnp.dot(
            turn, mixed, preferred_element_type=F32
        ).astype(BF16)

    keep_rows = rows // tp
    tile = min(512, width)
    mixed_copies = []
    for t in (*range(1, tp), 0):
        to = lax.rem(core + t, tp)

        @pl.loop(0, width // tile)
        def _(j):
            at = pl.ds(pl.multiple_of(j * tile, tile), tile)
            share[t, :, at] = jnp.dot(
                act[pl.ds(pl.multiple_of(to * keep_rows, keep_rows), keep_rows), :],
                wo_ref[:, at], preferred_element_type=F32,
            ).astype(BF16)

        if t:
            mixed_copies.append(send(share.at[t], others.at[t - 1], (h, u, m, v, to)))

    for w in range(3):
        for k in (1, 2, 3):
            first[w, k].wait_recv()
            pu, pv = peer(k)
            position = index(h, pu, m, pv)
            spread_h(w, k, place(weights[w], position), position)
            spread_m(w, k, 0, place(weights[w], position), position)

    for copy in mixed_copies:
        copy.wait_recv()
    line = min(32, keep_rows)

    @pl.loop(0, keep_rows // line)
    def _(i):
        at = pl.ds(pl.multiple_of(i * line, line), line)
        mixed = share[0, at, :].astype(F32)
        for t in range(1, tp):
            mixed = mixed + others[t - 1, at, :].astype(F32)
        carried = res_ref[at, :].astype(F32) + mixed.astype(BF16).astype(F32)
        scale = lax.rsqrt(jnp.mean(carried * carried, axis=-1, keepdims=True) + 1e-06)
        carried_ref[at, :] = carried
        rows_ref[0, 0, at, :] = (carried * scale * gain_ref[...]).astype(BF16)

    row_copies = {}
    for k in (3, 1, 2):
        pu, pv = peer(k)
        row_copies[k] = send(rows_ref.at[0, 0], rows_ref.at[0, k], (h, pu, m, pv, core))
    last = []
    for t in range(1, tp):
        last.append(send(rows_ref.at[0, 0], rows_ref.at[t, 0], (h, u, m, v, lax.rem(core + t, tp))))

    def pass_m(w, k):
        pu, pv = peer(k)
        for r in range(1, nh):
            over_h[w, k, r].wait_recv()
            position = index(lax.rem(h - r + nh, nh), pu, m, pv)
            spread_m(w, k, r, place(weights[w], position), position)

    for w in range(3):
        for k in range(4):
            pass_m(w, k)
        if w == 1:
            for k in (1, 2, 3):
                row_copies[k].wait_recv()
                for t in range(1, tp):
                    last.append(send(
                        rows_ref.at[0, k], rows_ref.at[t, k], (h, u, m, v, lax.rem(core + t, tp))
                    ))
    sent = [*first.values(), *over_h.values(), *over_m.values(), *states_out, *mixed_copies]
    row_sends = [*row_copies.values(), *last]
    for (w, *_), copy in over_m.items():
        if w < 2 or not fused:
            copy.wait_recv()
    for copy in last:
        copy.wait_recv()
    for copy in locals_:
        copy.wait()
    if fused:
        sent += back(
            sizes, send, peer, (h, u, m, v, core), weights, rows_ref, carried_ref, out_ref,
            hidden, partners, peers, row_sends, [c for (w, *_), c in over_m.items() if w == 2],
        )
    else:
        sent += row_sends
    for copy in sent:
        copy.wait_send()


def back(sizes, send, peer, here, weights, rows_ref, carried_ref, out_ref, hidden, partners,
         peers, row_sends, down_copies):
    tp = sizes["tp"]
    h, u, m, v, core = here
    _, _, keep_rows, width = rows_ref.shape
    across = (((1,), (1,)), ((), ()))

    @pl.loop(0, 4 * tp)
    def _(i):
        t, k = lax.div(i, 4), lax.rem(i, 4)
        block = rows_ref[t, k]
        gate = lax.dot_general(block, weights[0][...], across, preferred_element_type=F32)
        up = lax.dot_general(block, weights[1][...], across, preferred_element_type=F32)
        hidden[i] = (jax.nn.silu(gate) * up).astype(BF16)

    for copy in (*down_copies,):
        copy.wait_recv()
    for copy in row_sends:
        copy.wait_send()

    tile = min(512, width)
    line = min(32, keep_rows)
    sent = []
    peer_copies = []
    from_core = {}

    def reduce(k):
        for copy in from_core[k]:
            copy.wait_recv()

        @pl.loop(0, keep_rows // line)
        def _(i):
            at = pl.ds(pl.multiple_of(i * line, line), line)
            total = rows_ref[0, k, at, :].astype(F32)
            for t in range(1, tp):
                total = total + partners[k, t - 1, at, :].astype(F32)
            rows_ref[0, k, at, :] = total.astype(BF16)

        if k:
            pu, pv = peer(k)
            peer_copies.append(send(rows_ref.at[0, k], peers.at[k - 1], (h, pu, m, pv, core)))

    order = (3, 1, 2, 0)
    for step, k in enumerate(order):
        from_core[k] = []
        for t in (*range(1, tp), 0):
            @pl.loop(0, width // tile)
            def _(j):
                at = pl.ds(pl.multiple_of(j * tile, tile), tile)
                rows_ref[t, k, :, at] = jnp.dot(
                    hidden[t * 4 + k], weights[2][:, at], preferred_element_type=F32
                ).astype(BF16)

            if t:
                from_core[k].append(send(
                    rows_ref.at[t, k], partners.at[k, t - 1],
                    (h, u, m, v, lax.rem(core + tp - t, tp)),
                ))
        reduce(k)
        sent += from_core[k]
    for copy in peer_copies:
        copy.wait_recv()

    @pl.loop(0, keep_rows // line)
    def _(i):
        at = pl.ds(pl.multiple_of(i * line, line), line)
        total = rows_ref[0, 0, at, :].astype(F32)
        for k in range(1, 4):
            total = total + peers[k - 1, at, :].astype(F32)
        total = total.astype(BF16).astype(F32)
        out_ref[at, :] = (carried_ref[at, :] + 0.5 * total).astype(BF16)

    return sent + peer_copies


def streamed(sizes, x_hbm, residual_hbm, decay_re, decay_im, log_step, in_re, in_im, out_re, out_im,
             skip_hbm, wo_hbm, gain_hbm, gate_hbm, up_hbm, down_hbm, out_ref, *rest):
    weights, rest = rest[:3], rest[3:]
    (extra, rows_ref, carried_ref, gates, hidden, partners, firsts, seconds, work, read_in,
     read_out, ends, total, gathered, prefix, plane_total, planes, turn, act, share, others,
     x_raw, x_ref, res_ref, dr_ref, di_ref, ls_ref, inr_ref, ini_ref, outr_ref, outi_ref, k_ref,
     wo_ref, gain_ref, raw, turned, down_ref, a_ref, ratio, send_sem, recv_sem, local_sem, load_sem) = rest
    blocks, rows, cb = x_ref.shape
    sb = a_ref.shape[2]
    slab, depth = weights[0].shape[0], raw.shape[1]
    width = wo_ref.shape[1]
    keep_rows = rows // 2
    span = rows // CHUNKS
    nh, nm = sizes["h"], sizes["m"]
    n = nh * 4 * nm
    h, u, m, v, core = (lax.axis_index(name) for name in (*SP, "tp"))
    oh, ou, om, ov = 1 - h, 1 - u, 1 - m, 1 - v
    index = lambda h, u, m, v: ((h * 2 + u) * nm + m) * 2 + v
    me = index(h, u, m, v)
    to_x, to_z, to_y = (h, u, m, ov, core), (h, ou, m, v, core), (h, u, om, v, core)
    to_c, to_b, to_t = (oh, u, m, v, core), (oh, ou, m, v, core), (h, u, m, v, 1 - core)
    plane = [(h, b, c) for b in (u, ou) for c in (v, ov)]
    plane += [(oh, b, c) for b in (h, oh) for c in (v, ov)]
    is_inner = lax.rem(h + u, 2)
    inner = is_inner == 1
    across = (((1,), (1,)), ((), ()))
    slots, everywhere, inside, moves = {}, [], [], []
    counter = iter(range(send_sem.shape[0]))

    def slot(name):
        return slots.setdefault(name, len(slots))

    def describe(src, dst, device, name, number):
        return pltpu.make_async_remote_copy(
            src_ref=src, dst_ref=dst, send_sem=send_sem.at[number],
            recv_sem=recv_sem.at[slot(name) if isinstance(name, tuple) else name], device_id=device, device_id_type=MESH,
        )

    def send(src, dst, device, name, kept=everywhere):
        number = next(counter)
        copy = describe(src, dst, device, name, number)
        copy.start()
        kept.append((name, number) if kept is inside else copy)

    def arrive(dst, device, name):
        describe(dst, dst, device, name, 0).wait_recv()

    def place(w, position):
        return weights[w].at[:, pl.ds(pl.multiple_of(position * depth, depth), depth)]

    def spot(w, j, row=m):
        a, b, c = plane[j]
        return place(w, index(a, b, row, c))

    def mine(w, b, c):
        at = pl.ds(pl.multiple_of((b * 2 + c) * slab, slab), slab)
        return down_ref.at[at, :] if w == 2 else turned.at[w, at, :]

    def own(w):
        return mine(w, u, v)

    def send_x(w, s):
        if s:
            send(mine(w, ou, ov), extra.at[w], to_x, ("xo", w))
        else:
            send(mine(w, u, ov), spot(w, 0), to_x, ("xu", w))

    def send_z(w, s):
        send(extra.at[w] if s else mine(w, ou, v), spot(w, s), to_z, ("z", w, s))

    def send_c(w, s):
        early, late = slot(("e", w, s)), slot(("l", w, s))
        send(spot(w, 1) if s else own(w), spot(w, s), to_c, late + is_inner * (early - late))

    def send_b(w, s):
        send(extra.at[w] if s else mine(w, ou, v), spot(w, s), to_b, ("e", w, s), inside)

    def relay(w, s):
        send(spot(w, 2 + s), spot(w, 2 + s), to_c, ("l", w, s), inside)

    def send_y(w, j):
        send(own(w) if j == 0 else spot(w, j), spot(w, j), to_y, ("y", w, j))

    def wait_x(w, s):
        if s:
            arrive(extra.at[w], to_x, ("xo", w))
        else:
            arrive(spot(w, 1), to_x, ("xu", w))

    def wait_z(w, s):
        arrive(spot(w, 2 + s), to_z, ("z", w, s))

    def wait_e(w, s):
        arrive(spot(w, 4 + s), to_c, ("e", w, s))

    def wait_l(w, s):
        arrive(spot(w, 6 + s), to_c, ("l", w, s))

    def wait_y(w, j):
        arrive(spot(w, j, om), to_y, ("y", w, j))

    barrier = pltpu.get_barrier_semaphore()
    others_sp = []
    for k in range(1, n):
        to = lax.rem(me + k, n)
        there = (lax.div(to, 4 * nm), lax.rem(lax.div(to, 2 * nm), 2),
                 lax.rem(lax.div(to, 2), nm), lax.rem(to, 2), core)
        others_sp.append(there)
        pl.semaphore_signal(barrier, inc=1, device_id=there, device_id_type=MESH)
    pl.semaphore_signal(barrier, inc=1, device_id=to_t, device_id_type=MESH)
    pairs = ((gate_hbm, raw.at[0]), (up_hbm, raw.at[1]), (decay_re, dr_ref), (decay_im, di_ref),
             (log_step, ls_ref), (x_hbm, x_raw), (in_re, inr_ref), (in_im, ini_ref),
             (out_re, outr_ref), (out_im, outi_ref), (down_hbm, down_ref), (skip_hbm, k_ref),
             (wo_hbm, wo_ref), (residual_hbm, res_ref), (gain_hbm, gain_ref))
    loads = [pltpu.make_async_copy(a, b, load_sem.at[i]) for i, (a, b) in enumerate(pairs)]
    for copy in loads:
        copy.start()
    exact = lax.Precision.HIGHEST

    def flip_weights(w):
        for i in range(raw.shape[2] // depth):
            turned[w, i * depth:(i + 1) * depth, :] = raw[w, :, i * depth:(i + 1) * depth].T

    with jax.named_scope("A_flip"):
        loads[0].wait()
        flip_weights(0)
    with jax.named_scope("A_param"):
        for copy in loads[2:5]:
            copy.wait()
        states = sb // GATHER
        spread = (lax.rem(iota((states, sb), 1), states) == iota((states, sb), 0)).astype(F32)
        chosen = lax.div(iota((GATHER, sb), 1), states) == iota((GATHER, sb), 0)
        for b in range(blocks):
            def lanes(ref):
                wide = jnp.dot(ref[b * GATHER:(b + 1) * GATHER, :], spread, precision=exact,
                               preferred_element_type=F32)
                return jnp.sum(jnp.where(chosen, wide, 0.0), axis=0, keepdims=True)

            groups = ls_ref.shape[1]
            group = (lax.div(iota((groups, sb), 1), states) + b * GATHER
                     == iota((groups, sb), 0)).astype(F32)
            step_size = jnp.exp(jnp.dot(ls_ref[...], group, precision=exact,
                                        preferred_element_type=F32))
            re, im = lanes(dr_ref), lanes(di_ref)
            magnitude = jnp.exp(re * step_size)
            angle = im * step_size
            power_re = magnitude * jnp.cos(angle)
            power_im = magnitude * jnp.sin(angle)
            denom = re * re + im * im
            a_ref[b, 0:1, :] = power_re
            a_ref[b, 1:2, :] = power_im
            ratio[b, 0:1, :] = ((power_re - 1.0) * re + power_im * im) / denom
            ratio[b, 1:2, :] = (power_im * re - (power_re - 1.0) * im) / denom
    with jax.named_scope("A_x"):
        square = (rows, rows)
        source = lax.rem(iota(square, 0), span) * CHUNKS + lax.div(iota(square, 0), span)
        turn[...] = (iota(square, 1) == source).astype(BF16)
        loads[5].wait()
        for b in range(blocks):
            x_ref[b] = lax.dot_general(
                turn[...], x_raw[:, b * cb:(b + 1) * cb], (((0,), (0,)), ((), ())),
                preferred_element_type=F32,
            ).astype(BF16)
    with jax.named_scope("A_barrier"):
        pl.semaphore_wait(barrier, n)
    loads[10].wait()

    def send_inner(w, s):
        @pl.when(inner)
        def _():
            send_b(w, s)

    send_x(0, 1)
    send_z(0, 0)
    send_y(0, 0)
    send_inner(0, 0)
    with jax.named_scope("A_flip1"):
        loads[1].wait()
        flip_weights(1)
        for copy in loads[6:10]:
            copy.wait()

    local = []
    for w in range(3):
        copy = pltpu.make_async_copy(own(w), spot(w, 0), local_sem.at[w])
        copy.start()
        local.append(copy)

    def scan(b, start, keep):
        work[...] = jnp.dot(x_ref[b], read_in[b], preferred_element_type=F32)
        br = jnp.broadcast_to(a_ref[b, 0:1, :], (CHUNKS, sb))
        bi = jnp.broadcast_to(a_ref[b, 1:2, :], (CHUNKS, sb))

        def step(i, state):
            at = pl.ds(pl.multiple_of(i * CHUNKS, CHUNKS), CHUNKS)
            nr, ni = cmul(br, bi, *state)
            nr, ni = nr + work[at, :sb], ni + work[at, sb:]
            if keep:
                work[at, :sb] = nr
                work[at, sb:] = ni
            return nr, ni

        return lax.fori_loop(0, span, step, start, unroll=8)

    size = cb // GATHER
    with jax.named_scope("B_scan1"):
        @pl.loop(0, blocks)
        def _(b):
            keep = lax.div(iota((cb, sb), 0), size) == lax.div(iota((cb, sb), 1), states)
            at = pl.ds(pl.multiple_of(b * cb, cb), cb)
            vr, vi = (jnp.dot(ref[at, :], spread, precision=exact, preferred_element_type=F32)
                      for ref in (inr_ref, ini_ref))
            cr, ci = ratio[b, 0:1, :], ratio[b, 1:2, :]
            read_in[b, :, :sb] = jnp.where(keep, cr * vr - ci * vi, 0.0).astype(BF16)
            read_in[b, :, sb:] = jnp.where(keep, cr * vi + ci * vr, 0.0).astype(BF16)
            zero = jnp.zeros((CHUNKS, sb), F32)
            sr, si = scan(b, (zero, zero), False)
            ends[b, :, :sb] = sr
            ends[b, :, sb:] = si
            lr, li = cpow(a_ref[b, 0:1, :], a_ref[b, 1:2, :], span)
            er, ei = sr[0:1], si[0:1]
            for chunk in range(1, CHUNKS):
                er, ei = cmul(lr, li, er, ei)
                er, ei = er + sr[chunk:chunk + 1], ei + si[chunk:chunk + 1]
            total[b, :, :sb] = er
            total[b, :, sb:] = ei

    here = m * 2 + v
    level = h * 2 + u
    for k, there in enumerate((to_x, to_y, (h, u, om, ov, core))):
        send(total, gathered.at[here], there, ("s", k))
    gathered[here] = total[...]
    send_x(0, 0)
    for w in (1, 2):
        for s in (1, 0):
            send_x(w, s)
    send_y(1, 0)
    send_y(2, 0)
    with jax.named_scope("C_readout"):
        @pl.loop(0, blocks)
        def _(b):
            high = (lax.rem(iota((sb, states), 0), states) == iota((sb, states), 1)).astype(BF16)
            keep = lax.div(iota((sb, cb), 0), states) == lax.div(iota((sb, cb), 1), size)
            at = pl.ds(pl.multiple_of(b * cb, cb), cb)
            for place_in, ref, sign in ((0, outr_ref, 1.0), (1, outi_ref, -1.0)):
                wide = lax.dot_general(high, (sign * ref[at, :]).astype(BF16), across,
                                       preferred_element_type=F32)
                read_out[b, place_in * sb:(place_in + 1) * sb, :] = jnp.where(
                    keep, wide, 0.0).astype(BF16)

    with jax.named_scope("C_states1"):
        for k, (a, b) in enumerate(((m, ov), (om, v), (om, ov))):
            arrive(gathered.at[a * 2 + b], to_x, ("s", k))

    def power_of(b, count):
        return cpow(a_ref[b, 0:1, :], a_ref[b, 1:2, :], count)

    @pl.loop(0, blocks)
    def _(b):
        tr, ti = power_of(b, span * CHUNKS)
        hr = jnp.zeros((1, sb), F32)
        hi, pr, pi = hr, hr, hr
        for device in range(4):
            gr, gi = gathered[device, b, :, :sb], gathered[device, b, :, sb:]
            nr, ni = cmul(tr, ti, hr, hi)
            hr = jnp.where(device < here, nr + gr, hr)
            hi = jnp.where(device < here, ni + gi, hi)
            nr, ni = cmul(tr, ti, pr, pi)
            pr, pi = nr + gr, ni + gi
        prefix[b, :, :sb] = hr
        prefix[b, :, sb:] = hi
        plane_total[b, :, :sb] = pr
        plane_total[b, :, sb:] = pi

    for k, (a, b) in enumerate(((h, ou), (oh, u), (oh, ou))):
        send(plane_total, planes.at[level], (a, b, m, v, core), ("plane", k))
    planes[level] = plane_total[...]
    with jax.named_scope("C_x01"):
        wait_x(0, 1)
    send_z(0, 1)
    send_inner(0, 1)
    send_c(0, 0)
    for copy in loads[11:]:
        copy.wait()
    with jax.named_scope("C_states2"):
        for k, (a, b) in enumerate(((h, ou), (oh, u), (oh, ou))):
            arrive(planes.at[a * 2 + b], to_x, ("plane", k))
    with jax.named_scope("C_x00"):
        wait_x(0, 0)
    send_c(0, 1)
    send_y(0, 1)

    def second(b):
        lr, li = power_of(b, span)
        tr, ti = cpow(lr, li, CHUNKS)
        qr, qi = cpow(tr, ti, 4)
        hr = jnp.zeros((1, sb), F32)
        hi = hr
        for other in range(3):
            nr, ni = cmul(qr, qi, hr, hi)
            hr = jnp.where(other < level, nr + planes[other, b, :, :sb], hr)
            hi = jnp.where(other < level, ni + planes[other, b, :, sb:], hi)
        for device in range(3):
            nr, ni = cmul(tr, ti, hr, hi)
            hr, hi = jnp.where(device < here, nr, hr), jnp.where(device < here, ni, hi)
        hr, hi = hr + prefix[b, :, :sb], hi + prefix[b, :, sb:]
        starts_r, starts_i = [hr], [hi]
        for chunk in range(CHUNKS - 1):
            nr, ni = cmul(lr, li, hr, hi)
            hr = nr + ends[b, chunk:chunk + 1, :sb]
            hi = ni + ends[b, chunk:chunk + 1, sb:]
            starts_r.append(hr)
            starts_i.append(hi)
        scan(b, (jnp.concatenate(starts_r, axis=0), jnp.concatenate(starts_i, axis=0)), True)
        mixed = jnp.dot(work[...].astype(BF16), read_out[b], preferred_element_type=F32)
        at = pl.ds(pl.multiple_of(b * cb, cb), cb)
        mixed = mixed + k_ref[:, at] * x_ref[b].astype(F32)
        mixed = jax.nn.gelu(mixed).astype(BF16)
        act[:, at] = jnp.dot(
            turn[...], mixed, preferred_element_type=F32
        ).astype(BF16)

    def pass_z(w, s):
        with jax.named_scope(f"z{w}{s}"):
            wait_z(w, s)

        @pl.when(inner)
        def _():
            relay(w, s)

        send_y(w, 2 + s)

    def pass_e(w, s):
        with jax.named_scope(f"e{w}{s}"):
            wait_e(w, s)
        send_y(w, 4 + s)

    def pass_l(w, s):
        with jax.named_scope(f"l{w}{s}"):
            wait_l(w, s)
        send_y(w, 6 + s)

    with jax.named_scope("D_scan2a"):
        @pl.loop(0, blocks // 2)
        def _(b):
            second(b)

    pass_z(0, 0)
    send_z(1, 0)
    send_inner(1, 0)
    with jax.named_scope("D_scan2b"):
        @pl.loop(blocks // 2, blocks)
        def _(b):
            second(b)

    pass_z(0, 1)
    with jax.named_scope("D_x11"):
        wait_x(1, 1)
    send_z(1, 1)
    send_inner(1, 1)
    with jax.named_scope("D_x10"):
        wait_x(1, 0)
    send_y(1, 1)

    tile = min(512, width)
    with jax.named_scope("E_outproj"):
        for t in (1, 0):
            to = core if t == 0 else 1 - core

            @pl.loop(0, width // tile)
            def _(j):
                at = pl.ds(pl.multiple_of(j * tile, tile), tile)
                share[t, :, at] = jnp.dot(
                    act[pl.ds(pl.multiple_of(to * keep_rows, keep_rows), keep_rows), :],
                    wo_ref[:, at], preferred_element_type=F32,
                ).astype(BF16)

            if t:
                send(share.at[1], others, to_t, ("mix",))

    with jax.named_scope("G_mix"):
        arrive(others, to_t, ("mix",))
    line = min(32, keep_rows)
    with jax.named_scope("H_norm"):
        @pl.loop(0, keep_rows // line)
        def _(i):
            at = pl.ds(pl.multiple_of(i * line, line), line)
            mixed = share[0, at, :].astype(F32) + others[at, :].astype(F32)
            carried = res_ref[at, :].astype(F32) + mixed.astype(BF16).astype(F32)
            scale = lax.rsqrt(jnp.mean(carried * carried, axis=-1, keepdims=True) + 1e-06)
            carried_ref[at, :] = carried
            rows_ref[0, 0, at, :] = (carried * scale * gain_ref[...]).astype(BF16)

    send(rows_ref.at[0, 0], rows_ref.at[0, 1], to_x, ("r", 1), moves)
    for part in range(2):
        at = pl.ds(part * (keep_rows // 2), keep_rows // 2)
        send(rows_ref.at[0, 0, at], rows_ref.at[0, 2, at], to_z, ("r", 2, part), moves)
    send(rows_ref.at[0, 0], rows_ref.at[1, 0], to_t, ("t", 0), moves)

    def share_core(k):
        send(rows_ref.at[0, k], rows_ref.at[1, k], to_t, ("t", k), moves)

    def wait_core(k):
        arrive(rows_ref.at[1, k], to_t, ("t", k))

    def gate_part(t, k):
        with jax.named_scope(f"gate{t}{k}"):
            gates[4 * t + k] = lax.dot_general(
                rows_ref[t, k], weights[0][...], across, preferred_element_type=F32
            )

    def up_part(t, k):
        with jax.named_scope(f"up{t}{k}"):
            up = lax.dot_general(
                rows_ref[t, k], weights[1][...], across, preferred_element_type=F32
            )
            hidden[pl.ds((4 * t + k) * keep_rows, keep_rows), :] = (
                jax.nn.silu(gates[4 * t + k]) * up
            ).astype(BF16)

    half = keep_rows // 2

    def first_rows():
        with jax.named_scope("r1"):
            arrive(rows_ref.at[0, 1], to_x, ("r", 1))
        share_core(1)

    def relay_rows(part):
        at = pl.ds(part * half, half)
        with jax.named_scope(f"r2{part}"):
            arrive(rows_ref.at[0, 2, at], to_z, ("r", 2, part))
        send(rows_ref.at[0, 2, at], rows_ref.at[0, 3, at], to_x, ("r", 3, part), moves)
        if part:
            share_core(2)

    def last_rows():
        with jax.named_scope("r3"):
            for part in range(2):
                at = pl.ds(part * half, half)
                arrive(rows_ref.at[0, 3, at], to_x, ("r", 3, part))
        share_core(3)

    def second_weights():
        send_z(2, 0)
        send_inner(2, 0)
        send_c(2, 0)
        wait_x(2, 1)
        send_z(2, 1)
        send_inner(2, 1)
        wait_x(2, 0)
        send_y(2, 1)
        send_c(2, 1)

    def whole(w):
        with jax.named_scope(f"y{w}"):
            for j in range(8):
                wait_y(w, j)

    def core_rows(k):
        with jax.named_scope(f"t{k}"):
            wait_core(k)

    send_c(1, 0)
    send_c(1, 1)
    pass_e(0, 0)
    pass_e(0, 1)
    pass_z(1, 0)
    pass_z(1, 1)
    pass_l(0, 0)
    pass_l(0, 1)
    pass_e(1, 0)
    for copy in local:
        copy.wait()
    whole(0)
    core_rows(0)
    gate_part(0, 0)
    gate_part(1, 0)
    pass_e(1, 1)
    first_rows()
    relay_rows(0)
    gate_part(0, 1)
    second_weights()
    core_rows(1)
    gate_part(1, 1)
    pass_l(1, 0)
    pass_l(1, 1)
    relay_rows(1)
    gate_part(0, 2)
    core_rows(2)
    gate_part(1, 2)
    pass_z(2, 0)
    pass_e(2, 0)
    last_rows()
    gate_part(0, 3)
    whole(1)
    up_part(0, 1)
    up_part(1, 1)
    core_rows(3)
    gate_part(1, 3)
    up_part(0, 3)
    up_part(1, 3)
    pass_z(2, 1)
    pass_e(2, 1)
    up_part(0, 2)
    up_part(1, 2)
    pass_l(2, 0)
    up_part(0, 0)
    up_part(1, 0)
    pass_l(2, 1)
    with jax.named_scope("moves"):
        for copy in moves:
            copy.wait_send()

    across_u = width // 8
    chunks = [(a, b, c) for a in (h, oh) for c in (m, om) for b in range(2)]

    def columns(j):
        a, b, c = chunks[j]
        return pl.ds(pl.multiple_of(index(a, b, c, 0) * depth, across_u), across_u)

    def down(j):
        at = columns(j)
        for t in (1, 0):
            result = jnp.dot(
                hidden[4 * t * keep_rows:4 * (t + 1) * keep_rows, :], weights[2][:, at],
                preferred_element_type=F32,
            ).astype(BF16)
            for k in range(4):
                rows_ref[t, k, :, at] = result[k * keep_rows:(k + 1) * keep_rows]
            if t:
                send(rows_ref.at[1, :, :, at], partners.at[j], to_t, ("p", j))

    def add(target, j, other):
        at = columns(j)

        @pl.loop(0, keep_rows // line)
        def _(i):
            lines = pl.ds(pl.multiple_of(i * line, line), line)
            rows_ref[0, target, lines, at] = (
                rows_ref[0, target, lines, at].astype(F32) + other[lines, :].astype(F32)
            ).astype(BF16)

    def pair(j):
        at = columns(j)
        near, far = (1, 2) if j % 2 == 0 else (2, 1)
        device = to_x if j % 2 == 0 else to_z
        arrive(partners.at[j], to_t, ("p", j))
        for place_in, k in enumerate((3, near)):
            add(k, j, partners.at[j, k])
            send(rows_ref.at[0, k, :, at], firsts.at[j, place_in], device, ("f", j, place_in))
        add(far, j, partners.at[j, far])
        add(0, j, partners.at[j, 0])

    def combine(j):
        at = columns(j)
        far = 2 if j % 2 == 0 else 1
        device, other = (to_x, to_z) if j % 2 == 0 else (to_z, to_x)
        arrive(firsts.at[j, 0], device, ("f", j, 0))
        add(far, j, firsts.at[j, 0])
        send(rows_ref.at[0, far, :, at], seconds.at[j], other, ("g", j))
        arrive(firsts.at[j, 1], device, ("f", j, 1))
        add(0, j, firsts.at[j, 1])

    def finish(j):
        at = columns(j)
        arrive(seconds.at[j], to_z if j % 2 == 0 else to_x, ("g", j))

        @pl.loop(0, keep_rows // line)
        def _(i):
            lines = pl.ds(pl.multiple_of(i * line, line), line)
            summed = rows_ref[0, 0, lines, at].astype(F32) + seconds[j, lines, :].astype(F32)
            summed = summed.astype(BF16).astype(F32)
            out_ref[lines, at] = (carried_ref[lines, at] + 0.5 * summed).astype(BF16)

    lag = (1, 3, 5)
    for step in range(8 + lag[2]):
        if step < 8:
            if step == 2:
                with jax.named_scope("y2a"):
                    for j in range(4):
                        wait_y(2, j)
            if step == 6:
                with jax.named_scope("y2b"):
                    for j in range(4, 8):
                        wait_y(2, j)
            with jax.named_scope(f"down{step}"):
                down(step)
        if 0 <= step - lag[0] < 8:
            with jax.named_scope(f"pair{step - lag[0]}"):
                pair(step - lag[0])
        if 0 <= step - lag[1] < 8:
            with jax.named_scope(f"comb{step - lag[1]}"):
                combine(step - lag[1])
        if 0 <= step - lag[2] < 8:
            with jax.named_scope(f"fin{step - lag[2]}"):
                finish(step - lag[2])
    for copy in everywhere:
        copy.wait_send()

    @pl.when(inner)
    def _():
        for name, number in inside:
            describe(extra.at[0], extra.at[0], to_c, name, number).wait_send()


def shift(value, axis, count, by):
    return lax.ppermute(value, axis, [(i, (i + by) % count) for i in range(count)])


def flip(value, axes, count, k):
    return lax.ppermute(value, axes, [(i, i ^ k) for i in range(count)])


def on_device(sizes, mixer_in, residual, decay_real, decay_imag, log_step, in_real, in_imag,
              output_real, output_imaginary, skip, out_proj, norm_gain, w_gate, w_up, w_down):
    tp, nh, nm = sizes["tp"], sizes["h"], sizes["m"]
    n = nh * 4 * nm
    rows, channels = mixer_in.shape
    keep_rows, width = residual.shape
    depth, hidden_units = w_gate.shape
    part = hidden_units // 4
    groups, states = decay_real.shape
    blocks = groups // GATHER
    cb, sb = channels // blocks, GATHER * states
    vmem = pl.BlockSpec(memory_space=pltpu.VMEM)
    if depth % 128 == 0 and (tp, nh, nm) == (2, 2, 2):
        cut = width // 8
        return pl.pallas_call(
            functools.partial(streamed, sizes),
            in_specs=[pl.BlockSpec(memory_space=pl.ANY)] * 15,
            out_specs=vmem,
            out_shape=jax.ShapeDtypeStruct((keep_rows, width), BF16),
            scratch_shapes=[
                *[pltpu.VMEM((part, n * depth), BF16)] * 3,
                pltpu.VMEM((3, part, depth), BF16),
                pltpu.VMEM((2, 4, keep_rows, width), BF16),
                pltpu.VMEM((keep_rows, width), F32),
                pltpu.VMEM((8, keep_rows, part), F32),
                pltpu.VMEM((8 * keep_rows, part), BF16),
                pltpu.VMEM((8, 4, keep_rows, cut), BF16),
                pltpu.VMEM((8, 2, keep_rows, cut), BF16),
                pltpu.VMEM((8, keep_rows, cut), BF16),
                pltpu.VMEM((rows, 2 * sb), F32),
                pltpu.VMEM((blocks, cb, 2 * sb), BF16),
                pltpu.VMEM((blocks, 2 * sb, cb), BF16),
                pltpu.VMEM((blocks, CHUNKS, 2 * sb), F32),
                pltpu.VMEM((blocks, 1, 2 * sb), F32),
                pltpu.VMEM((4, blocks, 1, 2 * sb), F32),
                pltpu.VMEM((blocks, 1, 2 * sb), F32),
                pltpu.VMEM((blocks, 1, 2 * sb), F32),
                pltpu.VMEM((4, blocks, 1, 2 * sb), F32),
                pltpu.VMEM((rows, rows), BF16),
                pltpu.VMEM((rows, channels), BF16),
                pltpu.VMEM((2, keep_rows, width), BF16),
                pltpu.VMEM((keep_rows, width), BF16),
                pltpu.VMEM((rows, channels), BF16),
                pltpu.VMEM((blocks, rows, cb), BF16),
                pltpu.VMEM((keep_rows, width), BF16),
                *[pltpu.VMEM((groups, states), F32)] * 2,
                pltpu.VMEM((1, groups), F32),
                *[pltpu.VMEM((channels, states), F32)] * 4,
                pltpu.VMEM((1, channels), F32),
                pltpu.VMEM((channels, width), BF16),
                pltpu.VMEM((1, width), F32),
                pltpu.VMEM((2, depth, hidden_units), BF16),
                pltpu.VMEM((2, hidden_units, depth), BF16),
                pltpu.VMEM((hidden_units, depth), BF16),
                pltpu.VMEM((blocks, 2, sb), F32),
                pltpu.VMEM((blocks, 2, sb), F32),
                pltpu.SemaphoreType.DMA((160,)),
                pltpu.SemaphoreType.DMA((160,)),
                pltpu.SemaphoreType.DMA((3,)),
                pltpu.SemaphoreType.DMA((15,)),
            ],
            compiler_params=pltpu.CompilerParams(
                collective_id=0, has_side_effects=True, vmem_limit_bytes=62 * 2**20
            ),
            name="streamed",
        )(mixer_in, residual, decay_real, decay_imag, log_step.reshape(1, groups),
          in_real.transpose(0, 2, 1).reshape(channels, states),
          in_imag.transpose(0, 2, 1).reshape(channels, states),
          output_real.reshape(channels, states), output_imaginary.reshape(channels, states),
          skip.reshape(1, channels), out_proj, norm_gain.reshape(1, width), w_gate, w_up, w_down)
    power_re, power_im, bar_re, bar_im = discrete(
        decay_real, decay_imag, log_step, in_real, in_imag
    )
    rows_first = lambda t: jnp.transpose(t, (0, 2, 1)).reshape(blocks, -1, t.shape[1])
    read_in = jnp.stack([rows_first(bar_re), rows_first(bar_im)], axis=1).astype(BF16)
    read_out = jnp.stack(
        [rows_first(output_real), -rows_first(output_imaginary)], axis=1
    ).astype(BF16)
    power = jnp.stack([power_re.reshape(blocks, sb), power_im.reshape(blocks, sb)], axis=1)
    x = mixer_in.reshape(CHUNKS, rows // CHUNKS, blocks, cb).transpose(2, 1, 0, 3)
    x = x.reshape(blocks, rows, cb)
    operands = (x, read_in, read_out, power, skip.reshape(blocks, 1, cb), out_proj, residual,
                norm_gain.reshape(1, width), w_gate.T.reshape(4, part, depth),
                w_up.T.reshape(4, part, depth), w_down.reshape(4, part, depth))
    copies = 3 * (3 + 4 * (nh - 1) + 4 * nh * (nm - 1)) + (n - 1) + (tp - 1) + 3 + 4 * (tp - 1)
    laid = (part, n * depth) if depth % 128 == 0 else (n, part, depth)
    between = [(laid, BF16)] * 3 + [
        ((tp, 4, keep_rows, width), BF16), ((keep_rows, width), F32),
    ]
    fused = depth % 128 == 0
    if fused:
        copies += 4 * (tp - 1) + 3
        out_shape = [jax.ShapeDtypeStruct((keep_rows, width), BF16)]
        extra = [
            pltpu.VMEM((4 * tp, keep_rows, part), BF16),
            pltpu.VMEM((4, tp - 1, keep_rows, width), BF16),
            pltpu.VMEM((3, keep_rows, width), BF16),
            *(pltpu.VMEM(*item) for item in between),
        ]
    else:
        out_shape = [jax.ShapeDtypeStruct(*item) for item in between]
        extra = []
    results = pl.pallas_call(
        functools.partial(layer, sizes, fused),
        in_specs=[vmem] * 11,
        out_specs=[vmem] * len(out_shape),
        out_shape=out_shape,
        scratch_shapes=[
            *extra,
            pltpu.VMEM((rows, 2 * sb), F32),
            pltpu.VMEM((blocks, cb, 2 * sb), BF16),
            pltpu.VMEM((blocks, 2 * sb, cb), BF16),
            pltpu.VMEM((blocks, CHUNKS, 2 * sb), F32),
            pltpu.VMEM((blocks, 1, 2 * sb), F32),
            pltpu.VMEM((n, blocks, 1, 2 * sb), F32),
            pltpu.VMEM((rows, channels), BF16),
            pltpu.VMEM((tp, keep_rows, width), BF16),
            pltpu.VMEM((tp - 1, keep_rows, width), BF16),
            pltpu.SemaphoreType.DMA((copies,)),
            pltpu.SemaphoreType.DMA((copies,)),
            pltpu.SemaphoreType.DMA((3,)),
        ],
        compiler_params=pltpu.CompilerParams(
            collective_id=0, has_side_effects=True, vmem_limit_bytes=62 * 2**20
        ),
        name="layer",
    )(*operands)
    if fused:
        return results[0]
    full_gate, full_up, full_down, rows_all, carried = results
    if len(laid) == 3:
        full_gate, full_up, full_down = (
            t.transpose(1, 0, 2).reshape(part, width) for t in (full_gate, full_up, full_down)
        )

    flat = rows_all.reshape(-1, width)
    across = (((1,), (1,)), ((), ()))
    gate = lax.dot_general(flat, full_gate, across, preferred_element_type=F32)
    up = lax.dot_general(flat, full_up, across, preferred_element_type=F32)
    hidden = (jax.nn.silu(gate) * up).astype(BF16)
    down = jnp.dot(hidden, full_down, preferred_element_type=F32).astype(BF16)
    down = down.reshape(rows_all.shape)
    summed = down[0].astype(F32)
    for t in range(1, tp):
        summed = summed + shift(down[t], "tp", tp, -t).astype(F32)
    summed = summed.astype(BF16)
    total = summed[0].astype(F32)
    for k in range(1, 4):
        total = total + flip(summed[k], PEERS, 4, k).astype(F32)
    total = total.astype(BF16)
    return (carried + 0.5 * total.astype(F32)).astype(BF16)


def solution(mesh):
    sp, tp = mesh.shape["sp"], mesh.shape["tp"]
    sizes = {"h": sp // 8, "u": 2, "m": 2, "v": 2, "tp": tp}
    cut = Mesh(mesh.devices.reshape(tuple(sizes.values())), tuple(sizes))
    return jax.shard_map(
        functools.partial(on_device, sizes),
        mesh=cut,
        in_specs=(
            P(SP, "tp"),
            P((*SP, "tp"), None),
            P("tp", None),
            P("tp", None),
            P("tp"),
            P("tp", None, None),
            P("tp", None, None),
            P("tp", None, None),
            P("tp", None, None),
            P("tp"),
            P("tp", None),
            P(),
            P(SP, "tp"),
            P(SP, "tp"),
            P("tp", SP),
        ),
        out_specs=P((*SP, "tp"), None),
        check_vma=False,
    )
```

```python
import functools

import jax
import jax.numpy as jnp
from jax import lax
from jax.experimental import pallas as pl
from jax.experimental.pallas import tpu as pltpu
from jax.sharding import Mesh
from jax.sharding import PartitionSpec as P

F32 = jnp.float32
BF16 = jnp.bfloat16
SP = ("h", "u", "m", "v")
PEERS = ("u", "v")
GATHER = 8
CHUNKS = 8
X_FIRST = (1, 0, 1, 0, 1, 0, 1, 0)
PIECES = 4
MESH = pl.DeviceIdType.MESH


def discrete(decay_real, decay_imag, log_step, in_real, in_imag):
    step_size = jnp.exp(log_step)[:, None]
    magnitude = jnp.exp(decay_real * step_size)
    angle = decay_imag * step_size
    power_re = magnitude * jnp.cos(angle)
    power_im = magnitude * jnp.sin(angle)
    denom = decay_real * decay_real + decay_imag * decay_imag
    ratio_re = ((power_re - 1.0) * decay_real + power_im * decay_imag) / denom
    ratio_im = (power_im * decay_real - (power_re - 1.0) * decay_imag) / denom
    drive_re = ratio_re[..., None] * in_real - ratio_im[..., None] * in_imag
    drive_im = ratio_re[..., None] * in_imag + ratio_im[..., None] * in_real
    return (power_re, power_im, drive_re, drive_im)


def cmul(ar, ai, br, bi):
    return ar * br - ai * bi, ar * bi + ai * br


def cpow(ar, ai, count):
    result = None
    while count:
        if count & 1:
            result = (ar, ai) if result is None else cmul(*result, ar, ai)
        count >>= 1
        if count:
            ar, ai = cmul(ar, ai, ar, ai)
    return result


def iota(shape, dim):
    return lax.broadcasted_iota(jnp.int32, shape, dim)


def tiled(block, copies, across, down):
    rows, columns = block.shape
    wide = (columns, columns * copies)
    pick = (iota(wide, 0) == lax.rem(iota(wide, 1), columns)).astype(BF16)
    full = jnp.dot(block, pick, preferred_element_type=F32)
    keep = lax.div(iota(full.shape, 0), down) == lax.div(iota(full.shape, 1), across)
    return jnp.where(keep, full, 0.0).astype(BF16)


def layer(sizes, fused, x_ref, b_ref, c_ref, a_ref, k_ref, wo_ref, res_ref, gain_ref, *rest):
    quarters, rest = rest[:3], rest[3:]
    if fused:
        out_ref, *rest = rest
        hidden, partners, peers, *rest = rest
    weights, (rows_ref, carried_ref), rest = rest[:3], rest[3:5], rest[5:]
    (work, read_in, read_out, ends, total, gathered, act, share, others,
     send_sem, recv_sem, local_sem) = rest
    blocks, rows, cb = x_ref.shape
    sb = a_ref.shape[2]
    depth = quarters[0].shape[2]
    width = wo_ref.shape[1]
    span = rows // CHUNKS
    nh, nm, tp = sizes["h"], sizes["m"], sizes["tp"]
    n = nh * 4 * nm
    h, u, m, v, core = (lax.axis_index(name) for name in (*SP, "tp"))
    index = lambda h, u, m, v: ((h * 2 + u) * nm + m) * 2 + v
    me = index(h, u, m, v)
    peer = lambda k: (1 - u if k & 2 else u, 1 - v if k & 1 else v)
    counter = iter(range(send_sem.shape[0]))

    def send(src, dst, device):
        slot = next(counter)
        copy = pltpu.make_async_remote_copy(
            src_ref=src, dst_ref=dst, send_sem=send_sem.at[slot], recv_sem=recv_sem.at[slot],
            device_id=device, device_id_type=MESH,
        )
        copy.start()
        return copy

    def place(ref, position):
        if depth % 128:
            return ref.at[position]
        return ref.at[:, pl.ds(pl.multiple_of(position * depth, depth), depth)]

    barrier = pltpu.get_barrier_semaphore()
    others_sp = []
    for k in range(1, n):
        to = lax.rem(me + k, n)
        there = (lax.div(to, 4 * nm), lax.rem(lax.div(to, 2 * nm), 2),
                 lax.rem(lax.div(to, 2), nm), lax.rem(to, 2), core)
        others_sp.append(there)
        pl.semaphore_signal(barrier, inc=1, device_id=there, device_id_type=MESH)
    for t in range(1, tp):
        pl.semaphore_signal(
            barrier, inc=1, device_id=(h, u, m, v, lax.rem(core + t, tp)), device_id_type=MESH
        )
    pl.semaphore_wait(barrier, n - 1 + tp - 1)

    sent = []
    first = {}
    over_h = {}
    over_m = {}

    def spread_h(w, k, src, position):
        for r in range(1, nh):
            pu, pv = peer(k)
            copy = send(src, place(weights[w], position), (lax.rem(h + r, nh), u, m, v, core))
            over_h[w, k, r] = copy

    def spread_m(w, k, r, src, position):
        for s in range(1, nm):
            over_m[w, k, r, s] = send(
                src, place(weights[w], position), (h, u, lax.rem(m + s, nm), v, core)
            )

    own = u * 2 + v
    for w in range(3):
        for k in (3, 1, 2):
            pu, pv = peer(k)
            first[w, k] = send(
                quarters[w].at[pu * 2 + pv], place(weights[w], me), (h, pu, m, pv, core)
            )
    locals_ = []
    for w in range(3):
        spread_h(w, 0, quarters[w].at[own], me)
        spread_m(w, 0, 0, quarters[w].at[own], me)
        copy = pltpu.make_async_copy(quarters[w].at[own], place(weights[w], me), local_sem.at[w])
        copy.start()
        locals_.append(copy)

    def scan(b, start, keep):
        work[...] = jnp.dot(x_ref[b], read_in[b], preferred_element_type=F32)
        br = jnp.broadcast_to(a_ref[b, 0:1, :], (CHUNKS, sb))
        bi = jnp.broadcast_to(a_ref[b, 1:2, :], (CHUNKS, sb))

        def step(i, state):
            at = pl.ds(pl.multiple_of(i * CHUNKS, CHUNKS), CHUNKS)
            nr, ni = cmul(br, bi, *state)
            nr, ni = nr + work[at, :sb], ni + work[at, sb:]
            if keep:
                work[at, :sb] = nr
                work[at, sb:] = ni
            return nr, ni

        return lax.fori_loop(0, span, step, start, unroll=8)

    @pl.loop(0, blocks)
    def _(b):
        states = b_ref.shape[3]
        for half in range(2):
            read_in[b, :, half * sb:(half + 1) * sb] = tiled(
                b_ref[b, half], GATHER, states, cb // GATHER
            )
            read_out[b, half * sb:(half + 1) * sb, :] = tiled(
                c_ref[b, half], GATHER, cb // GATHER, states
            )
        zero = jnp.zeros((CHUNKS, sb), F32)
        sr, si = scan(b, (zero, zero), False)
        ends[b, :, :sb] = sr
        ends[b, :, sb:] = si
        lr, li = cpow(a_ref[b, 0:1, :], a_ref[b, 1:2, :], span)
        er, ei = sr[0:1], si[0:1]
        for chunk in range(1, CHUNKS):
            er, ei = cmul(lr, li, er, ei)
            er, ei = er + sr[chunk:chunk + 1], ei + si[chunk:chunk + 1]
        total[b, :, :sb] = er
        total[b, :, sb:] = ei

    states_out = [send(total, gathered.at[me], there) for there in others_sp]
    gathered[me] = total[...]
    for copy in states_out:
        copy.wait_recv()

    @pl.loop(0, blocks)
    def _(b):
        lr, li = cpow(a_ref[b, 0:1, :], a_ref[b, 1:2, :], span)
        tr, ti = cpow(lr, li, CHUNKS)
        hr = jnp.zeros((1, sb), F32)
        hi = hr
        for device in range(n - 1):
            nr, ni = cmul(tr, ti, hr, hi)
            nr = nr + gathered[device, b, :, :sb]
            ni = ni + gathered[device, b, :, sb:]
            hr, hi = jnp.where(device < me, nr, hr), jnp.where(device < me, ni, hi)
        starts_r, starts_i = [hr], [hi]
        for chunk in range(CHUNKS - 1):
            nr, ni = cmul(lr, li, hr, hi)
            hr = nr + ends[b, chunk:chunk + 1, :sb]
            hi = ni + ends[b, chunk:chunk + 1, sb:]
            starts_r.append(hr)
            starts_i.append(hi)
        scan(b, (jnp.concatenate(starts_r, axis=0), jnp.concatenate(starts_i, axis=0)), True)
        mixed = jnp.dot(work[...].astype(BF16), read_out[b], preferred_element_type=F32)
        mixed = mixed + k_ref[b] * x_ref[b].astype(F32)
        mixed = jax.nn.gelu(mixed).astype(BF16)
        square = (rows, rows)
        source = lax.rem(iota(square, 0), span) * CHUNKS + lax.div(iota(square, 0), span)
        turn = (iota(square, 1) == source).astype(BF16)
        act[:, pl.ds(pl.multiple_of(b * cb, cb), cb)] = jnp.dot(
            turn, mixed, preferred_element_type=F32
        ).astype(BF16)

    keep_rows = rows // tp
    tile = min(512, width)
    mixed_copies = []
    for t in (*range(1, tp), 0):
        to = lax.rem(core + t, tp)

        @pl.loop(0, width // tile)
        def _(j):
            at = pl.ds(pl.multiple_of(j * tile, tile), tile)
            share[t, :, at] = jnp.dot(
                act[pl.ds(pl.multiple_of(to * keep_rows, keep_rows), keep_rows), :],
                wo_ref[:, at], preferred_element_type=F32,
            ).astype(BF16)

        if t:
            mixed_copies.append(send(share.at[t], others.at[t - 1], (h, u, m, v, to)))

    for w in range(3):
        for k in (1, 2, 3):
            first[w, k].wait_recv()
            pu, pv = peer(k)
            position = index(h, pu, m, pv)
            spread_h(w, k, place(weights[w], position), position)
            spread_m(w, k, 0, place(weights[w], position), position)

    for copy in mixed_copies:
        copy.wait_recv()
    line = min(32, keep_rows)

    @pl.loop(0, keep_rows // line)
    def _(i):
        at = pl.ds(pl.multiple_of(i * line, line), line)
        mixed = share[0, at, :].astype(F32)
        for t in range(1, tp):
            mixed = mixed + others[t - 1, at, :].astype(F32)
        carried = res_ref[at, :].astype(F32) + mixed.astype(BF16).astype(F32)
        scale = lax.rsqrt(jnp.mean(carried * carried, axis=-1, keepdims=True) + 1e-06)
        carried_ref[at, :] = carried
        rows_ref[0, 0, at, :] = (carried * scale * gain_ref[...]).astype(BF16)

    row_copies = {}
    for k in (3, 1, 2):
        pu, pv = peer(k)
        row_copies[k] = send(rows_ref.at[0, 0], rows_ref.at[0, k], (h, pu, m, pv, core))
    last = []
    for t in range(1, tp):
        last.append(send(rows_ref.at[0, 0], rows_ref.at[t, 0], (h, u, m, v, lax.rem(core + t, tp))))

    def pass_m(w, k):
        pu, pv = peer(k)
        for r in range(1, nh):
            over_h[w, k, r].wait_recv()
            position = index(lax.rem(h - r + nh, nh), pu, m, pv)
            spread_m(w, k, r, place(weights[w], position), position)

    for w in range(3):
        for k in range(4):
            pass_m(w, k)
        if w == 1:
            for k in (1, 2, 3):
                row_copies[k].wait_recv()
                for t in range(1, tp):
                    last.append(send(
                        rows_ref.at[0, k], rows_ref.at[t, k], (h, u, m, v, lax.rem(core + t, tp))
                    ))
    sent = [*first.values(), *over_h.values(), *over_m.values(), *states_out, *mixed_copies]
    row_sends = [*row_copies.values(), *last]
    for (w, *_), copy in over_m.items():
        if w < 2 or not fused:
            copy.wait_recv()
    for copy in last:
        copy.wait_recv()
    for copy in locals_:
        copy.wait()
    if fused:
        sent += back(
            sizes, send, peer, (h, u, m, v, core), weights, rows_ref, carried_ref, out_ref,
            hidden, partners, peers, row_sends, [c for (w, *_), c in over_m.items() if w == 2],
        )
    else:
        sent += row_sends
    for copy in sent:
        copy.wait_send()


def back(sizes, send, peer, here, weights, rows_ref, carried_ref, out_ref, hidden, partners,
         peers, row_sends, down_copies):
    tp = sizes["tp"]
    h, u, m, v, core = here
    _, _, keep_rows, width = rows_ref.shape
    across = (((1,), (1,)), ((), ()))

    @pl.loop(0, 4 * tp)
    def _(i):
        t, k = lax.div(i, 4), lax.rem(i, 4)
        block = rows_ref[t, k]
        gate = lax.dot_general(block, weights[0][...], across, preferred_element_type=F32)
        up = lax.dot_general(block, weights[1][...], across, preferred_element_type=F32)
        hidden[i] = (jax.nn.silu(gate) * up).astype(BF16)

    for copy in (*down_copies,):
        copy.wait_recv()
    for copy in row_sends:
        copy.wait_send()

    tile = min(512, width)
    line = min(32, keep_rows)
    sent = []
    peer_copies = []
    from_core = {}

    def reduce(k):
        for copy in from_core[k]:
            copy.wait_recv()

        @pl.loop(0, keep_rows // line)
        def _(i):
            at = pl.ds(pl.multiple_of(i * line, line), line)
            total = rows_ref[0, k, at, :].astype(F32)
            for t in range(1, tp):
                total = total + partners[k, t - 1, at, :].astype(F32)
            rows_ref[0, k, at, :] = total.astype(BF16)

        if k:
            pu, pv = peer(k)
            peer_copies.append(send(rows_ref.at[0, k], peers.at[k - 1], (h, pu, m, pv, core)))

    order = (3, 1, 2, 0)
    for step, k in enumerate(order):
        from_core[k] = []
        for t in (*range(1, tp), 0):
            @pl.loop(0, width // tile)
            def _(j):
                at = pl.ds(pl.multiple_of(j * tile, tile), tile)
                rows_ref[t, k, :, at] = jnp.dot(
                    hidden[t * 4 + k], weights[2][:, at], preferred_element_type=F32
                ).astype(BF16)

            if t:
                from_core[k].append(send(
                    rows_ref.at[t, k], partners.at[k, t - 1],
                    (h, u, m, v, lax.rem(core + tp - t, tp)),
                ))
        reduce(k)
        sent += from_core[k]
    for copy in peer_copies:
        copy.wait_recv()

    @pl.loop(0, keep_rows // line)
    def _(i):
        at = pl.ds(pl.multiple_of(i * line, line), line)
        total = rows_ref[0, 0, at, :].astype(F32)
        for k in range(1, 4):
            total = total + peers[k - 1, at, :].astype(F32)
        total = total.astype(BF16).astype(F32)
        out_ref[at, :] = (carried_ref[at, :] + 0.5 * total).astype(BF16)

    return sent + peer_copies


def streamed(sizes, x_hbm, residual_hbm, decay_re, decay_im, log_step, in_re, in_im, out_re, out_im,
             skip_hbm, wo_hbm, gain_hbm, gate_hbm, up_hbm, down_hbm, out_ref, *rest):
    weights, rest = rest[:3], rest[3:]
    (extra, rows_ref, carried_ref, gates, hidden, partners, firsts, seconds, work, read_in,
     read_out, ends, total, gathered, prefix, plane_total, planes, turn, act, share, others,
     x_raw, x_ref, res_ref, dr_ref, di_ref, ls_ref, inr_ref, ini_ref, outr_ref, outi_ref, k_ref,
     wo_ref, gain_ref, raw, turned, down_ref, a_ref, ratio, send_sem, recv_sem, local_sem, load_sem) = rest
    blocks, rows, cb = x_ref.shape
    sb = a_ref.shape[2]
    slab, depth = weights[0].shape[0], raw.shape[1]
    width = wo_ref.shape[1]
    keep_rows = rows // 2
    span = rows // CHUNKS
    nh, nm = sizes["h"], sizes["m"]
    n = nh * 4 * nm
    h, u, m, v, core = (lax.axis_index(name) for name in (*SP, "tp"))
    oh, ou, om, ov = 1 - h, 1 - u, 1 - m, 1 - v
    index = lambda h, u, m, v: ((h * 2 + u) * nm + m) * 2 + v
    me = index(h, u, m, v)
    to_x, to_z, to_y = (h, u, m, ov, core), (h, ou, m, v, core), (h, u, om, v, core)
    to_c, to_b, to_t = (oh, u, m, v, core), (oh, ou, m, v, core), (h, u, m, v, 1 - core)
    plane = [(h, b, c) for b in (u, ou) for c in (v, ov)]
    plane += [(oh, b, c) for b in (h, oh) for c in (v, ov)]
    is_inner = lax.rem(h + u, 2)
    inner = is_inner == 1
    across = (((1,), (1,)), ((), ()))
    slots, everywhere, inside, moves = {}, [], [], []
    counter = iter(range(send_sem.shape[0]))

    def slot(name):
        return slots.setdefault(name, len(slots))

    def describe(src, dst, device, name, number):
        return pltpu.make_async_remote_copy(
            src_ref=src, dst_ref=dst, send_sem=send_sem.at[number],
            recv_sem=recv_sem.at[slot(name) if isinstance(name, tuple) else name], device_id=device, device_id_type=MESH,
        )

    def send(src, dst, device, name, kept=everywhere):
        number = next(counter)
        copy = describe(src, dst, device, name, number)
        copy.start()
        kept.append((name, number) if kept is inside else copy)

    def arrive(dst, device, name):
        describe(dst, dst, device, name, 0).wait_recv()

    def place(w, position):
        return weights[w].at[:, pl.ds(pl.multiple_of(position * depth, depth), depth)]

    def spot(w, j, row=m):
        a, b, c = plane[j]
        return place(w, index(a, b, row, c))

    def mine(w, b, c):
        at = pl.ds(pl.multiple_of((b * 2 + c) * slab, slab), slab)
        return down_ref.at[at, :] if w == 2 else turned.at[w, at, :]

    def own(w):
        return mine(w, u, v)

    def send_x(w, s):
        if s:
            send(mine(w, ou, ov), extra.at[w], to_x, ("xo", w))
        else:
            send(mine(w, u, ov), spot(w, 0), to_x, ("xu", w))

    def send_z(w, s):
        send(extra.at[w] if s else mine(w, ou, v), spot(w, s), to_z, ("z", w, s))

    numbers = {}

    def send_c(w, s, kind):
        number = numbers.setdefault((w, s), None) or next(counter)
        if numbers[w, s] is None:
            numbers[w, s] = number
            everywhere.append(describe(extra.at[0], extra.at[0], to_c, ("e", w, s), number))
        name = ("e" if kind else "l", w, s)

        @pl.when(is_inner == kind)
        def _():
            describe(spot(w, 1) if s else own(w), spot(w, s), to_c, name, number).start()

    def send_b(w, s):
        send(extra.at[w] if s else mine(w, ou, v), spot(w, s), to_b, ("e", w, s), inside)

    def relay(w, s):
        send(spot(w, 2 + s), spot(w, 2 + s), to_c, ("l", w, s), inside)

    def send_y(w, j):
        send(own(w) if j == 0 else spot(w, j), spot(w, j), to_y, ("y", w, j))

    def wait_x(w, s):
        if s:
            arrive(extra.at[w], to_x, ("xo", w))
        else:
            arrive(spot(w, 1), to_x, ("xu", w))

    def wait_z(w, s):
        arrive(spot(w, 2 + s), to_z, ("z", w, s))

    def wait_e(w, s):
        arrive(spot(w, 4 + s), to_c, ("e", w, s))

    def wait_l(w, s):
        arrive(spot(w, 6 + s), to_c, ("l", w, s))

    def wait_y(w, j):
        arrive(spot(w, j, om), to_y, ("y", w, j))

    barrier = pltpu.get_barrier_semaphore()
    others_sp = []
    for k in range(1, n):
        to = lax.rem(me + k, n)
        there = (lax.div(to, 4 * nm), lax.rem(lax.div(to, 2 * nm), 2),
                 lax.rem(lax.div(to, 2), nm), lax.rem(to, 2), core)
        others_sp.append(there)
        pl.semaphore_signal(barrier, inc=1, device_id=there, device_id_type=MESH)
    pl.semaphore_signal(barrier, inc=1, device_id=to_t, device_id_type=MESH)
    pairs = ((gate_hbm, raw.at[0]), (up_hbm, raw.at[1]), (decay_re, dr_ref), (decay_im, di_ref),
             (log_step, ls_ref), (x_hbm, x_raw), (in_re, inr_ref), (in_im, ini_ref),
             (out_re, outr_ref), (out_im, outi_ref), (down_hbm, down_ref), (skip_hbm, k_ref),
             (wo_hbm, wo_ref), (residual_hbm, res_ref), (gain_hbm, gain_ref))
    loads = [pltpu.make_async_copy(a, b, load_sem.at[i]) for i, (a, b) in enumerate(pairs)]
    for copy in loads:
        copy.start()
    exact = lax.Precision.HIGHEST

    def flip_weights(w):
        for i in range(raw.shape[2] // depth):
            turned[w, i * depth:(i + 1) * depth, :] = raw[w, :, i * depth:(i + 1) * depth].T

    with jax.named_scope("A_flip"):
        loads[0].wait()
        flip_weights(0)
    with jax.named_scope("A_param"):
        for copy in loads[2:5]:
            copy.wait()
        states = sb // GATHER
        spread = (lax.rem(iota((states, sb), 1), states) == iota((states, sb), 0)).astype(F32)
        chosen = lax.div(iota((GATHER, sb), 1), states) == iota((GATHER, sb), 0)
        for b in range(blocks):
            def lanes(ref):
                wide = jnp.dot(ref[b * GATHER:(b + 1) * GATHER, :], spread, precision=exact,
                               preferred_element_type=F32)
                return jnp.sum(jnp.where(chosen, wide, 0.0), axis=0, keepdims=True)

            groups = ls_ref.shape[1]
            group = (lax.div(iota((groups, sb), 1), states) + b * GATHER
                     == iota((groups, sb), 0)).astype(F32)
            step_size = jnp.exp(jnp.dot(ls_ref[...], group, precision=exact,
                                        preferred_element_type=F32))
            re, im = lanes(dr_ref), lanes(di_ref)
            magnitude = jnp.exp(re * step_size)
            angle = im * step_size
            power_re = magnitude * jnp.cos(angle)
            power_im = magnitude * jnp.sin(angle)
            denom = re * re + im * im
            a_ref[b, 0:1, :] = power_re
            a_ref[b, 1:2, :] = power_im
            ratio[b, 0:1, :] = ((power_re - 1.0) * re + power_im * im) / denom
            ratio[b, 1:2, :] = (power_im * re - (power_re - 1.0) * im) / denom
    with jax.named_scope("A_x"):
        square = (rows, rows)
        source = lax.rem(iota(square, 0), span) * CHUNKS + lax.div(iota(square, 0), span)
        turn[...] = (iota(square, 1) == source).astype(BF16)
        loads[5].wait()
        for b in range(blocks):
            x_ref[b] = lax.dot_general(
                turn[...], x_raw[:, b * cb:(b + 1) * cb], (((0,), (0,)), ((), ())),
                preferred_element_type=F32,
            ).astype(BF16)
    with jax.named_scope("A_barrier"):
        pl.semaphore_wait(barrier, n)
    loads[10].wait()

    def send_inner(w, s):
        @pl.when(inner)
        def _():
            send_b(w, s)

    send_x(0, 1)
    send_z(0, 0)
    send_y(0, 0)
    send_inner(0, 0)
    send_c(0, 0, 1)
    with jax.named_scope("A_flip1"):
        loads[1].wait()
        flip_weights(1)
        for copy in loads[6:10]:
            copy.wait()

    local = []
    for w in range(3):
        copy = pltpu.make_async_copy(own(w), spot(w, 0), local_sem.at[w])
        copy.start()
        local.append(copy)

    def scan(b, start, keep):
        work[...] = jnp.dot(x_ref[b], read_in[b], preferred_element_type=F32)
        br = jnp.broadcast_to(a_ref[b, 0:1, :], (CHUNKS, sb))
        bi = jnp.broadcast_to(a_ref[b, 1:2, :], (CHUNKS, sb))

        def step(i, state):
            at = pl.ds(pl.multiple_of(i * CHUNKS, CHUNKS), CHUNKS)
            nr, ni = cmul(br, bi, *state)
            nr, ni = nr + work[at, :sb], ni + work[at, sb:]
            if keep:
                work[at, :sb] = nr
                work[at, sb:] = ni
            return nr, ni

        return lax.fori_loop(0, span, step, start, unroll=8)

    size = cb // GATHER
    spread_narrow = spread.astype(BF16)
    with jax.named_scope("B_scan1"):
        @pl.loop(0, blocks)
        def _(b):
            keep = lax.div(iota((cb, sb), 0), size) == lax.div(iota((cb, sb), 1), states)
            at = pl.ds(pl.multiple_of(b * cb, cb), cb)
            def widen(ref):
                high = ref[at, :].astype(BF16)
                low = (ref[at, :] - high.astype(F32)).astype(BF16)
                return (jnp.dot(high, spread_narrow, preferred_element_type=F32)
                        + jnp.dot(low, spread_narrow, preferred_element_type=F32))

            vr, vi = widen(inr_ref), widen(ini_ref)
            cr, ci = ratio[b, 0:1, :], ratio[b, 1:2, :]
            read_in[b, :, :sb] = jnp.where(keep, cr * vr - ci * vi, 0.0).astype(BF16)
            read_in[b, :, sb:] = jnp.where(keep, cr * vi + ci * vr, 0.0).astype(BF16)
            zero = jnp.zeros((CHUNKS, sb), F32)
            sr, si = scan(b, (zero, zero), False)
            ends[b, :, :sb] = sr
            ends[b, :, sb:] = si
            lr, li = cpow(a_ref[b, 0:1, :], a_ref[b, 1:2, :], span)
            er, ei = sr[0:1], si[0:1]
            for chunk in range(1, CHUNKS):
                er, ei = cmul(lr, li, er, ei)
                er, ei = er + sr[chunk:chunk + 1], ei + si[chunk:chunk + 1]
            total[b, :, :sb] = er
            total[b, :, sb:] = ei

    here = m * 2 + v
    level = h * 2 + u
    for k, there in enumerate((to_x, to_y, (h, u, om, ov, core))):
        send(total, gathered.at[here], there, ("s", k))
    gathered[here] = total[...]
    send_x(0, 0)
    for w in (1, 2):
        for s in (1, 0):
            send_x(w, s)
    send_y(1, 0)
    send_y(2, 0)
    with jax.named_scope("C_readout"):
        @pl.loop(0, blocks)
        def _(b):
            high = (lax.rem(iota((sb, states), 0), states) == iota((sb, states), 1)).astype(BF16)
            keep = lax.div(iota((sb, cb), 0), states) == lax.div(iota((sb, cb), 1), size)
            at = pl.ds(pl.multiple_of(b * cb, cb), cb)
            for place_in, ref, sign in ((0, outr_ref, 1.0), (1, outi_ref, -1.0)):
                wide = lax.dot_general(high, (sign * ref[at, :]).astype(BF16), across,
                                       preferred_element_type=F32)
                read_out[b, place_in * sb:(place_in + 1) * sb, :] = jnp.where(
                    keep, wide, 0.0).astype(BF16)

    with jax.named_scope("C_states1"):
        for k, (a, b) in enumerate(((m, ov), (om, v), (om, ov))):
            arrive(gathered.at[a * 2 + b], to_x, ("s", k))

    def power_of(b, count):
        return cpow(a_ref[b, 0:1, :], a_ref[b, 1:2, :], count)

    @pl.loop(0, blocks)
    def _(b):
        tr, ti = power_of(b, span * CHUNKS)
        hr = jnp.zeros((1, sb), F32)
        hi, pr, pi = hr, hr, hr
        for device in range(4):
            gr, gi = gathered[device, b, :, :sb], gathered[device, b, :, sb:]
            nr, ni = cmul(tr, ti, hr, hi)
            hr = jnp.where(device < here, nr + gr, hr)
            hi = jnp.where(device < here, ni + gi, hi)
            nr, ni = cmul(tr, ti, pr, pi)
            pr, pi = nr + gr, ni + gi
        prefix[b, :, :sb] = hr
        prefix[b, :, sb:] = hi
        plane_total[b, :, :sb] = pr
        plane_total[b, :, sb:] = pi

    for k, (a, b) in enumerate(((h, ou), (oh, u), (oh, ou))):
        send(plane_total, planes.at[level], (a, b, m, v, core), ("plane", k))
    planes[level] = plane_total[...]
    with jax.named_scope("C_x01"):
        wait_x(0, 1)
    send_z(0, 1)
    send_inner(0, 1)
    send_c(0, 0, 0)
    for copy in loads[11:]:
        copy.wait()
    with jax.named_scope("C_states2"):
        for k, (a, b) in enumerate(((h, ou), (oh, u), (oh, ou))):
            arrive(planes.at[a * 2 + b], to_x, ("plane", k))
    with jax.named_scope("C_x00"):
        wait_x(0, 0)
    send_c(0, 1, 0)
    send_c(0, 1, 1)
    send_y(0, 1)

    def second(b):
        lr, li = power_of(b, span)
        tr, ti = cpow(lr, li, CHUNKS)
        qr, qi = cpow(tr, ti, 4)
        hr = jnp.zeros((1, sb), F32)
        hi = hr
        for other in range(3):
            nr, ni = cmul(qr, qi, hr, hi)
            hr = jnp.where(other < level, nr + planes[other, b, :, :sb], hr)
            hi = jnp.where(other < level, ni + planes[other, b, :, sb:], hi)
        for device in range(3):
            nr, ni = cmul(tr, ti, hr, hi)
            hr, hi = jnp.where(device < here, nr, hr), jnp.where(device < here, ni, hi)
        hr, hi = hr + prefix[b, :, :sb], hi + prefix[b, :, sb:]
        starts_r, starts_i = [hr], [hi]
        for chunk in range(CHUNKS - 1):
            nr, ni = cmul(lr, li, hr, hi)
            hr = nr + ends[b, chunk:chunk + 1, :sb]
            hi = ni + ends[b, chunk:chunk + 1, sb:]
            starts_r.append(hr)
            starts_i.append(hi)
        scan(b, (jnp.concatenate(starts_r, axis=0), jnp.concatenate(starts_i, axis=0)), True)
        mixed = jnp.dot(work[...].astype(BF16), read_out[b], preferred_element_type=F32)
        at = pl.ds(pl.multiple_of(b * cb, cb), cb)
        mixed = mixed + k_ref[:, at] * x_ref[b].astype(F32)
        mixed = jax.nn.gelu(mixed).astype(BF16)
        act[:, at] = jnp.dot(
            turn[...], mixed, preferred_element_type=F32
        ).astype(BF16)

    def pass_z(w, s):
        with jax.named_scope(f"z{w}{s}"):
            wait_z(w, s)

        @pl.when(inner)
        def _():
            relay(w, s)

        send_y(w, 2 + s)

    def pass_e(w, s):
        with jax.named_scope(f"e{w}{s}"):
            wait_e(w, s)
        send_y(w, 4 + s)

    def pass_l(w, s):
        with jax.named_scope(f"l{w}{s}"):
            wait_l(w, s)
        send_y(w, 6 + s)

    with jax.named_scope("D_scan2a"):
        @pl.loop(0, blocks // 2)
        def _(b):
            second(b)

    pass_z(0, 0)
    send_z(1, 0)
    send_inner(1, 0)
    with jax.named_scope("D_scan2b"):
        @pl.loop(blocks // 2, blocks)
        def _(b):
            second(b)

    pass_z(0, 1)
    with jax.named_scope("D_x11"):
        wait_x(1, 1)
    send_z(1, 1)
    send_inner(1, 1)
    with jax.named_scope("D_x10"):
        wait_x(1, 0)
    send_y(1, 1)

    tile = min(512, width)
    with jax.named_scope("E_outproj"):
        for t in (1, 0):
            to = core if t == 0 else 1 - core

            @pl.loop(0, width // tile)
            def _(j):
                at = pl.ds(pl.multiple_of(j * tile, tile), tile)
                share[t, :, at] = jnp.dot(
                    act[pl.ds(pl.multiple_of(to * keep_rows, keep_rows), keep_rows), :],
                    wo_ref[:, at], preferred_element_type=F32,
                ).astype(BF16)

            if t:
                send(share.at[1], others, to_t, ("mix",))

    with jax.named_scope("G_mix"):
        arrive(others, to_t, ("mix",))
    line = min(32, keep_rows)
    with jax.named_scope("H_norm"):
        @pl.loop(0, keep_rows // line)
        def _(i):
            at = pl.ds(pl.multiple_of(i * line, line), line)
            mixed = share[0, at, :].astype(F32) + others[at, :].astype(F32)
            carried = res_ref[at, :].astype(F32) + mixed.astype(BF16).astype(F32)
            scale = lax.rsqrt(jnp.mean(carried * carried, axis=-1, keepdims=True) + 1e-06)
            carried_ref[at, :] = carried
            rows_ref[0, 0, at, :] = (carried * scale * gain_ref[...]).astype(BF16)

    send(rows_ref.at[0, 0], rows_ref.at[0, 1], to_x, ("r", 1), moves)
    piece = keep_rows // PIECES
    for part in range(PIECES):
        at = pl.ds(part * piece, piece)
        send(rows_ref.at[0, 0, at], rows_ref.at[0, 2, at], to_z, ("r", 2, part), moves)
    send(rows_ref.at[0, 0], rows_ref.at[1, 0], to_t, ("t", 0), moves)

    def share_core(k):
        send(rows_ref.at[0, k], rows_ref.at[1, k], to_t, ("t", k), moves)

    def wait_core(k):
        arrive(rows_ref.at[1, k], to_t, ("t", k))

    def product(k, w):
        block = rows_ref[:, k].reshape(2 * keep_rows, width)
        return lax.dot_general(block, weights[w][...], across, preferred_element_type=F32)

    def gate_part(k):
        with jax.named_scope(f"gate{k}"):
            gates[k] = product(k, 0)

    def up_part(k):
        with jax.named_scope(f"up{k}"):
            result = (jax.nn.silu(gates[k]) * product(k, 1)).astype(BF16)
            for t in range(2):
                hidden[pl.ds((4 * t + k) * keep_rows, keep_rows), :] = (
                    result[t * keep_rows:(t + 1) * keep_rows])

    def first_rows():
        with jax.named_scope("r1"):
            arrive(rows_ref.at[0, 1], to_x, ("r", 1))
        share_core(1)

    def relay_rows(part):
        at = pl.ds(part * piece, piece)
        with jax.named_scope(f"r2{part}"):
            arrive(rows_ref.at[0, 2, at], to_z, ("r", 2, part))
        send(rows_ref.at[0, 2, at], rows_ref.at[0, 3, at], to_x, ("r", 3, part), moves)
        if part == PIECES - 1:
            share_core(2)

    def last_rows():
        with jax.named_scope("r3"):
            for part in range(PIECES):
                at = pl.ds(part * piece, piece)
                arrive(rows_ref.at[0, 3, at], to_x, ("r", 3, part))
        share_core(3)

    def second_weights():
        send_inner(2, 0)
        wait_x(2, 1)
        send_inner(2, 1)
        send_z(2, 0)
        send_z(2, 1)
        wait_x(2, 0)
        send_y(2, 1)
        send_c(2, 0, 0)
        send_c(2, 1, 0)

    def delayed_weights():
        send_c(2, 0, 1)
        send_c(2, 1, 1)

    def whole(w):
        with jax.named_scope(f"y{w}"):
            for j in range(8):
                wait_y(w, j)

    def core_rows(k):
        with jax.named_scope(f"t{k}"):
            wait_core(k)

    for s in range(2):
        send_c(1, s, 1)
        send_c(1, s, 0)
    pass_e(0, 0)
    pass_e(0, 1)
    pass_z(1, 0)
    pass_z(1, 1)
    pass_l(0, 0)
    pass_l(0, 1)
    pass_e(1, 0)
    for copy in local:
        copy.wait()
    whole(0)
    core_rows(0)
    gate_part(0)
    first_rows()
    second_weights()
    relay_rows(0)
    pass_e(1, 1)
    relay_rows(1)
    core_rows(1)
    gate_part(1)
    pass_l(1, 0)
    pass_l(1, 1)
    delayed_weights()
    relay_rows(2)
    whole(1)
    up_part(0)
    relay_rows(3)
    up_part(1)
    core_rows(2)
    gate_part(2)
    pass_z(2, 0)
    last_rows()
    up_part(2)
    core_rows(3)
    gate_part(3)
    up_part(3)
    pass_e(2, 0)
    with jax.named_scope("moves"):
        for copy in moves:
            copy.wait_send()

    across_u = width // 8
    chunks = [(h, h, m), (h, oh, m), (oh, h, m), (h, h, om), (h, oh, om), (oh, oh, m),
              (oh, h, om), (oh, oh, om)]

    def columns(j):
        a, b, c = chunks[j]
        return pl.ds(pl.multiple_of(index(a, b, c, 0) * depth, across_u), across_u)

    def down(j):
        at = columns(j)
        for t in (1, 0):
            result = jnp.dot(
                hidden[4 * t * keep_rows:4 * (t + 1) * keep_rows, :], weights[2][:, at],
                preferred_element_type=F32,
            ).astype(BF16)
            for k in range(4):
                rows_ref[t, k, :, at] = result[k * keep_rows:(k + 1) * keep_rows]
            if t:
                send(rows_ref.at[1, :, :, at], partners.at[j], to_t, ("p", j))

    def add(target, j, other):
        at = columns(j)

        @pl.loop(0, keep_rows // line)
        def _(i):
            lines = pl.ds(pl.multiple_of(i * line, line), line)
            rows_ref[0, target, lines, at] = (
                rows_ref[0, target, lines, at].astype(F32) + other[lines, :].astype(F32)
            ).astype(BF16)

    def pair(j):
        at = columns(j)
        near, far = (1, 2) if X_FIRST[j] else (2, 1)
        device = to_x if X_FIRST[j] else to_z
        arrive(partners.at[j], to_t, ("p", j))
        for place_in, k in enumerate((3, near)):
            add(k, j, partners.at[j, k])
            send(rows_ref.at[0, k, :, at], firsts.at[j, place_in], device, ("f", j, place_in))
        add(far, j, partners.at[j, far])
        add(0, j, partners.at[j, 0])

    def combine(j):
        at = columns(j)
        far = 2 if X_FIRST[j] else 1
        device, other = (to_x, to_z) if X_FIRST[j] else (to_z, to_x)
        arrive(firsts.at[j, 0], device, ("f", j, 0))
        add(far, j, firsts.at[j, 0])
        send(rows_ref.at[0, far, :, at], seconds.at[j], other, ("g", j))
        arrive(firsts.at[j, 1], device, ("f", j, 1))
        add(0, j, firsts.at[j, 1])

    def finish(j):
        at = columns(j)
        arrive(seconds.at[j], to_z if X_FIRST[j] else to_x, ("g", j))

        @pl.loop(0, keep_rows // line)
        def _(i):
            lines = pl.ds(pl.multiple_of(i * line, line), line)
            summed = rows_ref[0, 0, lines, at].astype(F32) + seconds[j, lines, :].astype(F32)
            summed = summed.astype(BF16).astype(F32)
            out_ref[lines, at] = (carried_ref[lines, at] + 0.5 * summed).astype(BF16)

    order = ("d0", "z", "p0", "d1", "e", "d2", "p1", "d3", "p2", "c0", "d4", "p3", "c1", "l", "d5",
             "p4", "c2", "f0", "d6", "p5", "c3", "f1", "d7", "p6", "c4", "f2", "p7", "c5", "f3",
             "c6", "f4", "c7", "f5", "f6", "f7")
    relayed, passed = next(counter), next(counter)
    inside.append((("l", 2, 1), relayed))
    everywhere.append(describe(extra.at[0], extra.at[0], to_y, ("y", 2, 3), passed))

    def late_z(kind):
        @pl.when(is_inner == kind)
        def _():
            wait_z(2, 1)
            if kind:
                describe(spot(2, 3), spot(2, 3), to_c, ("l", 2, 1), relayed).start()
            describe(spot(2, 3), spot(2, 3), to_y, ("y", 2, 3), passed).start()

    with jax.named_scope("z21"):
        late_z(1)
    stages = {"d": down, "p": pair, "c": combine, "f": finish}
    for word in order:
        if word == "z":
            late_z(0)
            continue
        if word == "e":
            pass_e(2, 1)
            continue
        if word == "l":
            pass_l(2, 0)
            pass_l(2, 1)
            continue
        j = int(word[1])
        if word in ("d3", "d6", "d7"):
            with jax.named_scope("y2" + word):
                for i in {"d3": (0, 1, 2, 3), "d6": (4, 5), "d7": (6, 7)}[word]:
                    wait_y(2, i)
        with jax.named_scope({"d": "down", "p": "pair", "c": "comb", "f": "fin"}[word[0]] + word[1]):
            stages[word[0]](j)
    for copy in everywhere:
        copy.wait_send()

    @pl.when(inner)
    def _():
        for name, number in inside:
            describe(extra.at[0], extra.at[0], to_c, name, number).wait_send()


def shift(value, axis, count, by):
    return lax.ppermute(value, axis, [(i, (i + by) % count) for i in range(count)])


def flip(value, axes, count, k):
    return lax.ppermute(value, axes, [(i, i ^ k) for i in range(count)])


def on_device(sizes, mixer_in, residual, decay_real, decay_imag, log_step, in_real, in_imag,
              output_real, output_imaginary, skip, out_proj, norm_gain, w_gate, w_up, w_down):
    tp, nh, nm = sizes["tp"], sizes["h"], sizes["m"]
    n = nh * 4 * nm
    rows, channels = mixer_in.shape
    keep_rows, width = residual.shape
    depth, hidden_units = w_gate.shape
    part = hidden_units // 4
    groups, states = decay_real.shape
    blocks = groups // GATHER
    cb, sb = channels // blocks, GATHER * states
    vmem = pl.BlockSpec(memory_space=pltpu.VMEM)
    if depth % 128 == 0 and (tp, nh, nm) == (2, 2, 2):
        cut = width // 8
        return pl.pallas_call(
            functools.partial(streamed, sizes),
            in_specs=[pl.BlockSpec(memory_space=pl.ANY)] * 15,
            out_specs=vmem,
            out_shape=jax.ShapeDtypeStruct((keep_rows, width), BF16),
            scratch_shapes=[
                *[pltpu.VMEM((part, n * depth), BF16)] * 3,
                pltpu.VMEM((3, part, depth), BF16),
                pltpu.VMEM((2, 4, keep_rows, width), BF16),
                pltpu.VMEM((keep_rows, width), F32),
                pltpu.VMEM((4, 2 * keep_rows, part), F32),
                pltpu.VMEM((8 * keep_rows, part), BF16),
                pltpu.VMEM((8, 4, keep_rows, cut), BF16),
                pltpu.VMEM((8, 2, keep_rows, cut), BF16),
                pltpu.VMEM((8, keep_rows, cut), BF16),
                pltpu.VMEM((rows, 2 * sb), F32),
                pltpu.VMEM((blocks, cb, 2 * sb), BF16),
                pltpu.VMEM((blocks, 2 * sb, cb), BF16),
                pltpu.VMEM((blocks, CHUNKS, 2 * sb), F32),
                pltpu.VMEM((blocks, 1, 2 * sb), F32),
                pltpu.VMEM((4, blocks, 1, 2 * sb), F32),
                pltpu.VMEM((blocks, 1, 2 * sb), F32),
                pltpu.VMEM((blocks, 1, 2 * sb), F32),
                pltpu.VMEM((4, blocks, 1, 2 * sb), F32),
                pltpu.VMEM((rows, rows), BF16),
                pltpu.VMEM((rows, channels), BF16),
                pltpu.VMEM((2, keep_rows, width), BF16),
                pltpu.VMEM((keep_rows, width), BF16),
                pltpu.VMEM((rows, channels), BF16),
                pltpu.VMEM((blocks, rows, cb), BF16),
                pltpu.VMEM((keep_rows, width), BF16),
                *[pltpu.VMEM((groups, states), F32)] * 2,
                pltpu.VMEM((1, groups), F32),
                *[pltpu.VMEM((channels, states), F32)] * 4,
                pltpu.VMEM((1, channels), F32),
                pltpu.VMEM((channels, width), BF16),
                pltpu.VMEM((1, width), F32),
                pltpu.VMEM((2, depth, hidden_units), BF16),
                pltpu.VMEM((2, hidden_units, depth), BF16),
                pltpu.VMEM((hidden_units, depth), BF16),
                pltpu.VMEM((blocks, 2, sb), F32),
                pltpu.VMEM((blocks, 2, sb), F32),
                pltpu.SemaphoreType.DMA((160,)),
                pltpu.SemaphoreType.DMA((160,)),
                pltpu.SemaphoreType.DMA((3,)),
                pltpu.SemaphoreType.DMA((15,)),
            ],
            compiler_params=pltpu.CompilerParams(
                collective_id=0, has_side_effects=True, vmem_limit_bytes=62 * 2**20
            ),
            name="streamed",
        )(mixer_in, residual, decay_real, decay_imag, log_step.reshape(1, groups),
          in_real.transpose(0, 2, 1).reshape(channels, states),
          in_imag.transpose(0, 2, 1).reshape(channels, states),
          output_real.reshape(channels, states), output_imaginary.reshape(channels, states),
          skip.reshape(1, channels), out_proj, norm_gain.reshape(1, width), w_gate, w_up, w_down)
    power_re, power_im, bar_re, bar_im = discrete(
        decay_real, decay_imag, log_step, in_real, in_imag
    )
    rows_first = lambda t: jnp.transpose(t, (0, 2, 1)).reshape(blocks, -1, t.shape[1])
    read_in = jnp.stack([rows_first(bar_re), rows_first(bar_im)], axis=1).astype(BF16)
    read_out = jnp.stack(
        [rows_first(output_real), -rows_first(output_imaginary)], axis=1
    ).astype(BF16)
    power = jnp.stack([power_re.reshape(blocks, sb), power_im.reshape(blocks, sb)], axis=1)
    x = mixer_in.reshape(CHUNKS, rows // CHUNKS, blocks, cb).transpose(2, 1, 0, 3)
    x = x.reshape(blocks, rows, cb)
    operands = (x, read_in, read_out, power, skip.reshape(blocks, 1, cb), out_proj, residual,
                norm_gain.reshape(1, width), w_gate.T.reshape(4, part, depth),
                w_up.T.reshape(4, part, depth), w_down.reshape(4, part, depth))
    copies = 3 * (3 + 4 * (nh - 1) + 4 * nh * (nm - 1)) + (n - 1) + (tp - 1) + 3 + 4 * (tp - 1)
    laid = (part, n * depth) if depth % 128 == 0 else (n, part, depth)
    between = [(laid, BF16)] * 3 + [
        ((tp, 4, keep_rows, width), BF16), ((keep_rows, width), F32),
    ]
    fused = depth % 128 == 0
    if fused:
        copies += 4 * (tp - 1) + 3
        out_shape = [jax.ShapeDtypeStruct((keep_rows, width), BF16)]
        extra = [
            pltpu.VMEM((4 * tp, keep_rows, part), BF16),
            pltpu.VMEM((4, tp - 1, keep_rows, width), BF16),
            pltpu.VMEM((3, keep_rows, width), BF16),
            *(pltpu.VMEM(*item) for item in between),
        ]
    else:
        out_shape = [jax.ShapeDtypeStruct(*item) for item in between]
        extra = []
    results = pl.pallas_call(
        functools.partial(layer, sizes, fused),
        in_specs=[vmem] * 11,
        out_specs=[vmem] * len(out_shape),
        out_shape=out_shape,
        scratch_shapes=[
            *extra,
            pltpu.VMEM((rows, 2 * sb), F32),
            pltpu.VMEM((blocks, cb, 2 * sb), BF16),
            pltpu.VMEM((blocks, 2 * sb, cb), BF16),
            pltpu.VMEM((blocks, CHUNKS, 2 * sb), F32),
            pltpu.VMEM((blocks, 1, 2 * sb), F32),
            pltpu.VMEM((n, blocks, 1, 2 * sb), F32),
            pltpu.VMEM((rows, channels), BF16),
            pltpu.VMEM((tp, keep_rows, width), BF16),
            pltpu.VMEM((tp - 1, keep_rows, width), BF16),
            pltpu.SemaphoreType.DMA((copies,)),
            pltpu.SemaphoreType.DMA((copies,)),
            pltpu.SemaphoreType.DMA((3,)),
        ],
        compiler_params=pltpu.CompilerParams(
            collective_id=0, has_side_effects=True, vmem_limit_bytes=62 * 2**20
        ),
        name="layer",
    )(*operands)
    if fused:
        return results[0]
    full_gate, full_up, full_down, rows_all, carried = results
    if len(laid) == 3:
        full_gate, full_up, full_down = (
            t.transpose(1, 0, 2).reshape(part, width) for t in (full_gate, full_up, full_down)
        )

    flat = rows_all.reshape(-1, width)
    across = (((1,), (1,)), ((), ()))
    gate = lax.dot_general(flat, full_gate, across, preferred_element_type=F32)
    up = lax.dot_general(flat, full_up, across, preferred_element_type=F32)
    hidden = (jax.nn.silu(gate) * up).astype(BF16)
    down = jnp.dot(hidden, full_down, preferred_element_type=F32).astype(BF16)
    down = down.reshape(rows_all.shape)
    summed = down[0].astype(F32)
    for t in range(1, tp):
        summed = summed + shift(down[t], "tp", tp, -t).astype(F32)
    summed = summed.astype(BF16)
    total = summed[0].astype(F32)
    for k in range(1, 4):
        total = total + flip(summed[k], PEERS, 4, k).astype(F32)
    total = total.astype(BF16)
    return (carried + 0.5 * total.astype(F32)).astype(BF16)


def solution(mesh):
    sp, tp = mesh.shape["sp"], mesh.shape["tp"]
    sizes = {"h": sp // 8, "u": 2, "m": 2, "v": 2, "tp": tp}
    cut = Mesh(mesh.devices.reshape(tuple(sizes.values())), tuple(sizes))
    return jax.shard_map(
        functools.partial(on_device, sizes),
        mesh=cut,
        in_specs=(
            P(SP, "tp"),
            P((*SP, "tp"), None),
            P("tp", None),
            P("tp", None),
            P("tp"),
            P("tp", None, None),
            P("tp", None, None),
            P("tp", None, None),
            P("tp", None, None),
            P("tp"),
            P("tp", None),
            P(),
            P(SP, "tp"),
            P(SP, "tp"),
            P("tp", SP),
        ),
        out_specs=P((*SP, "tp"), None),
        check_vma=False,
    )
```

```python
import functools

import jax
import jax.numpy as jnp
from jax import lax
from jax.experimental import pallas as pl
from jax.experimental.pallas import tpu as pltpu
from jax.sharding import Mesh
from jax.sharding import PartitionSpec as P

F32 = jnp.float32
BF16 = jnp.bfloat16
SP = ("h", "u", "m", "v")
PEERS = ("u", "v")
GATHER = 8
CHUNKS = 8
X_FIRST = (1, 1, 1, 0, 1, 0, 1, 0)
PIECES = 4
ORDER = ("d0", "e", "p0", "p1", "d1", "p2", "p3", "l", "d2", "p4", "p5", "c0", "d3", "p6", "p7",
         "c1", "c2", "c3", "c4", "c5", "f0", "f1", "c6", "c7", "f2", "f3", "f4", "f5", "f6", "f7")
MESH = pl.DeviceIdType.MESH


def discrete(decay_real, decay_imag, log_step, in_real, in_imag):
    step_size = jnp.exp(log_step)[:, None]
    magnitude = jnp.exp(decay_real * step_size)
    angle = decay_imag * step_size
    power_re = magnitude * jnp.cos(angle)
    power_im = magnitude * jnp.sin(angle)
    denom = decay_real * decay_real + decay_imag * decay_imag
    ratio_re = ((power_re - 1.0) * decay_real + power_im * decay_imag) / denom
    ratio_im = (power_im * decay_real - (power_re - 1.0) * decay_imag) / denom
    drive_re = ratio_re[..., None] * in_real - ratio_im[..., None] * in_imag
    drive_im = ratio_re[..., None] * in_imag + ratio_im[..., None] * in_real
    return (power_re, power_im, drive_re, drive_im)


def cmul(ar, ai, br, bi):
    return ar * br - ai * bi, ar * bi + ai * br


def cpow(ar, ai, count):
    result = None
    while count:
        if count & 1:
            result = (ar, ai) if result is None else cmul(*result, ar, ai)
        count >>= 1
        if count:
            ar, ai = cmul(ar, ai, ar, ai)
    return result


def iota(shape, dim):
    return lax.broadcasted_iota(jnp.int32, shape, dim)


def tiled(block, copies, across, down):
    rows, columns = block.shape
    wide = (columns, columns * copies)
    pick = (iota(wide, 0) == lax.rem(iota(wide, 1), columns)).astype(BF16)
    full = jnp.dot(block, pick, preferred_element_type=F32)
    keep = lax.div(iota(full.shape, 0), down) == lax.div(iota(full.shape, 1), across)
    return jnp.where(keep, full, 0.0).astype(BF16)


def layer(sizes, fused, x_ref, b_ref, c_ref, a_ref, k_ref, wo_ref, res_ref, gain_ref, *rest):
    quarters, rest = rest[:3], rest[3:]
    if fused:
        out_ref, *rest = rest
        hidden, partners, peers, *rest = rest
    weights, (rows_ref, carried_ref), rest = rest[:3], rest[3:5], rest[5:]
    (work, read_in, read_out, ends, total, gathered, act, share, others,
     send_sem, recv_sem, local_sem) = rest
    blocks, rows, cb = x_ref.shape
    sb = a_ref.shape[2]
    depth = quarters[0].shape[2]
    width = wo_ref.shape[1]
    span = rows // CHUNKS
    nh, nm, tp = sizes["h"], sizes["m"], sizes["tp"]
    n = nh * 4 * nm
    h, u, m, v, core = (lax.axis_index(name) for name in (*SP, "tp"))
    index = lambda h, u, m, v: ((h * 2 + u) * nm + m) * 2 + v
    me = index(h, u, m, v)
    peer = lambda k: (1 - u if k & 2 else u, 1 - v if k & 1 else v)
    counter = iter(range(send_sem.shape[0]))

    def send(src, dst, device):
        slot = next(counter)
        copy = pltpu.make_async_remote_copy(
            src_ref=src, dst_ref=dst, send_sem=send_sem.at[slot], recv_sem=recv_sem.at[slot],
            device_id=device, device_id_type=MESH,
        )
        copy.start()
        return copy

    def place(ref, position):
        if depth % 128:
            return ref.at[position]
        return ref.at[:, pl.ds(pl.multiple_of(position * depth, depth), depth)]

    barrier = pltpu.get_barrier_semaphore()
    others_sp = []
    for k in range(1, n):
        to = lax.rem(me + k, n)
        there = (lax.div(to, 4 * nm), lax.rem(lax.div(to, 2 * nm), 2),
                 lax.rem(lax.div(to, 2), nm), lax.rem(to, 2), core)
        others_sp.append(there)
        pl.semaphore_signal(barrier, inc=1, device_id=there, device_id_type=MESH)
    for t in range(1, tp):
        pl.semaphore_signal(
            barrier, inc=1, device_id=(h, u, m, v, lax.rem(core + t, tp)), device_id_type=MESH
        )
    pl.semaphore_wait(barrier, n - 1 + tp - 1)

    sent = []
    first = {}
    over_h = {}
    over_m = {}

    def spread_h(w, k, src, position):
        for r in range(1, nh):
            pu, pv = peer(k)
            copy = send(src, place(weights[w], position), (lax.rem(h + r, nh), u, m, v, core))
            over_h[w, k, r] = copy

    def spread_m(w, k, r, src, position):
        for s in range(1, nm):
            over_m[w, k, r, s] = send(
                src, place(weights[w], position), (h, u, lax.rem(m + s, nm), v, core)
            )

    own = u * 2 + v
    for w in range(3):
        for k in (3, 1, 2):
            pu, pv = peer(k)
            first[w, k] = send(
                quarters[w].at[pu * 2 + pv], place(weights[w], me), (h, pu, m, pv, core)
            )
    locals_ = []
    for w in range(3):
        spread_h(w, 0, quarters[w].at[own], me)
        spread_m(w, 0, 0, quarters[w].at[own], me)
        copy = pltpu.make_async_copy(quarters[w].at[own], place(weights[w], me), local_sem.at[w])
        copy.start()
        locals_.append(copy)

    def scan(b, start, keep):
        work[...] = jnp.dot(x_ref[b], read_in[b], preferred_element_type=F32)
        br = jnp.broadcast_to(a_ref[b, 0:1, :], (CHUNKS, sb))
        bi = jnp.broadcast_to(a_ref[b, 1:2, :], (CHUNKS, sb))

        def step(i, state):
            at = pl.ds(pl.multiple_of(i * CHUNKS, CHUNKS), CHUNKS)
            nr, ni = cmul(br, bi, *state)
            nr, ni = nr + work[at, :sb], ni + work[at, sb:]
            if keep:
                work[at, :sb] = nr
                work[at, sb:] = ni
            return nr, ni

        return lax.fori_loop(0, span, step, start, unroll=8)

    @pl.loop(0, blocks)
    def _(b):
        states = b_ref.shape[3]
        for half in range(2):
            read_in[b, :, half * sb:(half + 1) * sb] = tiled(
                b_ref[b, half], GATHER, states, cb // GATHER
            )
            read_out[b, half * sb:(half + 1) * sb, :] = tiled(
                c_ref[b, half], GATHER, cb // GATHER, states
            )
        zero = jnp.zeros((CHUNKS, sb), F32)
        sr, si = scan(b, (zero, zero), False)
        ends[b, :, :sb] = sr
        ends[b, :, sb:] = si
        lr, li = cpow(a_ref[b, 0:1, :], a_ref[b, 1:2, :], span)
        er, ei = sr[0:1], si[0:1]
        for chunk in range(1, CHUNKS):
            er, ei = cmul(lr, li, er, ei)
            er, ei = er + sr[chunk:chunk + 1], ei + si[chunk:chunk + 1]
        total[b, :, :sb] = er
        total[b, :, sb:] = ei

    states_out = [send(total, gathered.at[me], there) for there in others_sp]
    gathered[me] = total[...]
    for copy in states_out:
        copy.wait_recv()

    @pl.loop(0, blocks)
    def _(b):
        lr, li = cpow(a_ref[b, 0:1, :], a_ref[b, 1:2, :], span)
        tr, ti = cpow(lr, li, CHUNKS)
        hr = jnp.zeros((1, sb), F32)
        hi = hr
        for device in range(n - 1):
            nr, ni = cmul(tr, ti, hr, hi)
            nr = nr + gathered[device, b, :, :sb]
            ni = ni + gathered[device, b, :, sb:]
            hr, hi = jnp.where(device < me, nr, hr), jnp.where(device < me, ni, hi)
        starts_r, starts_i = [hr], [hi]
        for chunk in range(CHUNKS - 1):
            nr, ni = cmul(lr, li, hr, hi)
            hr = nr + ends[b, chunk:chunk + 1, :sb]
            hi = ni + ends[b, chunk:chunk + 1, sb:]
            starts_r.append(hr)
            starts_i.append(hi)
        scan(b, (jnp.concatenate(starts_r, axis=0), jnp.concatenate(starts_i, axis=0)), True)
        mixed = jnp.dot(work[...].astype(BF16), read_out[b], preferred_element_type=F32)
        mixed = mixed + k_ref[b] * x_ref[b].astype(F32)
        mixed = jax.nn.gelu(mixed).astype(BF16)
        square = (rows, rows)
        source = lax.rem(iota(square, 0), span) * CHUNKS + lax.div(iota(square, 0), span)
        turn = (iota(square, 1) == source).astype(BF16)
        act[:, pl.ds(pl.multiple_of(b * cb, cb), cb)] = jnp.dot(
            turn, mixed, preferred_element_type=F32
        ).astype(BF16)

    keep_rows = rows // tp
    tile = min(512, width)
    mixed_copies = []
    for t in (*range(1, tp), 0):
        to = lax.rem(core + t, tp)

        @pl.loop(0, width // tile)
        def _(j):
            at = pl.ds(pl.multiple_of(j * tile, tile), tile)
            share[t, :, at] = jnp.dot(
                act[pl.ds(pl.multiple_of(to * keep_rows, keep_rows), keep_rows), :],
                wo_ref[:, at], preferred_element_type=F32,
            ).astype(BF16)

        if t:
            mixed_copies.append(send(share.at[t], others.at[t - 1], (h, u, m, v, to)))

    for w in range(3):
        for k in (1, 2, 3):
            first[w, k].wait_recv()
            pu, pv = peer(k)
            position = index(h, pu, m, pv)
            spread_h(w, k, place(weights[w], position), position)
            spread_m(w, k, 0, place(weights[w], position), position)

    for copy in mixed_copies:
        copy.wait_recv()
    line = min(32, keep_rows)

    @pl.loop(0, keep_rows // line)
    def _(i):
        at = pl.ds(pl.multiple_of(i * line, line), line)
        mixed = share[0, at, :].astype(F32)
        for t in range(1, tp):
            mixed = mixed + others[t - 1, at, :].astype(F32)
        carried = res_ref[at, :].astype(F32) + mixed.astype(BF16).astype(F32)
        scale = lax.rsqrt(jnp.mean(carried * carried, axis=-1, keepdims=True) + 1e-06)
        carried_ref[at, :] = carried
        rows_ref[0, 0, at, :] = (carried * scale * gain_ref[...]).astype(BF16)

    row_copies = {}
    for k in (3, 1, 2):
        pu, pv = peer(k)
        row_copies[k] = send(rows_ref.at[0, 0], rows_ref.at[0, k], (h, pu, m, pv, core))
    last = []
    for t in range(1, tp):
        last.append(send(rows_ref.at[0, 0], rows_ref.at[t, 0], (h, u, m, v, lax.rem(core + t, tp))))

    def pass_m(w, k):
        pu, pv = peer(k)
        for r in range(1, nh):
            over_h[w, k, r].wait_recv()
            position = index(lax.rem(h - r + nh, nh), pu, m, pv)
            spread_m(w, k, r, place(weights[w], position), position)

    for w in range(3):
        for k in range(4):
            pass_m(w, k)
        if w == 1:
            for k in (1, 2, 3):
                row_copies[k].wait_recv()
                for t in range(1, tp):
                    last.append(send(
                        rows_ref.at[0, k], rows_ref.at[t, k], (h, u, m, v, lax.rem(core + t, tp))
                    ))
    sent = [*first.values(), *over_h.values(), *over_m.values(), *states_out, *mixed_copies]
    row_sends = [*row_copies.values(), *last]
    for (w, *_), copy in over_m.items():
        if w < 2 or not fused:
            copy.wait_recv()
    for copy in last:
        copy.wait_recv()
    for copy in locals_:
        copy.wait()
    if fused:
        sent += back(
            sizes, send, peer, (h, u, m, v, core), weights, rows_ref, carried_ref, out_ref,
            hidden, partners, peers, row_sends, [c for (w, *_), c in over_m.items() if w == 2],
        )
    else:
        sent += row_sends
    for copy in sent:
        copy.wait_send()


def back(sizes, send, peer, here, weights, rows_ref, carried_ref, out_ref, hidden, partners,
         peers, row_sends, down_copies):
    tp = sizes["tp"]
    h, u, m, v, core = here
    _, _, keep_rows, width = rows_ref.shape
    across = (((1,), (1,)), ((), ()))

    @pl.loop(0, 4 * tp)
    def _(i):
        t, k = lax.div(i, 4), lax.rem(i, 4)
        block = rows_ref[t, k]
        gate = lax.dot_general(block, weights[0][...], across, preferred_element_type=F32)
        up = lax.dot_general(block, weights[1][...], across, preferred_element_type=F32)
        hidden[i] = (jax.nn.silu(gate) * up).astype(BF16)

    for copy in (*down_copies,):
        copy.wait_recv()
    for copy in row_sends:
        copy.wait_send()

    tile = min(512, width)
    line = min(32, keep_rows)
    sent = []
    peer_copies = []
    from_core = {}

    def reduce(k):
        for copy in from_core[k]:
            copy.wait_recv()

        @pl.loop(0, keep_rows // line)
        def _(i):
            at = pl.ds(pl.multiple_of(i * line, line), line)
            total = rows_ref[0, k, at, :].astype(F32)
            for t in range(1, tp):
                total = total + partners[k, t - 1, at, :].astype(F32)
            rows_ref[0, k, at, :] = total.astype(BF16)

        if k:
            pu, pv = peer(k)
            peer_copies.append(send(rows_ref.at[0, k], peers.at[k - 1], (h, pu, m, pv, core)))

    order = (3, 1, 2, 0)
    for step, k in enumerate(order):
        from_core[k] = []
        for t in (*range(1, tp), 0):
            @pl.loop(0, width // tile)
            def _(j):
                at = pl.ds(pl.multiple_of(j * tile, tile), tile)
                rows_ref[t, k, :, at] = jnp.dot(
                    hidden[t * 4 + k], weights[2][:, at], preferred_element_type=F32
                ).astype(BF16)

            if t:
                from_core[k].append(send(
                    rows_ref.at[t, k], partners.at[k, t - 1],
                    (h, u, m, v, lax.rem(core + tp - t, tp)),
                ))
        reduce(k)
        sent += from_core[k]
    for copy in peer_copies:
        copy.wait_recv()

    @pl.loop(0, keep_rows // line)
    def _(i):
        at = pl.ds(pl.multiple_of(i * line, line), line)
        total = rows_ref[0, 0, at, :].astype(F32)
        for k in range(1, 4):
            total = total + peers[k - 1, at, :].astype(F32)
        total = total.astype(BF16).astype(F32)
        out_ref[at, :] = (carried_ref[at, :] + 0.5 * total).astype(BF16)

    return sent + peer_copies


def streamed(sizes, x_hbm, residual_hbm, decay_re, decay_im, log_step, in_re, in_im, out_re, out_im,
             skip_hbm, wo_hbm, gain_hbm, gate_hbm, up_hbm, down_hbm, out_hbm, *rest):
    (out_ref, out_sem, joined, down_full, extra, rows_ref, carried_ref, gates, hidden, partners, firsts, seconds, work, read_in,
     read_out, ends, total, gathered, prefix, plane_total, planes, turn, act, share, others,
     x_raw, x_ref, res_ref, dr_ref, di_ref, ls_ref, inr_ref, ini_ref, outr_ref, outi_ref, k_ref,
     wo_ref, gain_ref, raw, turned, down_ref, a_ref, ratio, send_sem, recv_sem, local_sem, load_sem) = rest
    blocks, rows, cb = x_ref.shape
    sb = a_ref.shape[2]
    slab, depth = down_full.shape[0], raw.shape[1]
    pitch = joined.shape[0] // 2
    width = wo_ref.shape[1]
    keep_rows = rows // 2
    span = rows // CHUNKS
    nh, nm = sizes["h"], sizes["m"]
    n = nh * 4 * nm
    h, u, m, v, core = (lax.axis_index(name) for name in (*SP, "tp"))
    oh, ou, om, ov = 1 - h, 1 - u, 1 - m, 1 - v
    index = lambda h, u, m, v: ((h * 2 + u) * nm + m) * 2 + v
    me = index(h, u, m, v)
    to_x, to_z, to_y = (h, u, m, ov, core), (h, ou, m, v, core), (h, u, om, v, core)
    to_c, to_b, to_t = (oh, u, m, v, core), (oh, ou, m, v, core), (h, u, m, v, 1 - core)
    plane = [(h, b, c) for b in (u, ou) for c in (v, ov)]
    plane += [(oh, b, c) for b in (h, oh) for c in (v, ov)]
    is_inner = lax.rem(h + u, 2)
    inner = is_inner == 1
    across = (((1,), (1,)), ((), ()))
    slots, everywhere, inside, moves = {}, [], [], []
    counter = iter(range(send_sem.shape[0]))

    def slot(name):
        return slots.setdefault(name, len(slots))

    def describe(src, dst, device, name, number):
        return pltpu.make_async_remote_copy(
            src_ref=src, dst_ref=dst, send_sem=send_sem.at[number],
            recv_sem=recv_sem.at[slot(name) if isinstance(name, tuple) else name], device_id=device, device_id_type=MESH,
        )

    def send(src, dst, device, name, kept=everywhere):
        number = next(counter)
        copy = describe(src, dst, device, name, number)
        copy.start()
        kept.append((name, number) if kept is inside else copy)

    def arrive(dst, device, name):
        describe(dst, dst, device, name, 0).wait_recv()

    def place(w, position):
        at = pl.ds(pl.multiple_of(position * depth, depth), depth)
        return down_full.at[:, at] if w == 2 else joined.at[pl.ds(w * pitch, slab), at]

    def spot(w, j, row=m):
        a, b, c = plane[j]
        return place(w, index(a, b, row, c))

    def mine(w, b, c):
        at = pl.ds(pl.multiple_of((b * 2 + c) * slab, slab), slab)
        return down_ref.at[at, :] if w == 2 else turned.at[w, at, :]

    def own(w):
        return mine(w, u, v)

    def send_x(w, s):
        if s:
            send(mine(w, ou, ov), extra.at[w], to_x, ("xo", w))
        else:
            send(mine(w, u, ov), spot(w, 0), to_x, ("xu", w))

    def send_z(w, s):
        send(extra.at[w] if s else mine(w, ou, v), spot(w, s), to_z, ("z", w, s))

    numbers = {}

    def send_c(w, s, kind):
        number = numbers.setdefault((w, s), None) or next(counter)
        if numbers[w, s] is None:
            numbers[w, s] = number
            everywhere.append(describe(extra.at[0], extra.at[0], to_c, ("e", w, s), number))
        name = ("e" if kind else "l", w, s)

        @pl.when(is_inner == kind)
        def _():
            describe(spot(w, 1) if s else own(w), spot(w, s), to_c, name, number).start()

    def send_b(w, s):
        send(extra.at[w] if s else mine(w, ou, v), spot(w, s), to_b, ("e", w, s), inside)

    def relay(w, s):
        send(spot(w, 2 + s), spot(w, 2 + s), to_c, ("l", w, s), inside)

    def send_y(w, j):
        send(own(w) if j == 0 else spot(w, j), spot(w, j), to_y, ("y", w, j))

    def wait_x(w, s):
        if s:
            arrive(extra.at[w], to_x, ("xo", w))
        else:
            arrive(spot(w, 1), to_x, ("xu", w))

    def wait_z(w, s):
        arrive(spot(w, 2 + s), to_z, ("z", w, s))

    def wait_e(w, s):
        arrive(spot(w, 4 + s), to_c, ("e", w, s))

    def wait_l(w, s):
        arrive(spot(w, 6 + s), to_c, ("l", w, s))

    def wait_y(w, j):
        arrive(spot(w, j, om), to_y, ("y", w, j))

    barrier = pltpu.get_barrier_semaphore()
    others_sp = []
    for k in range(1, n):
        to = lax.rem(me + k, n)
        there = (lax.div(to, 4 * nm), lax.rem(lax.div(to, 2 * nm), 2),
                 lax.rem(lax.div(to, 2), nm), lax.rem(to, 2), core)
        others_sp.append(there)
        pl.semaphore_signal(barrier, inc=1, device_id=there, device_id_type=MESH)
    pl.semaphore_signal(barrier, inc=1, device_id=to_t, device_id_type=MESH)
    pairs = ((gate_hbm, raw.at[0]), (up_hbm, raw.at[1]), (decay_re, dr_ref), (decay_im, di_ref),
             (log_step, ls_ref), (x_hbm, x_raw), (in_re, inr_ref), (in_im, ini_ref),
             (out_re, outr_ref), (out_im, outi_ref), (down_hbm, down_ref), (skip_hbm, k_ref),
             (wo_hbm, wo_ref), (residual_hbm, res_ref), (gain_hbm, gain_ref))
    loads = [pltpu.make_async_copy(a, b, load_sem.at[i]) for i, (a, b) in enumerate(pairs)]
    for copy in loads:
        copy.start()
    exact = lax.Precision.HIGHEST

    def flip_weights(w):
        for i in range(raw.shape[2] // depth):
            turned[w, i * depth:(i + 1) * depth, :] = raw[w, :, i * depth:(i + 1) * depth].T

    with jax.named_scope("A_flip"):
        loads[0].wait()
        flip_weights(0)
    with jax.named_scope("A_barrier"):
        pl.semaphore_wait(barrier, n)
    loads[10].wait()
    if pitch > slab:
        for w in range(2):
            joined[w * pitch + slab:(w + 1) * pitch, :] = jnp.zeros(
                (pitch - slab, joined.shape[1]), BF16)

    def send_inner(w, s):
        @pl.when(inner)
        def _():
            send_b(w, s)

    send_x(0, 1)
    send_z(0, 0)
    send_y(0, 0)
    send_inner(0, 0)
    send_c(0, 0, 1)
    with jax.named_scope("A_param"):
        for copy in loads[2:5]:
            copy.wait()
        states = sb // GATHER
        spread = (lax.rem(iota((states, sb), 1), states) == iota((states, sb), 0)).astype(F32)
        chosen = lax.div(iota((GATHER, sb), 1), states) == iota((GATHER, sb), 0)
        for b in range(blocks):
            def lanes(ref):
                wide = jnp.dot(ref[b * GATHER:(b + 1) * GATHER, :], spread, precision=exact,
                               preferred_element_type=F32)
                return jnp.sum(jnp.where(chosen, wide, 0.0), axis=0, keepdims=True)

            groups = ls_ref.shape[1]
            group = (lax.div(iota((groups, sb), 1), states) + b * GATHER
                     == iota((groups, sb), 0)).astype(F32)
            step_size = jnp.exp(jnp.dot(ls_ref[...], group, precision=exact,
                                        preferred_element_type=F32))
            re, im = lanes(dr_ref), lanes(di_ref)
            magnitude = jnp.exp(re * step_size)
            angle = im * step_size
            power_re = magnitude * jnp.cos(angle)
            power_im = magnitude * jnp.sin(angle)
            denom = re * re + im * im
            a_ref[b, 0:1, :] = power_re
            a_ref[b, 1:2, :] = power_im
            ratio[b, 0:1, :] = ((power_re - 1.0) * re + power_im * im) / denom
            ratio[b, 1:2, :] = (power_im * re - (power_re - 1.0) * im) / denom
    with jax.named_scope("A_x"):
        square = (rows, rows)
        source = lax.rem(iota(square, 0), span) * CHUNKS + lax.div(iota(square, 0), span)
        turn[...] = (iota(square, 1) == source).astype(BF16)
        loads[5].wait()
        for b in range(blocks):
            x_ref[b] = lax.dot_general(
                turn[...], x_raw[:, b * cb:(b + 1) * cb], (((0,), (0,)), ((), ())),
                preferred_element_type=F32,
            ).astype(BF16)
    with jax.named_scope("A_flip1"):
        loads[1].wait()
        flip_weights(1)
        for copy in loads[6:10]:
            copy.wait()

    local = []
    for w in range(3):
        copy = pltpu.make_async_copy(own(w), spot(w, 0), local_sem.at[w])
        copy.start()
        local.append(copy)

    def scan(b, start, keep):
        work[...] = jnp.dot(x_ref[b], read_in[b], preferred_element_type=F32)
        br = jnp.broadcast_to(a_ref[b, 0:1, :], (CHUNKS, sb))
        bi = jnp.broadcast_to(a_ref[b, 1:2, :], (CHUNKS, sb))

        def step(i, state):
            at = pl.ds(pl.multiple_of(i * CHUNKS, CHUNKS), CHUNKS)
            nr, ni = cmul(br, bi, *state)
            nr, ni = nr + work[at, :sb], ni + work[at, sb:]
            if keep:
                work[at, :sb] = nr
                work[at, sb:] = ni
            return nr, ni

        return lax.fori_loop(0, span, step, start, unroll=8)

    size = cb // GATHER
    spread_narrow = spread.astype(BF16)
    with jax.named_scope("B_scan1"):
        @pl.loop(0, blocks)
        def _(b):
            keep = lax.div(iota((cb, sb), 0), size) == lax.div(iota((cb, sb), 1), states)
            at = pl.ds(pl.multiple_of(b * cb, cb), cb)
            def widen(ref):
                high = ref[at, :].astype(BF16)
                low = (ref[at, :] - high.astype(F32)).astype(BF16)
                return (jnp.dot(high, spread_narrow, preferred_element_type=F32)
                        + jnp.dot(low, spread_narrow, preferred_element_type=F32))

            vr, vi = widen(inr_ref), widen(ini_ref)
            cr, ci = ratio[b, 0:1, :], ratio[b, 1:2, :]
            read_in[b, :, :sb] = jnp.where(keep, cr * vr - ci * vi, 0.0).astype(BF16)
            read_in[b, :, sb:] = jnp.where(keep, cr * vi + ci * vr, 0.0).astype(BF16)
            zero = jnp.zeros((CHUNKS, sb), F32)
            sr, si = scan(b, (zero, zero), False)
            ends[b, :, :sb] = sr
            ends[b, :, sb:] = si
            lr, li = cpow(a_ref[b, 0:1, :], a_ref[b, 1:2, :], span)
            er, ei = sr[0:1], si[0:1]
            for chunk in range(1, CHUNKS):
                er, ei = cmul(lr, li, er, ei)
                er, ei = er + sr[chunk:chunk + 1], ei + si[chunk:chunk + 1]
            total[b, :, :sb] = er
            total[b, :, sb:] = ei

    def pass_z(w, s):
        with jax.named_scope(f"z{w}{s}"):
            wait_z(w, s)

        @pl.when(inner)
        def _():
            relay(w, s)

        send_y(w, 2 + s)

    def pass_e(w, s):
        with jax.named_scope(f"e{w}{s}"):
            wait_e(w, s)
        send_y(w, 4 + s)

    def pass_l(w, s):
        with jax.named_scope(f"l{w}{s}"):
            wait_l(w, s)
        send_y(w, 6 + s)

    here = m * 2 + v
    level = h * 2 + u
    for k, there in enumerate((to_x, to_y, (h, u, om, ov, core))):
        send(total, gathered.at[here], there, ("s", k))
    gathered[here] = total[...]
    send_x(0, 0)
    for w in (1, 2):
        for s in (1, 0):
            send_x(w, s)
    send_y(1, 0)
    send_y(2, 0)
    with jax.named_scope("C_readout"):
        @pl.loop(0, blocks)
        def _(b):
            high = (lax.rem(iota((sb, states), 0), states) == iota((sb, states), 1)).astype(BF16)
            keep = lax.div(iota((sb, cb), 0), states) == lax.div(iota((sb, cb), 1), size)
            at = pl.ds(pl.multiple_of(b * cb, cb), cb)
            for place_in, ref, sign in ((0, outr_ref, 1.0), (1, outi_ref, -1.0)):
                wide = lax.dot_general(high, (sign * ref[at, :]).astype(BF16), across,
                                       preferred_element_type=F32)
                read_out[b, place_in * sb:(place_in + 1) * sb, :] = jnp.where(
                    keep, wide, 0.0).astype(BF16)

    with jax.named_scope("C_states1"):
        for k, (a, b) in enumerate(((m, ov), (om, v), (om, ov))):
            arrive(gathered.at[a * 2 + b], to_x, ("s", k))

    def power_of(b, count):
        return cpow(a_ref[b, 0:1, :], a_ref[b, 1:2, :], count)

    @pl.loop(0, blocks)
    def _(b):
        tr, ti = power_of(b, span * CHUNKS)
        hr = jnp.zeros((1, sb), F32)
        hi, pr, pi = hr, hr, hr
        for device in range(4):
            gr, gi = gathered[device, b, :, :sb], gathered[device, b, :, sb:]
            nr, ni = cmul(tr, ti, hr, hi)
            hr = jnp.where(device < here, nr + gr, hr)
            hi = jnp.where(device < here, ni + gi, hi)
            nr, ni = cmul(tr, ti, pr, pi)
            pr, pi = nr + gr, ni + gi
        prefix[b, :, :sb] = hr
        prefix[b, :, sb:] = hi
        plane_total[b, :, :sb] = pr
        plane_total[b, :, sb:] = pi

    for k, (a, b) in enumerate(((h, ou), (oh, u), (oh, ou))):
        send(plane_total, planes.at[level], (a, b, m, v, core), ("plane", k))
    planes[level] = plane_total[...]
    with jax.named_scope("C_x01"):
        wait_x(0, 1)
    send_z(0, 1)
    send_inner(0, 1)
    send_c(0, 0, 0)
    for copy in loads[11:]:
        copy.wait()
    pass_z(0, 0)
    with jax.named_scope("C_states2"):
        for k, (a, b) in enumerate(((h, ou), (oh, u), (oh, ou))):
            arrive(planes.at[a * 2 + b], to_x, ("plane", k))
    with jax.named_scope("C_x00"):
        wait_x(0, 0)
    send_c(0, 1, 0)
    send_c(0, 1, 1)
    send_y(0, 1)
    send_z(1, 0)
    send_inner(1, 0)
    send_z(2, 0)

    def second(b):
        lr, li = power_of(b, span)
        tr, ti = cpow(lr, li, CHUNKS)
        qr, qi = cpow(tr, ti, 4)
        hr = jnp.zeros((1, sb), F32)
        hi = hr
        for other in range(3):
            nr, ni = cmul(qr, qi, hr, hi)
            hr = jnp.where(other < level, nr + planes[other, b, :, :sb], hr)
            hi = jnp.where(other < level, ni + planes[other, b, :, sb:], hi)
        for device in range(3):
            nr, ni = cmul(tr, ti, hr, hi)
            hr, hi = jnp.where(device < here, nr, hr), jnp.where(device < here, ni, hi)
        hr, hi = hr + prefix[b, :, :sb], hi + prefix[b, :, sb:]
        starts_r, starts_i = [hr], [hi]
        for chunk in range(CHUNKS - 1):
            nr, ni = cmul(lr, li, hr, hi)
            hr = nr + ends[b, chunk:chunk + 1, :sb]
            hi = ni + ends[b, chunk:chunk + 1, sb:]
            starts_r.append(hr)
            starts_i.append(hi)
        scan(b, (jnp.concatenate(starts_r, axis=0), jnp.concatenate(starts_i, axis=0)), True)
        mixed = jnp.dot(work[...].astype(BF16), read_out[b], preferred_element_type=F32)
        at = pl.ds(pl.multiple_of(b * cb, cb), cb)
        mixed = mixed + k_ref[:, at] * x_ref[b].astype(F32)
        mixed = jax.nn.gelu(mixed).astype(BF16)
        act[:, at] = jnp.dot(
            turn[...], mixed, preferred_element_type=F32
        ).astype(BF16)

    with jax.named_scope("D_scan2a"):
        @pl.loop(0, blocks // 2)
        def _(b):
            second(b)

    pass_z(0, 1)
    with jax.named_scope("D_x11"):
        wait_x(1, 1)
    send_z(1, 1)
    send_inner(1, 1)
    with jax.named_scope("D_scan2b"):
        @pl.loop(blocks // 2, blocks)
        def _(b):
            second(b)

    with jax.named_scope("D_x10"):
        wait_x(1, 0)
    send_y(1, 1)
    send_c(1, 0, 1)
    send_c(1, 1, 1)

    tile = min(512, width)
    with jax.named_scope("E_outproj"):
        for t in (1, 0):
            to = core if t == 0 else 1 - core

            @pl.loop(0, width // tile)
            def _(j):
                at = pl.ds(pl.multiple_of(j * tile, tile), tile)
                share[t, :, at] = jnp.dot(
                    act[pl.ds(pl.multiple_of(to * keep_rows, keep_rows), keep_rows), :],
                    wo_ref[:, at], preferred_element_type=F32,
                ).astype(BF16)

            if t:
                send(share.at[1], others, to_t, ("mix",))

    with jax.named_scope("G_mix"):
        arrive(others, to_t, ("mix",))
    line = min(32, keep_rows)
    with jax.named_scope("H_norm"):
        @pl.loop(0, keep_rows // line)
        def _(i):
            at = pl.ds(pl.multiple_of(i * line, line), line)
            mixed = share[0, at, :].astype(F32) + others[at, :].astype(F32)
            carried = res_ref[at, :].astype(F32) + mixed.astype(BF16).astype(F32)
            scale = lax.rsqrt(jnp.mean(carried * carried, axis=-1, keepdims=True) + 1e-06)
            carried_ref[at, :] = carried
            rows_ref[0, 0, at, :] = (carried * scale * gain_ref[...]).astype(BF16)

    send(rows_ref.at[0, 0], rows_ref.at[0, 1], to_x, ("r", 1), moves)
    piece = keep_rows // PIECES
    for part in range(PIECES):
        at = pl.ds(part * piece, piece)
        send(rows_ref.at[0, 0, at], rows_ref.at[0, 2, at], to_z, ("r", 2, part), moves)
    send(rows_ref.at[0, 0], rows_ref.at[1, 0], to_t, ("t", 0), moves)

    def share_core(k):
        send(rows_ref.at[0, k], rows_ref.at[1, k], to_t, ("t", k), moves)

    def wait_core(k):
        arrive(rows_ref.at[1, k], to_t, ("t", k))

    def product(k, at):
        block = rows_ref[:, k].reshape(2 * keep_rows, width)
        return lax.dot_general(block, joined[at, :], across, preferred_element_type=F32)

    def keep_hidden(k, gate, up):
        result = (jax.nn.silu(gate) * up).astype(BF16)
        for t in range(2):
            hidden[pl.ds((4 * t + k) * keep_rows, keep_rows), :] = (
                result[t * keep_rows:(t + 1) * keep_rows])

    def gate_part(k):
        with jax.named_scope(f"gate{k}"):
            gates[k] = product(k, pl.ds(0, slab))

    def up_part(k):
        with jax.named_scope(f"up{k}"):
            keep_hidden(k, gates[k], product(k, pl.ds(pitch, slab)))

    def both_parts(k):
        with jax.named_scope(f"both{k}"):
            result = product(k, pl.ds(0, 2 * pitch))
            keep_hidden(k, result[:, :slab], result[:, pitch:pitch + slab])

    def first_rows():
        with jax.named_scope("r1"):
            arrive(rows_ref.at[0, 1], to_x, ("r", 1))
        share_core(1)

    def relay_rows(part):
        at = pl.ds(part * piece, piece)
        with jax.named_scope(f"r2{part}"):
            arrive(rows_ref.at[0, 2, at], to_z, ("r", 2, part))
        send(rows_ref.at[0, 2, at], rows_ref.at[0, 3, at], to_x, ("r", 3, part), moves)
        if part == PIECES - 1:
            share_core(2)

    def last_rows():
        with jax.named_scope("r3"):
            for part in range(PIECES):
                at = pl.ds(part * piece, piece)
                arrive(rows_ref.at[0, 3, at], to_x, ("r", 3, part))
        share_core(3)

    def second_weights():
        send_inner(2, 0)
        wait_x(2, 1)
        send_inner(2, 1)
        send_z(2, 1)
        wait_x(2, 0)
        send_y(2, 1)
        send_c(2, 0, 0)
        send_c(2, 1, 0)

    def delayed_weights():
        send_c(2, 0, 1)
        send_c(2, 1, 1)

    def whole(w):
        with jax.named_scope(f"y{w}"):
            for j in range(8):
                wait_y(w, j)

    def core_rows(k):
        with jax.named_scope(f"t{k}"):
            wait_core(k)

    for s in range(2):
        send_c(1, s, 0)
    pass_e(0, 0)
    pass_e(0, 1)
    pass_z(1, 0)
    pass_z(1, 1)
    pass_l(0, 0)
    pass_l(0, 1)
    pass_e(1, 0)
    for copy in local:
        copy.wait()
    whole(0)
    core_rows(0)
    gate_part(0)
    first_rows()
    second_weights()
    relay_rows(0)
    pass_e(1, 1)
    relay_rows(1)
    core_rows(1)
    gate_part(1)
    pass_l(1, 0)
    pass_l(1, 1)
    delayed_weights()
    relay_rows(2)
    whole(1)
    up_part(0)
    relay_rows(3)
    up_part(1)
    core_rows(2)
    pass_z(2, 0)
    both_parts(2)
    last_rows()
    pass_z(2, 1)
    core_rows(3)
    both_parts(3)
    pass_e(2, 0)
    with jax.named_scope("moves"):
        for copy in moves:
            copy.wait_send()

    across_u = width // 8
    chunks = [(h, h, m), (h, oh, m), (h, h, om), (h, oh, om), (oh, h, m), (oh, oh, m),
              (oh, h, om), (oh, oh, om)]

    def columns(j):
        a, b, c = chunks[j]
        return pl.ds(pl.multiple_of(index(a, b, c, 0) * depth, across_u), across_u)

    def down(j):
        pair_of = (2 * j, 2 * j + 1)
        right = jnp.concatenate([down_full[:, columns(i)] for i in pair_of], axis=1)
        for t in (1, 0):
            result = jnp.dot(
                hidden[4 * t * keep_rows:4 * (t + 1) * keep_rows, :], right,
                preferred_element_type=F32,
            ).astype(BF16)
            for side, i in enumerate(pair_of):
                for k in range(4):
                    rows_ref[t, k, :, columns(i)] = result[
                        k * keep_rows:(k + 1) * keep_rows, side * across_u:(side + 1) * across_u]
                if t:
                    send(rows_ref.at[1, :, :, columns(i)], partners.at[i], to_t, ("p", i))

    def add(target, j, other):
        at = columns(j)

        @pl.loop(0, keep_rows // line)
        def _(i):
            lines = pl.ds(pl.multiple_of(i * line, line), line)
            rows_ref[0, target, lines, at] = (
                rows_ref[0, target, lines, at].astype(F32) + other[lines, :].astype(F32)
            ).astype(BF16)

    def pair(j):
        at = columns(j)
        near, far = (1, 2) if X_FIRST[j] else (2, 1)
        device = to_x if X_FIRST[j] else to_z
        arrive(partners.at[j], to_t, ("p", j))
        for place_in, k in enumerate((3, near)):
            add(k, j, partners.at[j, k])
            send(rows_ref.at[0, k, :, at], firsts.at[j, place_in], device, ("f", j, place_in))
        add(far, j, partners.at[j, far])
        add(0, j, partners.at[j, 0])

    def combine(j):
        at = columns(j)
        far = 2 if X_FIRST[j] else 1
        device, other = (to_x, to_z) if X_FIRST[j] else (to_z, to_x)
        arrive(firsts.at[j, 0], device, ("f", j, 0))
        add(far, j, firsts.at[j, 0])
        send(rows_ref.at[0, far, :, at], seconds.at[j], other, ("g", j))
        arrive(firsts.at[j, 1], device, ("f", j, 1))
        add(0, j, firsts.at[j, 1])

    stored = []

    def finish(j):
        at = columns(j)
        arrive(seconds.at[j], to_z if X_FIRST[j] else to_x, ("g", j))

        @pl.loop(0, keep_rows // line)
        def _(i):
            lines = pl.ds(pl.multiple_of(i * line, line), line)
            summed = rows_ref[0, 0, lines, at].astype(F32) + seconds[j, lines, :].astype(F32)
            summed = summed.astype(BF16).astype(F32)
            out_ref[lines, at] = (carried_ref[lines, at] + 0.5 * summed).astype(BF16)

        copy = pltpu.make_async_copy(out_ref.at[:, at], out_hbm.at[:, at], out_sem.at[j])
        copy.start()
        stored.append(copy)

    order = ORDER
    stages = {"d": down, "p": pair, "c": combine, "f": finish}
    for word in order:
        if word == "e":
            pass_e(2, 1)
            continue
        if word == "l":
            pass_l(2, 0)
            pass_l(2, 1)
            continue
        j = int(word[1])
        if word in ("d1", "d3"):
            with jax.named_scope("y2" + word):
                for i in range(4 * (j // 2), 4 * (j // 2) + 4):
                    wait_y(2, i)
        with jax.named_scope({"d": "down", "p": "pair", "c": "comb", "f": "fin"}[word[0]] + word[1]):
            stages[word[0]](j)
    with jax.named_scope("end_sends"):
        for copy in everywhere:
            copy.wait_send()

        @pl.when(inner)
        def _():
            for name, number in inside:
                describe(extra.at[0], extra.at[0], to_c, name, number).wait_send()

    with jax.named_scope("end_store"):
        for copy in stored:
            copy.wait()


def shift(value, axis, count, by):
    return lax.ppermute(value, axis, [(i, (i + by) % count) for i in range(count)])


def flip(value, axes, count, k):
    return lax.ppermute(value, axes, [(i, i ^ k) for i in range(count)])


def on_device(sizes, mixer_in, residual, decay_real, decay_imag, log_step, in_real, in_imag,
              output_real, output_imaginary, skip, out_proj, norm_gain, w_gate, w_up, w_down):
    tp, nh, nm = sizes["tp"], sizes["h"], sizes["m"]
    n = nh * 4 * nm
    rows, channels = mixer_in.shape
    keep_rows, width = residual.shape
    depth, hidden_units = w_gate.shape
    part = hidden_units // 4
    groups, states = decay_real.shape
    blocks = groups // GATHER
    cb, sb = channels // blocks, GATHER * states
    vmem = pl.BlockSpec(memory_space=pltpu.VMEM)
    if depth % 128 == 0 and (tp, nh, nm) == (2, 2, 2):
        cut = width // 8
        pitch = -(-part // 128) * 128
        return pl.pallas_call(
            functools.partial(streamed, sizes),
            in_specs=[pl.BlockSpec(memory_space=pl.ANY)] * 15,
            out_specs=pl.BlockSpec(memory_space=pl.ANY),
            out_shape=jax.ShapeDtypeStruct((keep_rows, width), BF16),
            scratch_shapes=[
                pltpu.VMEM((keep_rows, width), BF16),
                pltpu.SemaphoreType.DMA((8,)),
                pltpu.VMEM((2 * pitch, n * depth), BF16),
                pltpu.VMEM((part, n * depth), BF16),
                pltpu.VMEM((3, part, depth), BF16),
                pltpu.VMEM((2, 4, keep_rows, width), BF16),
                pltpu.VMEM((keep_rows, width), F32),
                pltpu.VMEM((4, 2 * keep_rows, part), F32),
                pltpu.VMEM((8 * keep_rows, part), BF16),
                pltpu.VMEM((8, 4, keep_rows, cut), BF16),
                pltpu.VMEM((8, 2, keep_rows, cut), BF16),
                pltpu.VMEM((8, keep_rows, cut), BF16),
                pltpu.VMEM((rows, 2 * sb), F32),
                pltpu.VMEM((blocks, cb, 2 * sb), BF16),
                pltpu.VMEM((blocks, 2 * sb, cb), BF16),
                pltpu.VMEM((blocks, CHUNKS, 2 * sb), F32),
                pltpu.VMEM((blocks, 1, 2 * sb), F32),
                pltpu.VMEM((4, blocks, 1, 2 * sb), F32),
                pltpu.VMEM((blocks, 1, 2 * sb), F32),
                pltpu.VMEM((blocks, 1, 2 * sb), F32),
                pltpu.VMEM((4, blocks, 1, 2 * sb), F32),
                pltpu.VMEM((rows, rows), BF16),
                pltpu.VMEM((rows, channels), BF16),
                pltpu.VMEM((2, keep_rows, width), BF16),
                pltpu.VMEM((keep_rows, width), BF16),
                pltpu.VMEM((rows, channels), BF16),
                pltpu.VMEM((blocks, rows, cb), BF16),
                pltpu.VMEM((keep_rows, width), BF16),
                *[pltpu.VMEM((groups, states), F32)] * 2,
                pltpu.VMEM((1, groups), F32),
                *[pltpu.VMEM((channels, states), F32)] * 4,
                pltpu.VMEM((1, channels), F32),
                pltpu.VMEM((channels, width), BF16),
                pltpu.VMEM((1, width), F32),
                pltpu.VMEM((2, depth, hidden_units), BF16),
                pltpu.VMEM((2, hidden_units, depth), BF16),
                pltpu.VMEM((hidden_units, depth), BF16),
                pltpu.VMEM((blocks, 2, sb), F32),
                pltpu.VMEM((blocks, 2, sb), F32),
                pltpu.SemaphoreType.DMA((106,)),
                pltpu.SemaphoreType.DMA((100,)),
                pltpu.SemaphoreType.DMA((3,)),
                pltpu.SemaphoreType.DMA((15,)),
            ],
            compiler_params=pltpu.CompilerParams(
                collective_id=0, has_side_effects=True, vmem_limit_bytes=62 * 2**20
            ),
            name="streamed",
        )(mixer_in, residual, decay_real, decay_imag, log_step.reshape(1, groups),
          in_real.transpose(0, 2, 1).reshape(channels, states),
          in_imag.transpose(0, 2, 1).reshape(channels, states),
          output_real.reshape(channels, states), output_imaginary.reshape(channels, states),
          skip.reshape(1, channels), out_proj, norm_gain.reshape(1, width), w_gate, w_up, w_down)
    power_re, power_im, bar_re, bar_im = discrete(
        decay_real, decay_imag, log_step, in_real, in_imag
    )
    rows_first = lambda t: jnp.transpose(t, (0, 2, 1)).reshape(blocks, -1, t.shape[1])
    read_in = jnp.stack([rows_first(bar_re), rows_first(bar_im)], axis=1).astype(BF16)
    read_out = jnp.stack(
        [rows_first(output_real), -rows_first(output_imaginary)], axis=1
    ).astype(BF16)
    power = jnp.stack([power_re.reshape(blocks, sb), power_im.reshape(blocks, sb)], axis=1)
    x = mixer_in.reshape(CHUNKS, rows // CHUNKS, blocks, cb).transpose(2, 1, 0, 3)
    x = x.reshape(blocks, rows, cb)
    operands = (x, read_in, read_out, power, skip.reshape(blocks, 1, cb), out_proj, residual,
                norm_gain.reshape(1, width), w_gate.T.reshape(4, part, depth),
                w_up.T.reshape(4, part, depth), w_down.reshape(4, part, depth))
    copies = 3 * (3 + 4 * (nh - 1) + 4 * nh * (nm - 1)) + (n - 1) + (tp - 1) + 3 + 4 * (tp - 1)
    laid = (part, n * depth) if depth % 128 == 0 else (n, part, depth)
    between = [(laid, BF16)] * 3 + [
        ((tp, 4, keep_rows, width), BF16), ((keep_rows, width), F32),
    ]
    fused = depth % 128 == 0
    if fused:
        copies += 4 * (tp - 1) + 3
        out_shape = [jax.ShapeDtypeStruct((keep_rows, width), BF16)]
        extra = [
            pltpu.VMEM((4 * tp, keep_rows, part), BF16),
            pltpu.VMEM((4, tp - 1, keep_rows, width), BF16),
            pltpu.VMEM((3, keep_rows, width), BF16),
            *(pltpu.VMEM(*item) for item in between),
        ]
    else:
        out_shape = [jax.ShapeDtypeStruct(*item) for item in between]
        extra = []
    results = pl.pallas_call(
        functools.partial(layer, sizes, fused),
        in_specs=[vmem] * 11,
        out_specs=[vmem] * len(out_shape),
        out_shape=out_shape,
        scratch_shapes=[
            *extra,
            pltpu.VMEM((rows, 2 * sb), F32),
            pltpu.VMEM((blocks, cb, 2 * sb), BF16),
            pltpu.VMEM((blocks, 2 * sb, cb), BF16),
            pltpu.VMEM((blocks, CHUNKS, 2 * sb), F32),
            pltpu.VMEM((blocks, 1, 2 * sb), F32),
            pltpu.VMEM((n, blocks, 1, 2 * sb), F32),
            pltpu.VMEM((rows, channels), BF16),
            pltpu.VMEM((tp, keep_rows, width), BF16),
            pltpu.VMEM((tp - 1, keep_rows, width), BF16),
            pltpu.SemaphoreType.DMA((copies,)),
            pltpu.SemaphoreType.DMA((copies,)),
            pltpu.SemaphoreType.DMA((3,)),
        ],
        compiler_params=pltpu.CompilerParams(
            collective_id=0, has_side_effects=True, vmem_limit_bytes=62 * 2**20
        ),
        name="layer",
    )(*operands)
    if fused:
        return results[0]
    full_gate, full_up, full_down, rows_all, carried = results
    if len(laid) == 3:
        full_gate, full_up, full_down = (
            t.transpose(1, 0, 2).reshape(part, width) for t in (full_gate, full_up, full_down)
        )

    flat = rows_all.reshape(-1, width)
    across = (((1,), (1,)), ((), ()))
    gate = lax.dot_general(flat, full_gate, across, preferred_element_type=F32)
    up = lax.dot_general(flat, full_up, across, preferred_element_type=F32)
    hidden = (jax.nn.silu(gate) * up).astype(BF16)
    down = jnp.dot(hidden, full_down, preferred_element_type=F32).astype(BF16)
    down = down.reshape(rows_all.shape)
    summed = down[0].astype(F32)
    for t in range(1, tp):
        summed = summed + shift(down[t], "tp", tp, -t).astype(F32)
    summed = summed.astype(BF16)
    total = summed[0].astype(F32)
    for k in range(1, 4):
        total = total + flip(summed[k], PEERS, 4, k).astype(F32)
    total = total.astype(BF16)
    return (carried + 0.5 * total.astype(F32)).astype(BF16)


def solution(mesh):
    sp, tp = mesh.shape["sp"], mesh.shape["tp"]
    sizes = {"h": sp // 8, "u": 2, "m": 2, "v": 2, "tp": tp}
    cut = Mesh(mesh.devices.reshape(tuple(sizes.values())), tuple(sizes))
    return jax.shard_map(
        functools.partial(on_device, sizes),
        mesh=cut,
        in_specs=(
            P(SP, "tp"),
            P((*SP, "tp"), None),
            P("tp", None),
            P("tp", None),
            P("tp"),
            P("tp", None, None),
            P("tp", None, None),
            P("tp", None, None),
            P("tp", None, None),
            P("tp"),
            P("tp", None),
            P(),
            P(SP, "tp"),
            P(SP, "tp"),
            P("tp", SP),
        ),
        out_specs=P((*SP, "tp"), None),
        check_vma=False,
    )
```

```python
import functools

import jax
import jax.numpy as jnp
from jax import lax
from jax.experimental import pallas as pl
from jax.experimental.pallas import tpu as pltpu
from jax.sharding import Mesh
from jax.sharding import PartitionSpec as P

F32 = jnp.float32
BF16 = jnp.bfloat16
SP = ("h", "u", "m", "v")
PEERS = ("u", "v")
GATHER = 8
CHUNKS = 8
X_FIRST = (1, 1, 1, 0, 1, 0, 1, 0)
PIECES = 4
ORDER = ("d0", "e", "p0", "p1", "d1", "p2", "p3", "l", "d2", "p4", "p5", "c0", "d3", "p6", "p7",
         "c1", "c2", "c3", "c4", "c5", "f0", "f1", "c6", "c7", "f2", "f3", "f4", "f5", "f6", "f7")
MESH = pl.DeviceIdType.MESH


def discrete(decay_real, decay_imag, log_step, in_real, in_imag):
    step_size = jnp.exp(log_step)[:, None]
    magnitude = jnp.exp(decay_real * step_size)
    angle = decay_imag * step_size
    power_re = magnitude * jnp.cos(angle)
    power_im = magnitude * jnp.sin(angle)
    denom = decay_real * decay_real + decay_imag * decay_imag
    ratio_re = ((power_re - 1.0) * decay_real + power_im * decay_imag) / denom
    ratio_im = (power_im * decay_real - (power_re - 1.0) * decay_imag) / denom
    drive_re = ratio_re[..., None] * in_real - ratio_im[..., None] * in_imag
    drive_im = ratio_re[..., None] * in_imag + ratio_im[..., None] * in_real
    return (power_re, power_im, drive_re, drive_im)


def cmul(ar, ai, br, bi):
    return ar * br - ai * bi, ar * bi + ai * br


def cpow(ar, ai, count):
    result = None
    while count:
        if count & 1:
            result = (ar, ai) if result is None else cmul(*result, ar, ai)
        count >>= 1
        if count:
            ar, ai = cmul(ar, ai, ar, ai)
    return result


def iota(shape, dim):
    return lax.broadcasted_iota(jnp.int32, shape, dim)


def tiled(block, copies, across, down):
    rows, columns = block.shape
    wide = (columns, columns * copies)
    pick = (iota(wide, 0) == lax.rem(iota(wide, 1), columns)).astype(BF16)
    full = jnp.dot(block, pick, preferred_element_type=F32)
    keep = lax.div(iota(full.shape, 0), down) == lax.div(iota(full.shape, 1), across)
    return jnp.where(keep, full, 0.0).astype(BF16)


def layer(sizes, fused, x_ref, b_ref, c_ref, a_ref, k_ref, wo_ref, res_ref, gain_ref, *rest):
    quarters, rest = rest[:3], rest[3:]
    if fused:
        out_ref, *rest = rest
        hidden, partners, peers, *rest = rest
    weights, (rows_ref, carried_ref), rest = rest[:3], rest[3:5], rest[5:]
    (work, read_in, read_out, ends, total, gathered, act, share, others,
     send_sem, recv_sem, local_sem) = rest
    blocks, rows, cb = x_ref.shape
    sb = a_ref.shape[2]
    depth = quarters[0].shape[2]
    width = wo_ref.shape[1]
    span = rows // CHUNKS
    nh, nm, tp = sizes["h"], sizes["m"], sizes["tp"]
    n = nh * 4 * nm
    h, u, m, v, core = (lax.axis_index(name) for name in (*SP, "tp"))
    index = lambda h, u, m, v: ((h * 2 + u) * nm + m) * 2 + v
    me = index(h, u, m, v)
    peer = lambda k: (1 - u if k & 2 else u, 1 - v if k & 1 else v)
    counter = iter(range(send_sem.shape[0]))

    def send(src, dst, device):
        slot = next(counter)
        copy = pltpu.make_async_remote_copy(
            src_ref=src, dst_ref=dst, send_sem=send_sem.at[slot], recv_sem=recv_sem.at[slot],
            device_id=device, device_id_type=MESH,
        )
        copy.start()
        return copy

    def place(ref, position):
        if depth % 128:
            return ref.at[position]
        return ref.at[:, pl.ds(pl.multiple_of(position * depth, depth), depth)]

    barrier = pltpu.get_barrier_semaphore()
    others_sp = []
    for k in range(1, n):
        to = lax.rem(me + k, n)
        there = (lax.div(to, 4 * nm), lax.rem(lax.div(to, 2 * nm), 2),
                 lax.rem(lax.div(to, 2), nm), lax.rem(to, 2), core)
        others_sp.append(there)
        pl.semaphore_signal(barrier, inc=1, device_id=there, device_id_type=MESH)
    for t in range(1, tp):
        pl.semaphore_signal(
            barrier, inc=1, device_id=(h, u, m, v, lax.rem(core + t, tp)), device_id_type=MESH
        )
    pl.semaphore_wait(barrier, n - 1 + tp - 1)

    sent = []
    first = {}
    over_h = {}
    over_m = {}

    def spread_h(w, k, src, position):
        for r in range(1, nh):
            pu, pv = peer(k)
            copy = send(src, place(weights[w], position), (lax.rem(h + r, nh), u, m, v, core))
            over_h[w, k, r] = copy

    def spread_m(w, k, r, src, position):
        for s in range(1, nm):
            over_m[w, k, r, s] = send(
                src, place(weights[w], position), (h, u, lax.rem(m + s, nm), v, core)
            )

    own = u * 2 + v
    for w in range(3):
        for k in (3, 1, 2):
            pu, pv = peer(k)
            first[w, k] = send(
                quarters[w].at[pu * 2 + pv], place(weights[w], me), (h, pu, m, pv, core)
            )
    locals_ = []
    for w in range(3):
        spread_h(w, 0, quarters[w].at[own], me)
        spread_m(w, 0, 0, quarters[w].at[own], me)
        copy = pltpu.make_async_copy(quarters[w].at[own], place(weights[w], me), local_sem.at[w])
        copy.start()
        locals_.append(copy)

    def scan(b, start, keep):
        work[...] = jnp.dot(x_ref[b], read_in[b], preferred_element_type=F32)
        br = jnp.broadcast_to(a_ref[b, 0:1, :], (CHUNKS, sb))
        bi = jnp.broadcast_to(a_ref[b, 1:2, :], (CHUNKS, sb))

        def step(i, state):
            at = pl.ds(pl.multiple_of(i * CHUNKS, CHUNKS), CHUNKS)
            nr, ni = cmul(br, bi, *state)
            nr, ni = nr + work[at, :sb], ni + work[at, sb:]
            if keep:
                work[at, :sb] = nr
                work[at, sb:] = ni
            return nr, ni

        return lax.fori_loop(0, span, step, start, unroll=8)

    @pl.loop(0, blocks)
    def _(b):
        states = b_ref.shape[3]
        for half in range(2):
            read_in[b, :, half * sb:(half + 1) * sb] = tiled(
                b_ref[b, half], GATHER, states, cb // GATHER
            )
            read_out[b, half * sb:(half + 1) * sb, :] = tiled(
                c_ref[b, half], GATHER, cb // GATHER, states
            )
        zero = jnp.zeros((CHUNKS, sb), F32)
        sr, si = scan(b, (zero, zero), False)
        ends[b, :, :sb] = sr
        ends[b, :, sb:] = si
        lr, li = cpow(a_ref[b, 0:1, :], a_ref[b, 1:2, :], span)
        er, ei = sr[0:1], si[0:1]
        for chunk in range(1, CHUNKS):
            er, ei = cmul(lr, li, er, ei)
            er, ei = er + sr[chunk:chunk + 1], ei + si[chunk:chunk + 1]
        total[b, :, :sb] = er
        total[b, :, sb:] = ei

    states_out = [send(total, gathered.at[me], there) for there in others_sp]
    gathered[me] = total[...]
    for copy in states_out:
        copy.wait_recv()

    @pl.loop(0, blocks)
    def _(b):
        lr, li = cpow(a_ref[b, 0:1, :], a_ref[b, 1:2, :], span)
        tr, ti = cpow(lr, li, CHUNKS)
        hr = jnp.zeros((1, sb), F32)
        hi = hr
        for device in range(n - 1):
            nr, ni = cmul(tr, ti, hr, hi)
            nr = nr + gathered[device, b, :, :sb]
            ni = ni + gathered[device, b, :, sb:]
            hr, hi = jnp.where(device < me, nr, hr), jnp.where(device < me, ni, hi)
        starts_r, starts_i = [hr], [hi]
        for chunk in range(CHUNKS - 1):
            nr, ni = cmul(lr, li, hr, hi)
            hr = nr + ends[b, chunk:chunk + 1, :sb]
            hi = ni + ends[b, chunk:chunk + 1, sb:]
            starts_r.append(hr)
            starts_i.append(hi)
        scan(b, (jnp.concatenate(starts_r, axis=0), jnp.concatenate(starts_i, axis=0)), True)
        mixed = jnp.dot(work[...].astype(BF16), read_out[b], preferred_element_type=F32)
        mixed = mixed + k_ref[b] * x_ref[b].astype(F32)
        mixed = jax.nn.gelu(mixed).astype(BF16)
        square = (rows, rows)
        source = lax.rem(iota(square, 0), span) * CHUNKS + lax.div(iota(square, 0), span)
        turn = (iota(square, 1) == source).astype(BF16)
        act[:, pl.ds(pl.multiple_of(b * cb, cb), cb)] = jnp.dot(
            turn, mixed, preferred_element_type=F32
        ).astype(BF16)

    keep_rows = rows // tp
    tile = min(512, width)
    mixed_copies = []
    for t in (*range(1, tp), 0):
        to = lax.rem(core + t, tp)

        @pl.loop(0, width // tile)
        def _(j):
            at = pl.ds(pl.multiple_of(j * tile, tile), tile)
            share[t, :, at] = jnp.dot(
                act[pl.ds(pl.multiple_of(to * keep_rows, keep_rows), keep_rows), :],
                wo_ref[:, at], preferred_element_type=F32,
            ).astype(BF16)

        if t:
            mixed_copies.append(send(share.at[t], others.at[t - 1], (h, u, m, v, to)))

    for w in range(3):
        for k in (1, 2, 3):
            first[w, k].wait_recv()
            pu, pv = peer(k)
            position = index(h, pu, m, pv)
            spread_h(w, k, place(weights[w], position), position)
            spread_m(w, k, 0, place(weights[w], position), position)

    for copy in mixed_copies:
        copy.wait_recv()
    line = min(32, keep_rows)

    @pl.loop(0, keep_rows // line)
    def _(i):
        at = pl.ds(pl.multiple_of(i * line, line), line)
        mixed = share[0, at, :].astype(F32)
        for t in range(1, tp):
            mixed = mixed + others[t - 1, at, :].astype(F32)
        carried = res_ref[at, :].astype(F32) + mixed.astype(BF16).astype(F32)
        scale = lax.rsqrt(jnp.mean(carried * carried, axis=-1, keepdims=True) + 1e-06)
        carried_ref[at, :] = carried
        rows_ref[0, 0, at, :] = (carried * scale * gain_ref[...]).astype(BF16)

    row_copies = {}
    for k in (3, 1, 2):
        pu, pv = peer(k)
        row_copies[k] = send(rows_ref.at[0, 0], rows_ref.at[0, k], (h, pu, m, pv, core))
    last = []
    for t in range(1, tp):
        last.append(send(rows_ref.at[0, 0], rows_ref.at[t, 0], (h, u, m, v, lax.rem(core + t, tp))))

    def pass_m(w, k):
        pu, pv = peer(k)
        for r in range(1, nh):
            over_h[w, k, r].wait_recv()
            position = index(lax.rem(h - r + nh, nh), pu, m, pv)
            spread_m(w, k, r, place(weights[w], position), position)

    for w in range(3):
        for k in range(4):
            pass_m(w, k)
        if w == 1:
            for k in (1, 2, 3):
                row_copies[k].wait_recv()
                for t in range(1, tp):
                    last.append(send(
                        rows_ref.at[0, k], rows_ref.at[t, k], (h, u, m, v, lax.rem(core + t, tp))
                    ))
    sent = [*first.values(), *over_h.values(), *over_m.values(), *states_out, *mixed_copies]
    row_sends = [*row_copies.values(), *last]
    for (w, *_), copy in over_m.items():
        if w < 2 or not fused:
            copy.wait_recv()
    for copy in last:
        copy.wait_recv()
    for copy in locals_:
        copy.wait()
    if fused:
        sent += back(
            sizes, send, peer, (h, u, m, v, core), weights, rows_ref, carried_ref, out_ref,
            hidden, partners, peers, row_sends, [c for (w, *_), c in over_m.items() if w == 2],
        )
    else:
        sent += row_sends
    for copy in sent:
        copy.wait_send()


def back(sizes, send, peer, here, weights, rows_ref, carried_ref, out_ref, hidden, partners,
         peers, row_sends, down_copies):
    tp = sizes["tp"]
    h, u, m, v, core = here
    _, _, keep_rows, width = rows_ref.shape
    across = (((1,), (1,)), ((), ()))

    @pl.loop(0, 4 * tp)
    def _(i):
        t, k = lax.div(i, 4), lax.rem(i, 4)
        block = rows_ref[t, k]
        gate = lax.dot_general(block, weights[0][...], across, preferred_element_type=F32)
        up = lax.dot_general(block, weights[1][...], across, preferred_element_type=F32)
        hidden[i] = (jax.nn.silu(gate) * up).astype(BF16)

    for copy in (*down_copies,):
        copy.wait_recv()
    for copy in row_sends:
        copy.wait_send()

    tile = min(512, width)
    line = min(32, keep_rows)
    sent = []
    peer_copies = []
    from_core = {}

    def reduce(k):
        for copy in from_core[k]:
            copy.wait_recv()

        @pl.loop(0, keep_rows // line)
        def _(i):
            at = pl.ds(pl.multiple_of(i * line, line), line)
            total = rows_ref[0, k, at, :].astype(F32)
            for t in range(1, tp):
                total = total + partners[k, t - 1, at, :].astype(F32)
            rows_ref[0, k, at, :] = total.astype(BF16)

        if k:
            pu, pv = peer(k)
            peer_copies.append(send(rows_ref.at[0, k], peers.at[k - 1], (h, pu, m, pv, core)))

    order = (3, 1, 2, 0)
    for step, k in enumerate(order):
        from_core[k] = []
        for t in (*range(1, tp), 0):
            @pl.loop(0, width // tile)
            def _(j):
                at = pl.ds(pl.multiple_of(j * tile, tile), tile)
                rows_ref[t, k, :, at] = jnp.dot(
                    hidden[t * 4 + k], weights[2][:, at], preferred_element_type=F32
                ).astype(BF16)

            if t:
                from_core[k].append(send(
                    rows_ref.at[t, k], partners.at[k, t - 1],
                    (h, u, m, v, lax.rem(core + tp - t, tp)),
                ))
        reduce(k)
        sent += from_core[k]
    for copy in peer_copies:
        copy.wait_recv()

    @pl.loop(0, keep_rows // line)
    def _(i):
        at = pl.ds(pl.multiple_of(i * line, line), line)
        total = rows_ref[0, 0, at, :].astype(F32)
        for k in range(1, 4):
            total = total + peers[k - 1, at, :].astype(F32)
        total = total.astype(BF16).astype(F32)
        out_ref[at, :] = (carried_ref[at, :] + 0.5 * total).astype(BF16)

    return sent + peer_copies


def streamed(sizes, x_hbm, residual_hbm, decay_re, decay_im, log_step, in_re, in_im, out_re, out_im,
             skip_hbm, wo_hbm, gain_hbm, gate_hbm, up_hbm, down_hbm, out_hbm, *rest):
    (out_ref, out_sem, joined, down_full, extra, rows_ref, carried_ref, gates, hidden, partners, firsts, seconds, work, read_in,
     read_out, ends, total, gathered, prefix, plane_total, planes, turn, act, share, others,
     x_raw, x_ref, res_ref, dr_ref, di_ref, ls_ref, inr_ref, ini_ref, outr_ref, outi_ref, k_ref,
     wo_ref, gain_ref, raw, turned, down_ref, a_ref, ratio, send_sem, recv_sem, local_sem, load_sem) = rest
    blocks, rows, cb = x_ref.shape
    sb = a_ref.shape[2]
    slab, depth = down_full.shape[0], raw.shape[1]
    pitch = joined.shape[0] // 2
    width = wo_ref.shape[1]
    keep_rows = rows // 2
    span = rows // CHUNKS
    nh, nm = sizes["h"], sizes["m"]
    n = nh * 4 * nm
    h, u, m, v, core = (lax.axis_index(name) for name in (*SP, "tp"))
    oh, ou, om, ov = 1 - h, 1 - u, 1 - m, 1 - v
    index = lambda h, u, m, v: ((h * 2 + u) * nm + m) * 2 + v
    me = index(h, u, m, v)
    to_x, to_z, to_y = (h, u, m, ov, core), (h, ou, m, v, core), (h, u, om, v, core)
    to_c, to_b, to_t = (oh, u, m, v, core), (oh, ou, m, v, core), (h, u, m, v, 1 - core)
    plane = [(h, b, c) for b in (u, ou) for c in (v, ov)]
    plane += [(oh, b, c) for b in (h, oh) for c in (v, ov)]
    is_inner = lax.rem(h + u, 2)
    inner = is_inner == 1
    across = (((1,), (1,)), ((), ()))
    slots, everywhere, moves = {}, [], []
    groups_of, fixed = {}, {}
    counter = iter(range(send_sem.shape[0]))

    def slot(name):
        return slots.setdefault(name, len(slots))

    def describe(src, dst, device, name, number):
        return pltpu.make_async_remote_copy(
            src_ref=src, dst_ref=dst, send_sem=send_sem.at[number],
            recv_sem=recv_sem.at[slot(name) if isinstance(name, tuple) else name], device_id=device, device_id_type=MESH,
        )

    def group_number(group):
        if group not in fixed:
            fixed[group] = next(counter)
        groups_of[group] = groups_of.get(group, 0) + 1
        return fixed[group]

    def send(src, dst, device, name, kept=everywhere, group=None):
        number = next(counter) if group is None else group_number(group)
        copy = describe(src, dst, device, name, number)
        copy.start()
        if group is None:
            kept.append(copy)

    def arrive(dst, device, name):
        describe(dst, dst, device, name, 0).wait_recv()

    def place(w, position):
        at = pl.ds(pl.multiple_of(position * depth, depth), depth)
        return down_full.at[:, at] if w == 2 else joined.at[pl.ds(w * pitch, slab), at]

    def spot(w, j, row=m):
        a, b, c = plane[j]
        return place(w, index(a, b, row, c))

    def mine(w, b, c):
        at = pl.ds(pl.multiple_of((b * 2 + c) * slab, slab), slab)
        return down_ref.at[at, :] if w == 2 else turned.at[w, at, :]

    def own(w):
        return mine(w, u, v)

    def send_x(w, s):
        if s:
            send(mine(w, ou, ov), extra.at[w], to_x, ("xo", w), group=("w", w))
        else:
            send(mine(w, u, ov), spot(w, 0), to_x, ("xu", w), group=("w", w))

    def send_z(w, s):
        send(extra.at[w] if s else mine(w, ou, v), spot(w, s), to_z, ("z", w, s), group=("w", w))

    numbers = {}

    def send_c(w, s, kind):
        if (w, s) not in numbers:
            numbers[w, s] = group_number(("w", w))
        number = numbers[w, s]
        name = ("e" if kind else "l", w, s)

        @pl.when(is_inner == kind)
        def _():
            describe(spot(w, 1) if s else own(w), spot(w, s), to_c, name, number).start()

    def send_b(w, s):
        send(extra.at[w] if s else mine(w, ou, v), spot(w, s), to_b, ("e", w, s), group="inside")

    def relay(w, s):
        send(spot(w, 2 + s), spot(w, 2 + s), to_c, ("l", w, s), group="inside")

    def send_y(w, j):
        send(own(w) if j == 0 else spot(w, j), spot(w, j), to_y, ("y", w, j), group=("w", w))

    def wait_x(w, s):
        if s:
            arrive(extra.at[w], to_x, ("xo", w))
        else:
            arrive(spot(w, 1), to_x, ("xu", w))

    def wait_z(w, s):
        arrive(spot(w, 2 + s), to_z, ("z", w, s))

    def wait_e(w, s):
        arrive(spot(w, 4 + s), to_c, ("e", w, s))

    def wait_l(w, s):
        arrive(spot(w, 6 + s), to_c, ("l", w, s))

    def wait_y(w, j):
        arrive(spot(w, j, om), to_y, ("y", w, j))

    barrier = pltpu.get_barrier_semaphore()
    others_sp = []
    for k in range(1, n):
        to = lax.rem(me + k, n)
        there = (lax.div(to, 4 * nm), lax.rem(lax.div(to, 2 * nm), 2),
                 lax.rem(lax.div(to, 2), nm), lax.rem(to, 2), core)
        others_sp.append(there)
        pl.semaphore_signal(barrier, inc=1, device_id=there, device_id_type=MESH)
    pl.semaphore_signal(barrier, inc=1, device_id=to_t, device_id_type=MESH)
    pairs = ((gate_hbm, raw.at[0]), (up_hbm, raw.at[1]), (decay_re, dr_ref), (decay_im, di_ref),
             (log_step, ls_ref), (x_hbm, x_raw), (in_re, inr_ref), (in_im, ini_ref),
             (out_re, outr_ref), (out_im, outi_ref), (down_hbm, down_ref), (skip_hbm, k_ref),
             (wo_hbm, wo_ref), (residual_hbm, res_ref), (gain_hbm, gain_ref))
    loads = [pltpu.make_async_copy(a, b, load_sem.at[i]) for i, (a, b) in enumerate(pairs)]
    for copy in loads:
        copy.start()
    exact = lax.Precision.HIGHEST

    def flip_weights(w):
        for i in range(raw.shape[2] // depth):
            turned[w, i * depth:(i + 1) * depth, :] = raw[w, :, i * depth:(i + 1) * depth].T

    with jax.named_scope("A_flip"):
        loads[0].wait()
        flip_weights(0)
    with jax.named_scope("A_barrier"):
        pl.semaphore_wait(barrier, n)
    loads[10].wait()
    if pitch > slab:
        for w in range(2):
            joined[w * pitch + slab:(w + 1) * pitch, :] = jnp.zeros(
                (pitch - slab, joined.shape[1]), BF16)

    def send_inner(w, s):
        @pl.when(inner)
        def _():
            send_b(w, s)

    send_x(0, 1)
    send_z(0, 0)
    send_y(0, 0)
    send_inner(0, 0)
    send_c(0, 0, 1)
    with jax.named_scope("A_param"):
        for copy in loads[2:5]:
            copy.wait()
        states = sb // GATHER
        spread = (lax.rem(iota((states, sb), 1), states) == iota((states, sb), 0)).astype(F32)
        chosen = lax.div(iota((GATHER, sb), 1), states) == iota((GATHER, sb), 0)
        for b in range(blocks):
            def lanes(ref):
                wide = jnp.dot(ref[b * GATHER:(b + 1) * GATHER, :], spread, precision=exact,
                               preferred_element_type=F32)
                return jnp.sum(jnp.where(chosen, wide, 0.0), axis=0, keepdims=True)

            groups = ls_ref.shape[1]
            group = (lax.div(iota((groups, sb), 1), states) + b * GATHER
                     == iota((groups, sb), 0)).astype(F32)
            step_size = jnp.exp(jnp.dot(ls_ref[...], group, precision=exact,
                                        preferred_element_type=F32))
            re, im = lanes(dr_ref), lanes(di_ref)
            magnitude = jnp.exp(re * step_size)
            angle = im * step_size
            power_re = magnitude * jnp.cos(angle)
            power_im = magnitude * jnp.sin(angle)
            denom = re * re + im * im
            a_ref[b, 0:1, :] = power_re
            a_ref[b, 1:2, :] = power_im
            ratio[b, 0:1, :] = ((power_re - 1.0) * re + power_im * im) / denom
            ratio[b, 1:2, :] = (power_im * re - (power_re - 1.0) * im) / denom
    with jax.named_scope("A_x"):
        square = (rows, rows)
        source = lax.rem(iota(square, 0), span) * CHUNKS + lax.div(iota(square, 0), span)
        turn[...] = (iota(square, 1) == source).astype(BF16)
        loads[5].wait()
        for b in range(blocks):
            x_ref[b] = lax.dot_general(
                turn[...], x_raw[:, b * cb:(b + 1) * cb], (((0,), (0,)), ((), ())),
                preferred_element_type=F32,
            ).astype(BF16)
    with jax.named_scope("A_flip1"):
        loads[1].wait()
        flip_weights(1)
        for copy in loads[6:10]:
            copy.wait()

    local = []
    for w in range(3):
        copy = pltpu.make_async_copy(own(w), spot(w, 0), local_sem.at[w])
        copy.start()
        local.append(copy)

    def scan(b, start, keep):
        work[...] = jnp.dot(x_ref[b], read_in[b], preferred_element_type=F32)
        br = jnp.broadcast_to(a_ref[b, 0:1, :], (CHUNKS, sb))
        bi = jnp.broadcast_to(a_ref[b, 1:2, :], (CHUNKS, sb))

        def step(i, state):
            at = pl.ds(pl.multiple_of(i * CHUNKS, CHUNKS), CHUNKS)
            nr, ni = cmul(br, bi, *state)
            nr, ni = nr + work[at, :sb], ni + work[at, sb:]
            if keep:
                work[at, :sb] = nr
                work[at, sb:] = ni
            return nr, ni

        return lax.fori_loop(0, span, step, start, unroll=8)

    size = cb // GATHER
    spread_narrow = spread.astype(BF16)
    with jax.named_scope("B_scan1"):
        @pl.loop(0, blocks)
        def _(b):
            keep = lax.div(iota((cb, sb), 0), size) == lax.div(iota((cb, sb), 1), states)
            at = pl.ds(pl.multiple_of(b * cb, cb), cb)
            def widen(ref):
                high = ref[at, :].astype(BF16)
                low = (ref[at, :] - high.astype(F32)).astype(BF16)
                return (jnp.dot(high, spread_narrow, preferred_element_type=F32)
                        + jnp.dot(low, spread_narrow, preferred_element_type=F32))

            vr, vi = widen(inr_ref), widen(ini_ref)
            cr, ci = ratio[b, 0:1, :], ratio[b, 1:2, :]
            read_in[b, :, :sb] = jnp.where(keep, cr * vr - ci * vi, 0.0).astype(BF16)
            read_in[b, :, sb:] = jnp.where(keep, cr * vi + ci * vr, 0.0).astype(BF16)
            zero = jnp.zeros((CHUNKS, sb), F32)
            sr, si = scan(b, (zero, zero), False)
            ends[b, :, :sb] = sr
            ends[b, :, sb:] = si
            lr, li = cpow(a_ref[b, 0:1, :], a_ref[b, 1:2, :], span)
            er, ei = sr[0:1], si[0:1]
            for chunk in range(1, CHUNKS):
                er, ei = cmul(lr, li, er, ei)
                er, ei = er + sr[chunk:chunk + 1], ei + si[chunk:chunk + 1]
            total[b, :, :sb] = er
            total[b, :, sb:] = ei

    def pass_z(w, s):
        with jax.named_scope(f"z{w}{s}"):
            wait_z(w, s)

        @pl.when(inner)
        def _():
            relay(w, s)

        send_y(w, 2 + s)

    def pass_e(w, s):
        with jax.named_scope(f"e{w}{s}"):
            wait_e(w, s)
        send_y(w, 4 + s)

    def pass_l(w, s):
        with jax.named_scope(f"l{w}{s}"):
            wait_l(w, s)
        send_y(w, 6 + s)

    here = m * 2 + v
    level = h * 2 + u
    for k, there in enumerate((to_x, to_y, (h, u, om, ov, core))):
        send(total, gathered.at[here], there, ("s", k))
    gathered[here] = total[...]
    send_x(0, 0)
    for w in (1, 2):
        for s in (1, 0):
            send_x(w, s)
    send_y(1, 0)
    send_y(2, 0)
    with jax.named_scope("C_readout"):
        @pl.loop(0, blocks)
        def _(b):
            high = (lax.rem(iota((sb, states), 0), states) == iota((sb, states), 1)).astype(BF16)
            keep = lax.div(iota((sb, cb), 0), states) == lax.div(iota((sb, cb), 1), size)
            at = pl.ds(pl.multiple_of(b * cb, cb), cb)
            for place_in, ref, sign in ((0, outr_ref, 1.0), (1, outi_ref, -1.0)):
                wide = lax.dot_general(high, (sign * ref[at, :]).astype(BF16), across,
                                       preferred_element_type=F32)
                read_out[b, place_in * sb:(place_in + 1) * sb, :] = jnp.where(
                    keep, wide, 0.0).astype(BF16)

    with jax.named_scope("C_states1"):
        for k, (a, b) in enumerate(((m, ov), (om, v), (om, ov))):
            arrive(gathered.at[a * 2 + b], to_x, ("s", k))

    def power_of(b, count):
        return cpow(a_ref[b, 0:1, :], a_ref[b, 1:2, :], count)

    @pl.loop(0, blocks)
    def _(b):
        tr, ti = power_of(b, span * CHUNKS)
        hr = jnp.zeros((1, sb), F32)
        hi, pr, pi = hr, hr, hr
        for device in range(4):
            gr, gi = gathered[device, b, :, :sb], gathered[device, b, :, sb:]
            nr, ni = cmul(tr, ti, hr, hi)
            hr = jnp.where(device < here, nr + gr, hr)
            hi = jnp.where(device < here, ni + gi, hi)
            nr, ni = cmul(tr, ti, pr, pi)
            pr, pi = nr + gr, ni + gi
        prefix[b, :, :sb] = hr
        prefix[b, :, sb:] = hi
        plane_total[b, :, :sb] = pr
        plane_total[b, :, sb:] = pi

    for k, (a, b) in enumerate(((h, ou), (oh, u), (oh, ou))):
        send(plane_total, planes.at[level], (a, b, m, v, core), ("plane", k))
    planes[level] = plane_total[...]
    with jax.named_scope("C_x01"):
        wait_x(0, 1)
    send_z(0, 1)
    send_inner(0, 1)
    send_c(0, 0, 0)
    for copy in loads[11:]:
        copy.wait()
    pass_z(0, 0)
    with jax.named_scope("C_states2"):
        for k, (a, b) in enumerate(((h, ou), (oh, u), (oh, ou))):
            arrive(planes.at[a * 2 + b], to_x, ("plane", k))
    with jax.named_scope("C_x00"):
        wait_x(0, 0)
    send_c(0, 1, 0)
    send_c(0, 1, 1)
    send_y(0, 1)
    send_z(1, 0)
    send_inner(1, 0)

    def second(b):
        lr, li = power_of(b, span)
        tr, ti = cpow(lr, li, CHUNKS)
        qr, qi = cpow(tr, ti, 4)
        hr = jnp.zeros((1, sb), F32)
        hi = hr
        for other in range(3):
            nr, ni = cmul(qr, qi, hr, hi)
            hr = jnp.where(other < level, nr + planes[other, b, :, :sb], hr)
            hi = jnp.where(other < level, ni + planes[other, b, :, sb:], hi)
        for device in range(3):
            nr, ni = cmul(tr, ti, hr, hi)
            hr, hi = jnp.where(device < here, nr, hr), jnp.where(device < here, ni, hi)
        hr, hi = hr + prefix[b, :, :sb], hi + prefix[b, :, sb:]
        starts_r, starts_i = [hr], [hi]
        for chunk in range(CHUNKS - 1):
            nr, ni = cmul(lr, li, hr, hi)
            hr = nr + ends[b, chunk:chunk + 1, :sb]
            hi = ni + ends[b, chunk:chunk + 1, sb:]
            starts_r.append(hr)
            starts_i.append(hi)
        scan(b, (jnp.concatenate(starts_r, axis=0), jnp.concatenate(starts_i, axis=0)), True)
        mixed = jnp.dot(work[...].astype(BF16), read_out[b], preferred_element_type=F32)
        at = pl.ds(pl.multiple_of(b * cb, cb), cb)
        mixed = mixed + k_ref[:, at] * x_ref[b].astype(F32)
        mixed = jax.nn.gelu(mixed).astype(BF16)
        act[:, at] = jnp.dot(
            turn[...], mixed, preferred_element_type=F32
        ).astype(BF16)

    with jax.named_scope("D_scan2a"):
        @pl.loop(0, blocks // 2)
        def _(b):
            second(b)

    pass_z(0, 1)
    with jax.named_scope("D_x11"):
        wait_x(1, 1)
    send_z(1, 1)
    send_inner(1, 1)
    with jax.named_scope("D_scan2b"):
        @pl.loop(blocks // 2, blocks)
        def _(b):
            second(b)

    with jax.named_scope("D_x10"):
        wait_x(1, 0)
    send_y(1, 1)
    send_c(1, 0, 1)
    send_c(1, 1, 1)

    tile = min(512, width)
    with jax.named_scope("E_outproj"):
        for t in (1, 0):
            to = core if t == 0 else 1 - core

            @pl.loop(0, width // tile)
            def _(j):
                at = pl.ds(pl.multiple_of(j * tile, tile), tile)
                share[t, :, at] = jnp.dot(
                    act[pl.ds(pl.multiple_of(to * keep_rows, keep_rows), keep_rows), :],
                    wo_ref[:, at], preferred_element_type=F32,
                ).astype(BF16)

            if t:
                send(share.at[1], others, to_t, ("mix",))

    with jax.named_scope("G_mix"):
        arrive(others, to_t, ("mix",))
    line = min(32, keep_rows)
    with jax.named_scope("H_norm"):
        @pl.loop(0, keep_rows // line)
        def _(i):
            at = pl.ds(pl.multiple_of(i * line, line), line)
            mixed = share[0, at, :].astype(F32) + others[at, :].astype(F32)
            carried = res_ref[at, :].astype(F32) + mixed.astype(BF16).astype(F32)
            scale = lax.rsqrt(jnp.mean(carried * carried, axis=-1, keepdims=True) + 1e-06)
            carried_ref[at, :] = carried
            rows_ref[0, 0, at, :] = (carried * scale * gain_ref[...]).astype(BF16)

    send(rows_ref.at[0, 0], rows_ref.at[0, 1], to_x, ("r", 1), moves)
    piece = keep_rows // PIECES
    for part in range(PIECES):
        at = pl.ds(part * piece, piece)
        send(rows_ref.at[0, 0, at], rows_ref.at[0, 2, at], to_z, ("r", 2, part), moves)
    send(rows_ref.at[0, 0], rows_ref.at[1, 0], to_t, ("t", 0), moves)

    def share_core(k):
        send(rows_ref.at[0, k], rows_ref.at[1, k], to_t, ("t", k), moves)

    def wait_core(k):
        arrive(rows_ref.at[1, k], to_t, ("t", k))

    def product(k, at):
        block = rows_ref[:, k].reshape(2 * keep_rows, width)
        return lax.dot_general(block, joined[at, :], across, preferred_element_type=F32)

    def keep_hidden(k, gate, up):
        result = (jax.nn.silu(gate) * up).astype(BF16)
        for t in range(2):
            hidden[pl.ds((4 * t + k) * keep_rows, keep_rows), :] = (
                result[t * keep_rows:(t + 1) * keep_rows])

    def gate_part(k):
        with jax.named_scope(f"gate{k}"):
            gates[k] = product(k, pl.ds(0, slab))

    def up_part(k):
        with jax.named_scope(f"up{k}"):
            keep_hidden(k, gates[k], product(k, pl.ds(pitch, slab)))

    def both_parts(k):
        with jax.named_scope(f"both{k}"):
            result = product(k, pl.ds(0, 2 * pitch))
            keep_hidden(k, result[:, :slab], result[:, pitch:pitch + slab])

    def first_rows():
        with jax.named_scope("r1"):
            arrive(rows_ref.at[0, 1], to_x, ("r", 1))
        share_core(1)

    def relay_rows(part):
        at = pl.ds(part * piece, piece)
        with jax.named_scope(f"r2{part}"):
            arrive(rows_ref.at[0, 2, at], to_z, ("r", 2, part))
        send(rows_ref.at[0, 2, at], rows_ref.at[0, 3, at], to_x, ("r", 3, part), moves)
        if part == PIECES - 1:
            share_core(2)

    def last_rows():
        with jax.named_scope("r3"):
            for part in range(PIECES):
                at = pl.ds(part * piece, piece)
                arrive(rows_ref.at[0, 3, at], to_x, ("r", 3, part))
        share_core(3)

    def second_weights():
        send_inner(2, 0)
        wait_x(2, 1)
        send_inner(2, 1)
        send_z(2, 0)
        send_z(2, 1)
        wait_x(2, 0)
        send_y(2, 1)
        send_c(2, 0, 0)
        send_c(2, 1, 0)

    def delayed_weights():
        send_c(2, 0, 1)
        send_c(2, 1, 1)

    def whole(w):
        with jax.named_scope(f"y{w}"):
            for j in range(8):
                wait_y(w, j)

    def core_rows(k):
        with jax.named_scope(f"t{k}"):
            wait_core(k)

    for s in range(2):
        send_c(1, s, 0)
    pass_e(0, 0)
    pass_e(0, 1)
    pass_z(1, 0)
    pass_z(1, 1)
    pass_l(0, 0)
    pass_l(0, 1)
    pass_e(1, 0)
    for copy in local:
        copy.wait()
    whole(0)
    core_rows(0)
    gate_part(0)
    first_rows()
    second_weights()
    relay_rows(0)
    pass_e(1, 1)
    relay_rows(1)
    core_rows(1)
    gate_part(1)
    pass_l(1, 0)
    pass_l(1, 1)
    delayed_weights()
    relay_rows(2)
    whole(1)
    up_part(0)
    relay_rows(3)
    up_part(1)
    core_rows(2)
    pass_z(2, 0)
    both_parts(2)
    last_rows()
    pass_z(2, 1)
    core_rows(3)
    both_parts(3)
    pass_e(2, 0)
    with jax.named_scope("moves"):
        for copy in moves:
            copy.wait_send()

    across_u = width // 8
    chunks = [(h, h, m), (h, oh, m), (h, h, om), (h, oh, om), (oh, h, m), (oh, oh, m),
              (oh, h, om), (oh, oh, om)]

    def columns(j):
        a, b, c = chunks[j]
        return pl.ds(pl.multiple_of(index(a, b, c, 0) * depth, across_u), across_u)

    def down(j):
        pair_of = (2 * j, 2 * j + 1)
        right = jnp.concatenate([down_full[:, columns(i)] for i in pair_of], axis=1)
        for t in (1, 0):
            result = jnp.dot(
                hidden[4 * t * keep_rows:4 * (t + 1) * keep_rows, :], right,
                preferred_element_type=F32,
            ).astype(BF16)
            for side, i in enumerate(pair_of):
                for k in range(4):
                    rows_ref[t, k, :, columns(i)] = result[
                        k * keep_rows:(k + 1) * keep_rows, side * across_u:(side + 1) * across_u]
                if t:
                    send(rows_ref.at[1, :, :, columns(i)], partners.at[i], to_t, ("p", i), group="p")

    def add(target, j, other):
        at = columns(j)

        @pl.loop(0, keep_rows // line)
        def _(i):
            lines = pl.ds(pl.multiple_of(i * line, line), line)
            rows_ref[0, target, lines, at] = (
                rows_ref[0, target, lines, at].astype(F32) + other[lines, :].astype(F32)
            ).astype(BF16)

    def pair(j):
        at = columns(j)
        near, far = (1, 2) if X_FIRST[j] else (2, 1)
        device = to_x if X_FIRST[j] else to_z
        arrive(partners.at[j], to_t, ("p", j))
        for place_in, k in enumerate((3, near)):
            add(k, j, partners.at[j, k])
            send(rows_ref.at[0, k, :, at], firsts.at[j, place_in], device, ("f", j, place_in), group="f")
        add(far, j, partners.at[j, far])
        add(0, j, partners.at[j, 0])

    def combine(j):
        at = columns(j)
        far = 2 if X_FIRST[j] else 1
        device, other = (to_x, to_z) if X_FIRST[j] else (to_z, to_x)
        arrive(firsts.at[j, 0], device, ("f", j, 0))
        add(far, j, firsts.at[j, 0])
        send(rows_ref.at[0, far, :, at], seconds.at[j], other, ("g", j), group="g")
        arrive(firsts.at[j, 1], device, ("f", j, 1))
        add(0, j, firsts.at[j, 1])

    stored = []

    def finish(j):
        at = columns(j)
        arrive(seconds.at[j], to_z if X_FIRST[j] else to_x, ("g", j))

        @pl.loop(0, keep_rows // line)
        def _(i):
            lines = pl.ds(pl.multiple_of(i * line, line), line)
            summed = rows_ref[0, 0, lines, at].astype(F32) + seconds[j, lines, :].astype(F32)
            summed = summed.astype(BF16).astype(F32)
            out_ref[lines, at] = (carried_ref[lines, at] + 0.5 * summed).astype(BF16)

        copy = pltpu.make_async_copy(out_ref.at[:, at], out_hbm.at[:, at], out_sem.at[j])
        copy.start()
        stored.append(copy)

    order = ORDER
    stages = {"d": down, "p": pair, "c": combine, "f": finish}
    for word in order:
        if word == "e":
            pass_e(2, 1)
            continue
        if word == "l":
            pass_l(2, 0)
            pass_l(2, 1)
            continue
        j = int(word[1])
        if word in ("d1", "d3"):
            with jax.named_scope("y2" + word):
                for i in range(4 * (j // 2), 4 * (j // 2) + 4):
                    wait_y(2, i)
        with jax.named_scope({"d": "down", "p": "pair", "c": "comb", "f": "fin"}[word[0]] + word[1]):
            stages[word[0]](j)
    def drain(group, ref):
        describe(ref, ref, to_x, ("mix",), fixed[group]).wait_send()

    with jax.named_scope("end_sends"):
        for copy in everywhere:
            copy.wait_send()
        for w in range(3):
            drain(("w", w), down_full.at[:, pl.ds(0, groups_of["w", w] * depth)])
        drain("p", partners)
        drain("f", firsts)
        drain("g", seconds)

        @pl.when(inner)
        def _():
            drain("inside", down_full.at[:, pl.ds(0, groups_of["inside"] * depth)])

    with jax.named_scope("end_store"):
        for copy in stored:
            copy.wait()


def shift(value, axis, count, by):
    return lax.ppermute(value, axis, [(i, (i + by) % count) for i in range(count)])


def flip(value, axes, count, k):
    return lax.ppermute(value, axes, [(i, i ^ k) for i in range(count)])


def on_device(sizes, mixer_in, residual, decay_real, decay_imag, log_step, in_real, in_imag,
              output_real, output_imaginary, skip, out_proj, norm_gain, w_gate, w_up, w_down):
    tp, nh, nm = sizes["tp"], sizes["h"], sizes["m"]
    n = nh * 4 * nm
    rows, channels = mixer_in.shape
    keep_rows, width = residual.shape
    depth, hidden_units = w_gate.shape
    part = hidden_units // 4
    groups, states = decay_real.shape
    blocks = groups // GATHER
    cb, sb = channels // blocks, GATHER * states
    vmem = pl.BlockSpec(memory_space=pltpu.VMEM)
    if depth % 128 == 0 and (tp, nh, nm) == (2, 2, 2):
        cut = width // 8
        pitch = -(-part // 128) * 128
        return pl.pallas_call(
            functools.partial(streamed, sizes),
            in_specs=[pl.BlockSpec(memory_space=pl.ANY)] * 15,
            out_specs=pl.BlockSpec(memory_space=pl.ANY),
            out_shape=jax.ShapeDtypeStruct((keep_rows, width), BF16),
            scratch_shapes=[
                pltpu.VMEM((keep_rows, width), BF16),
                pltpu.SemaphoreType.DMA((8,)),
                pltpu.VMEM((2 * pitch, n * depth), BF16),
                pltpu.VMEM((part, n * depth), BF16),
                pltpu.VMEM((3, part, depth), BF16),
                pltpu.VMEM((2, 4, keep_rows, width), BF16),
                pltpu.VMEM((keep_rows, width), F32),
                pltpu.VMEM((4, 2 * keep_rows, part), F32),
                pltpu.VMEM((8 * keep_rows, part), BF16),
                pltpu.VMEM((8, 4, keep_rows, cut), BF16),
                pltpu.VMEM((8, 2, keep_rows, cut), BF16),
                pltpu.VMEM((8, keep_rows, cut), BF16),
                pltpu.VMEM((rows, 2 * sb), F32),
                pltpu.VMEM((blocks, cb, 2 * sb), BF16),
                pltpu.VMEM((blocks, 2 * sb, cb), BF16),
                pltpu.VMEM((blocks, CHUNKS, 2 * sb), F32),
                pltpu.VMEM((blocks, 1, 2 * sb), F32),
                pltpu.VMEM((4, blocks, 1, 2 * sb), F32),
                pltpu.VMEM((blocks, 1, 2 * sb), F32),
                pltpu.VMEM((blocks, 1, 2 * sb), F32),
                pltpu.VMEM((4, blocks, 1, 2 * sb), F32),
                pltpu.VMEM((rows, rows), BF16),
                pltpu.VMEM((rows, channels), BF16),
                pltpu.VMEM((2, keep_rows, width), BF16),
                pltpu.VMEM((keep_rows, width), BF16),
                pltpu.VMEM((rows, channels), BF16),
                pltpu.VMEM((blocks, rows, cb), BF16),
                pltpu.VMEM((keep_rows, width), BF16),
                *[pltpu.VMEM((groups, states), F32)] * 2,
                pltpu.VMEM((1, groups), F32),
                *[pltpu.VMEM((channels, states), F32)] * 4,
                pltpu.VMEM((1, channels), F32),
                pltpu.VMEM((channels, width), BF16),
                pltpu.VMEM((1, width), F32),
                pltpu.VMEM((2, depth, hidden_units), BF16),
                pltpu.VMEM((2, hidden_units, depth), BF16),
                pltpu.VMEM((hidden_units, depth), BF16),
                pltpu.VMEM((blocks, 2, sb), F32),
                pltpu.VMEM((blocks, 2, sb), F32),
                pltpu.SemaphoreType.DMA((27,)),
                pltpu.SemaphoreType.DMA((100,)),
                pltpu.SemaphoreType.DMA((3,)),
                pltpu.SemaphoreType.DMA((15,)),
            ],
            compiler_params=pltpu.CompilerParams(
                collective_id=0, has_side_effects=True, vmem_limit_bytes=62 * 2**20
            ),
            name="streamed",
        )(mixer_in, residual, decay_real, decay_imag, log_step.reshape(1, groups),
          in_real.transpose(0, 2, 1).reshape(channels, states),
          in_imag.transpose(0, 2, 1).reshape(channels, states),
          output_real.reshape(channels, states), output_imaginary.reshape(channels, states),
          skip.reshape(1, channels), out_proj, norm_gain.reshape(1, width), w_gate, w_up, w_down)
    power_re, power_im, bar_re, bar_im = discrete(
        decay_real, decay_imag, log_step, in_real, in_imag
    )
    rows_first = lambda t: jnp.transpose(t, (0, 2, 1)).reshape(blocks, -1, t.shape[1])
    read_in = jnp.stack([rows_first(bar_re), rows_first(bar_im)], axis=1).astype(BF16)
    read_out = jnp.stack(
        [rows_first(output_real), -rows_first(output_imaginary)], axis=1
    ).astype(BF16)
    power = jnp.stack([power_re.reshape(blocks, sb), power_im.reshape(blocks, sb)], axis=1)
    x = mixer_in.reshape(CHUNKS, rows // CHUNKS, blocks, cb).transpose(2, 1, 0, 3)
    x = x.reshape(blocks, rows, cb)
    operands = (x, read_in, read_out, power, skip.reshape(blocks, 1, cb), out_proj, residual,
                norm_gain.reshape(1, width), w_gate.T.reshape(4, part, depth),
                w_up.T.reshape(4, part, depth), w_down.reshape(4, part, depth))
    copies = 3 * (3 + 4 * (nh - 1) + 4 * nh * (nm - 1)) + (n - 1) + (tp - 1) + 3 + 4 * (tp - 1)
    laid = (part, n * depth) if depth % 128 == 0 else (n, part, depth)
    between = [(laid, BF16)] * 3 + [
        ((tp, 4, keep_rows, width), BF16), ((keep_rows, width), F32),
    ]
    fused = depth % 128 == 0
    if fused:
        copies += 4 * (tp - 1) + 3
        out_shape = [jax.ShapeDtypeStruct((keep_rows, width), BF16)]
        extra = [
            pltpu.VMEM((4 * tp, keep_rows, part), BF16),
            pltpu.VMEM((4, tp - 1, keep_rows, width), BF16),
            pltpu.VMEM((3, keep_rows, width), BF16),
            *(pltpu.VMEM(*item) for item in between),
        ]
    else:
        out_shape = [jax.ShapeDtypeStruct(*item) for item in between]
        extra = []
    results = pl.pallas_call(
        functools.partial(layer, sizes, fused),
        in_specs=[vmem] * 11,
        out_specs=[vmem] * len(out_shape),
        out_shape=out_shape,
        scratch_shapes=[
            *extra,
            pltpu.VMEM((rows, 2 * sb), F32),
            pltpu.VMEM((blocks, cb, 2 * sb), BF16),
            pltpu.VMEM((blocks, 2 * sb, cb), BF16),
            pltpu.VMEM((blocks, CHUNKS, 2 * sb), F32),
            pltpu.VMEM((blocks, 1, 2 * sb), F32),
            pltpu.VMEM((n, blocks, 1, 2 * sb), F32),
            pltpu.VMEM((rows, channels), BF16),
            pltpu.VMEM((tp, keep_rows, width), BF16),
            pltpu.VMEM((tp - 1, keep_rows, width), BF16),
            pltpu.SemaphoreType.DMA((copies,)),
            pltpu.SemaphoreType.DMA((copies,)),
            pltpu.SemaphoreType.DMA((3,)),
        ],
        compiler_params=pltpu.CompilerParams(
            collective_id=0, has_side_effects=True, vmem_limit_bytes=62 * 2**20
        ),
        name="layer",
    )(*operands)
    if fused:
        return results[0]
    full_gate, full_up, full_down, rows_all, carried = results
    if len(laid) == 3:
        full_gate, full_up, full_down = (
            t.transpose(1, 0, 2).reshape(part, width) for t in (full_gate, full_up, full_down)
        )

    flat = rows_all.reshape(-1, width)
    across = (((1,), (1,)), ((), ()))
    gate = lax.dot_general(flat, full_gate, across, preferred_element_type=F32)
    up = lax.dot_general(flat, full_up, across, preferred_element_type=F32)
    hidden = (jax.nn.silu(gate) * up).astype(BF16)
    down = jnp.dot(hidden, full_down, preferred_element_type=F32).astype(BF16)
    down = down.reshape(rows_all.shape)
    summed = down[0].astype(F32)
    for t in range(1, tp):
        summed = summed + shift(down[t], "tp", tp, -t).astype(F32)
    summed = summed.astype(BF16)
    total = summed[0].astype(F32)
    for k in range(1, 4):
        total = total + flip(summed[k], PEERS, 4, k).astype(F32)
    total = total.astype(BF16)
    return (carried + 0.5 * total.astype(F32)).astype(BF16)


def solution(mesh):
    sp, tp = mesh.shape["sp"], mesh.shape["tp"]
    sizes = {"h": sp // 8, "u": 2, "m": 2, "v": 2, "tp": tp}
    cut = Mesh(mesh.devices.reshape(tuple(sizes.values())), tuple(sizes))
    return jax.shard_map(
        functools.partial(on_device, sizes),
        mesh=cut,
        in_specs=(
            P(SP, "tp"),
            P((*SP, "tp"), None),
            P("tp", None),
            P("tp", None),
            P("tp"),
            P("tp", None, None),
            P("tp", None, None),
            P("tp", None, None),
            P("tp", None, None),
            P("tp"),
            P("tp", None),
            P(),
            P(SP, "tp"),
            P(SP, "tp"),
            P("tp", SP),
        ),
        out_specs=P((*SP, "tp"), None),
        check_vma=False,
    )
```

```python
import functools

import jax
import jax.numpy as jnp
from jax import lax
from jax.experimental import pallas as pl
from jax.experimental.pallas import tpu as pltpu
from jax.sharding import Mesh
from jax.sharding import PartitionSpec as P

F32 = jnp.float32
BF16 = jnp.bfloat16
SP = ("h", "u", "m", "v")
PEERS = ("u", "v")
GATHER = 8
CHUNKS = 8
X_FIRST = (1, 1, 1, 0, 1, 0, 1, 0)
PIECES = 4
ORDER = ("d0", "e", "p0", "p1", "d1", "p2", "p3", "l", "d2", "p4", "p5", "c0", "c1", "d3", "p6",
         "p7", "c2", "c3", "c4", "c5", "f0", "f1", "c6", "c7", "f2", "f3", "f4", "f5", "f6", "f7")
MESH = pl.DeviceIdType.MESH


def discrete(decay_real, decay_imag, log_step, in_real, in_imag):
    step_size = jnp.exp(log_step)[:, None]
    magnitude = jnp.exp(decay_real * step_size)
    angle = decay_imag * step_size
    power_re = magnitude * jnp.cos(angle)
    power_im = magnitude * jnp.sin(angle)
    denom = decay_real * decay_real + decay_imag * decay_imag
    ratio_re = ((power_re - 1.0) * decay_real + power_im * decay_imag) / denom
    ratio_im = (power_im * decay_real - (power_re - 1.0) * decay_imag) / denom
    drive_re = ratio_re[..., None] * in_real - ratio_im[..., None] * in_imag
    drive_im = ratio_re[..., None] * in_imag + ratio_im[..., None] * in_real
    return (power_re, power_im, drive_re, drive_im)


def cmul(ar, ai, br, bi):
    return ar * br - ai * bi, ar * bi + ai * br


def cpow(ar, ai, count):
    result = None
    while count:
        if count & 1:
            result = (ar, ai) if result is None else cmul(*result, ar, ai)
        count >>= 1
        if count:
            ar, ai = cmul(ar, ai, ar, ai)
    return result


def iota(shape, dim):
    return lax.broadcasted_iota(jnp.int32, shape, dim)


def tiled(block, copies, across, down):
    rows, columns = block.shape
    wide = (columns, columns * copies)
    pick = (iota(wide, 0) == lax.rem(iota(wide, 1), columns)).astype(BF16)
    full = jnp.dot(block, pick, preferred_element_type=F32)
    keep = lax.div(iota(full.shape, 0), down) == lax.div(iota(full.shape, 1), across)
    return jnp.where(keep, full, 0.0).astype(BF16)


def layer(sizes, fused, x_ref, b_ref, c_ref, a_ref, k_ref, wo_ref, res_ref, gain_ref, *rest):
    quarters, rest = rest[:3], rest[3:]
    if fused:
        out_ref, *rest = rest
        hidden, partners, peers, *rest = rest
    weights, (rows_ref, carried_ref), rest = rest[:3], rest[3:5], rest[5:]
    (work, read_in, read_out, ends, total, gathered, act, share, others,
     send_sem, recv_sem, local_sem) = rest
    blocks, rows, cb = x_ref.shape
    sb = a_ref.shape[2]
    depth = quarters[0].shape[2]
    width = wo_ref.shape[1]
    span = rows // CHUNKS
    nh, nm, tp = sizes["h"], sizes["m"], sizes["tp"]
    n = nh * 4 * nm
    h, u, m, v, core = (lax.axis_index(name) for name in (*SP, "tp"))
    index = lambda h, u, m, v: ((h * 2 + u) * nm + m) * 2 + v
    me = index(h, u, m, v)
    peer = lambda k: (1 - u if k & 2 else u, 1 - v if k & 1 else v)
    counter = iter(range(send_sem.shape[0]))

    def send(src, dst, device):
        slot = next(counter)
        copy = pltpu.make_async_remote_copy(
            src_ref=src, dst_ref=dst, send_sem=send_sem.at[slot], recv_sem=recv_sem.at[slot],
            device_id=device, device_id_type=MESH,
        )
        copy.start()
        return copy

    def place(ref, position):
        if depth % 128:
            return ref.at[position]
        return ref.at[:, pl.ds(pl.multiple_of(position * depth, depth), depth)]

    barrier = pltpu.get_barrier_semaphore()
    others_sp = []
    for k in range(1, n):
        to = lax.rem(me + k, n)
        there = (lax.div(to, 4 * nm), lax.rem(lax.div(to, 2 * nm), 2),
                 lax.rem(lax.div(to, 2), nm), lax.rem(to, 2), core)
        others_sp.append(there)
        pl.semaphore_signal(barrier, inc=1, device_id=there, device_id_type=MESH)
    for t in range(1, tp):
        pl.semaphore_signal(
            barrier, inc=1, device_id=(h, u, m, v, lax.rem(core + t, tp)), device_id_type=MESH
        )
    pl.semaphore_wait(barrier, n - 1 + tp - 1)

    sent = []
    first = {}
    over_h = {}
    over_m = {}

    def spread_h(w, k, src, position):
        for r in range(1, nh):
            pu, pv = peer(k)
            copy = send(src, place(weights[w], position), (lax.rem(h + r, nh), u, m, v, core))
            over_h[w, k, r] = copy

    def spread_m(w, k, r, src, position):
        for s in range(1, nm):
            over_m[w, k, r, s] = send(
                src, place(weights[w], position), (h, u, lax.rem(m + s, nm), v, core)
            )

    own = u * 2 + v
    for w in range(3):
        for k in (3, 1, 2):
            pu, pv = peer(k)
            first[w, k] = send(
                quarters[w].at[pu * 2 + pv], place(weights[w], me), (h, pu, m, pv, core)
            )
    locals_ = []
    for w in range(3):
        spread_h(w, 0, quarters[w].at[own], me)
        spread_m(w, 0, 0, quarters[w].at[own], me)
        copy = pltpu.make_async_copy(quarters[w].at[own], place(weights[w], me), local_sem.at[w])
        copy.start()
        locals_.append(copy)

    def scan(b, start, keep):
        work[...] = jnp.dot(x_ref[b], read_in[b], preferred_element_type=F32)
        br = jnp.broadcast_to(a_ref[b, 0:1, :], (CHUNKS, sb))
        bi = jnp.broadcast_to(a_ref[b, 1:2, :], (CHUNKS, sb))

        def step(i, state):
            at = pl.ds(pl.multiple_of(i * CHUNKS, CHUNKS), CHUNKS)
            nr, ni = cmul(br, bi, *state)
            nr, ni = nr + work[at, :sb], ni + work[at, sb:]
            if keep:
                work[at, :sb] = nr
                work[at, sb:] = ni
            return nr, ni

        return lax.fori_loop(0, span, step, start, unroll=8)

    @pl.loop(0, blocks)
    def _(b):
        states = b_ref.shape[3]
        for half in range(2):
            read_in[b, :, half * sb:(half + 1) * sb] = tiled(
                b_ref[b, half], GATHER, states, cb // GATHER
            )
            read_out[b, half * sb:(half + 1) * sb, :] = tiled(
                c_ref[b, half], GATHER, cb // GATHER, states
            )
        zero = jnp.zeros((CHUNKS, sb), F32)
        sr, si = scan(b, (zero, zero), False)
        ends[b, :, :sb] = sr
        ends[b, :, sb:] = si
        lr, li = cpow(a_ref[b, 0:1, :], a_ref[b, 1:2, :], span)
        er, ei = sr[0:1], si[0:1]
        for chunk in range(1, CHUNKS):
            er, ei = cmul(lr, li, er, ei)
            er, ei = er + sr[chunk:chunk + 1], ei + si[chunk:chunk + 1]
        total[b, :, :sb] = er
        total[b, :, sb:] = ei

    states_out = [send(total, gathered.at[me], there) for there in others_sp]
    gathered[me] = total[...]
    for copy in states_out:
        copy.wait_recv()

    @pl.loop(0, blocks)
    def _(b):
        lr, li = cpow(a_ref[b, 0:1, :], a_ref[b, 1:2, :], span)
        tr, ti = cpow(lr, li, CHUNKS)
        hr = jnp.zeros((1, sb), F32)
        hi = hr
        for device in range(n - 1):
            nr, ni = cmul(tr, ti, hr, hi)
            nr = nr + gathered[device, b, :, :sb]
            ni = ni + gathered[device, b, :, sb:]
            hr, hi = jnp.where(device < me, nr, hr), jnp.where(device < me, ni, hi)
        starts_r, starts_i = [hr], [hi]
        for chunk in range(CHUNKS - 1):
            nr, ni = cmul(lr, li, hr, hi)
            hr = nr + ends[b, chunk:chunk + 1, :sb]
            hi = ni + ends[b, chunk:chunk + 1, sb:]
            starts_r.append(hr)
            starts_i.append(hi)
        scan(b, (jnp.concatenate(starts_r, axis=0), jnp.concatenate(starts_i, axis=0)), True)
        mixed = jnp.dot(work[...].astype(BF16), read_out[b], preferred_element_type=F32)
        mixed = mixed + k_ref[b] * x_ref[b].astype(F32)
        mixed = jax.nn.gelu(mixed).astype(BF16)
        square = (rows, rows)
        source = lax.rem(iota(square, 0), span) * CHUNKS + lax.div(iota(square, 0), span)
        turn = (iota(square, 1) == source).astype(BF16)
        act[:, pl.ds(pl.multiple_of(b * cb, cb), cb)] = jnp.dot(
            turn, mixed, preferred_element_type=F32
        ).astype(BF16)

    keep_rows = rows // tp
    tile = min(512, width)
    mixed_copies = []
    for t in (*range(1, tp), 0):
        to = lax.rem(core + t, tp)

        @pl.loop(0, width // tile)
        def _(j):
            at = pl.ds(pl.multiple_of(j * tile, tile), tile)
            share[t, :, at] = jnp.dot(
                act[pl.ds(pl.multiple_of(to * keep_rows, keep_rows), keep_rows), :],
                wo_ref[:, at], preferred_element_type=F32,
            ).astype(BF16)

        if t:
            mixed_copies.append(send(share.at[t], others.at[t - 1], (h, u, m, v, to)))

    for w in range(3):
        for k in (1, 2, 3):
            first[w, k].wait_recv()
            pu, pv = peer(k)
            position = index(h, pu, m, pv)
            spread_h(w, k, place(weights[w], position), position)
            spread_m(w, k, 0, place(weights[w], position), position)

    for copy in mixed_copies:
        copy.wait_recv()
    line = min(32, keep_rows)

    @pl.loop(0, keep_rows // line)
    def _(i):
        at = pl.ds(pl.multiple_of(i * line, line), line)
        mixed = share[0, at, :].astype(F32)
        for t in range(1, tp):
            mixed = mixed + others[t - 1, at, :].astype(F32)
        carried = res_ref[at, :].astype(F32) + mixed.astype(BF16).astype(F32)
        scale = lax.rsqrt(jnp.mean(carried * carried, axis=-1, keepdims=True) + 1e-06)
        carried_ref[at, :] = carried
        rows_ref[0, 0, at, :] = (carried * scale * gain_ref[...]).astype(BF16)

    row_copies = {}
    for k in (3, 1, 2):
        pu, pv = peer(k)
        row_copies[k] = send(rows_ref.at[0, 0], rows_ref.at[0, k], (h, pu, m, pv, core))
    last = []
    for t in range(1, tp):
        last.append(send(rows_ref.at[0, 0], rows_ref.at[t, 0], (h, u, m, v, lax.rem(core + t, tp))))

    def pass_m(w, k):
        pu, pv = peer(k)
        for r in range(1, nh):
            over_h[w, k, r].wait_recv()
            position = index(lax.rem(h - r + nh, nh), pu, m, pv)
            spread_m(w, k, r, place(weights[w], position), position)

    for w in range(3):
        for k in range(4):
            pass_m(w, k)
        if w == 1:
            for k in (1, 2, 3):
                row_copies[k].wait_recv()
                for t in range(1, tp):
                    last.append(send(
                        rows_ref.at[0, k], rows_ref.at[t, k], (h, u, m, v, lax.rem(core + t, tp))
                    ))
    sent = [*first.values(), *over_h.values(), *over_m.values(), *states_out, *mixed_copies]
    row_sends = [*row_copies.values(), *last]
    for (w, *_), copy in over_m.items():
        if w < 2 or not fused:
            copy.wait_recv()
    for copy in last:
        copy.wait_recv()
    for copy in locals_:
        copy.wait()
    if fused:
        sent += back(
            sizes, send, peer, (h, u, m, v, core), weights, rows_ref, carried_ref, out_ref,
            hidden, partners, peers, row_sends, [c for (w, *_), c in over_m.items() if w == 2],
        )
    else:
        sent += row_sends
    for copy in sent:
        copy.wait_send()


def back(sizes, send, peer, here, weights, rows_ref, carried_ref, out_ref, hidden, partners,
         peers, row_sends, down_copies):
    tp = sizes["tp"]
    h, u, m, v, core = here
    _, _, keep_rows, width = rows_ref.shape
    across = (((1,), (1,)), ((), ()))

    @pl.loop(0, 4 * tp)
    def _(i):
        t, k = lax.div(i, 4), lax.rem(i, 4)
        block = rows_ref[t, k]
        gate = lax.dot_general(block, weights[0][...], across, preferred_element_type=F32)
        up = lax.dot_general(block, weights[1][...], across, preferred_element_type=F32)
        hidden[i] = (jax.nn.silu(gate) * up).astype(BF16)

    for copy in (*down_copies,):
        copy.wait_recv()
    for copy in row_sends:
        copy.wait_send()

    tile = min(512, width)
    line = min(32, keep_rows)
    sent = []
    peer_copies = []
    from_core = {}

    def reduce(k):
        for copy in from_core[k]:
            copy.wait_recv()

        @pl.loop(0, keep_rows // line)
        def _(i):
            at = pl.ds(pl.multiple_of(i * line, line), line)
            total = rows_ref[0, k, at, :].astype(F32)
            for t in range(1, tp):
                total = total + partners[k, t - 1, at, :].astype(F32)
            rows_ref[0, k, at, :] = total.astype(BF16)

        if k:
            pu, pv = peer(k)
            peer_copies.append(send(rows_ref.at[0, k], peers.at[k - 1], (h, pu, m, pv, core)))

    order = (3, 1, 2, 0)
    for step, k in enumerate(order):
        from_core[k] = []
        for t in (*range(1, tp), 0):
            @pl.loop(0, width // tile)
            def _(j):
                at = pl.ds(pl.multiple_of(j * tile, tile), tile)
                rows_ref[t, k, :, at] = jnp.dot(
                    hidden[t * 4 + k], weights[2][:, at], preferred_element_type=F32
                ).astype(BF16)

            if t:
                from_core[k].append(send(
                    rows_ref.at[t, k], partners.at[k, t - 1],
                    (h, u, m, v, lax.rem(core + tp - t, tp)),
                ))
        reduce(k)
        sent += from_core[k]
    for copy in peer_copies:
        copy.wait_recv()

    @pl.loop(0, keep_rows // line)
    def _(i):
        at = pl.ds(pl.multiple_of(i * line, line), line)
        total = rows_ref[0, 0, at, :].astype(F32)
        for k in range(1, 4):
            total = total + peers[k - 1, at, :].astype(F32)
        total = total.astype(BF16).astype(F32)
        out_ref[at, :] = (carried_ref[at, :] + 0.5 * total).astype(BF16)

    return sent + peer_copies


def streamed(sizes, x_hbm, residual_hbm, decay_re, decay_im, log_step, in_re, in_im, out_re, out_im,
             skip_hbm, wo_hbm, gain_hbm, gate_hbm, up_hbm, down_hbm, out_hbm, *rest):
    (out_ref, out_sem, joined, down_full, extra, rows_ref, carried_ref, gates, hidden, partners, firsts, seconds, work, read_in,
     read_out, ends, total, gathered, prefix, plane_total, planes, turn, act, share, others,
     x_raw, x_ref, res_ref, dr_ref, di_ref, ls_ref, inr_ref, ini_ref, outr_ref, outi_ref, k_ref,
     wo_ref, gain_ref, raw, turned, down_ref, a_ref, ratio, send_sem, recv_sem, local_sem, load_sem) = rest
    blocks, rows, cb = x_ref.shape
    sb = a_ref.shape[2]
    slab, depth = down_full.shape[0], raw.shape[1]
    pitch = joined.shape[0] // 2
    width = wo_ref.shape[1]
    keep_rows = rows // 2
    span = rows // CHUNKS
    nh, nm = sizes["h"], sizes["m"]
    n = nh * 4 * nm
    h, u, m, v, core = (lax.axis_index(name) for name in (*SP, "tp"))
    oh, ou, om, ov = 1 - h, 1 - u, 1 - m, 1 - v
    index = lambda h, u, m, v: ((h * 2 + u) * nm + m) * 2 + v
    me = index(h, u, m, v)
    to_x, to_z, to_y = (h, u, m, ov, core), (h, ou, m, v, core), (h, u, om, v, core)
    to_c, to_b, to_t = (oh, u, m, v, core), (oh, ou, m, v, core), (h, u, m, v, 1 - core)
    plane = [(h, b, c) for b in (u, ou) for c in (v, ov)]
    plane += [(oh, b, c) for b in (h, oh) for c in (v, ov)]
    is_inner = lax.rem(h + u, 2)
    inner = is_inner == 1
    across = (((1,), (1,)), ((), ()))
    slots, everywhere, moves = {}, [], []
    groups_of, fixed = {}, {}
    counter = iter(range(send_sem.shape[0]))

    def slot(name):
        return slots.setdefault(name, len(slots))

    def describe(src, dst, device, name, number):
        return pltpu.make_async_remote_copy(
            src_ref=src, dst_ref=dst, send_sem=send_sem.at[number],
            recv_sem=recv_sem.at[slot(name) if isinstance(name, tuple) else name], device_id=device, device_id_type=MESH,
        )

    def group_number(group):
        if group not in fixed:
            fixed[group] = next(counter)
        groups_of[group] = groups_of.get(group, 0) + 1
        return fixed[group]

    def send(src, dst, device, name, kept=everywhere, group=None):
        number = next(counter) if group is None else group_number(group)
        copy = describe(src, dst, device, name, number)
        copy.start()
        if group is None:
            kept.append(copy)

    def arrive(dst, device, name):
        describe(dst, dst, device, name, 0).wait_recv()

    def place(w, position):
        at = pl.ds(pl.multiple_of(position * depth, depth), depth)
        return down_full.at[:, at] if w == 2 else joined.at[pl.ds(w * pitch, slab), at]

    def spot(w, j, row=m):
        a, b, c = plane[j]
        return place(w, index(a, b, row, c))

    def mine(w, b, c):
        at = pl.ds(pl.multiple_of((b * 2 + c) * slab, slab), slab)
        return down_ref.at[at, :] if w == 2 else turned.at[w, at, :]

    def own(w):
        return mine(w, u, v)

    def send_x(w, s):
        if s:
            send(mine(w, ou, ov), extra.at[w], to_x, ("xo", w), group=("w", w))
        else:
            send(mine(w, u, ov), spot(w, 0), to_x, ("xu", w), group=("w", w))

    def send_z(w, s):
        send(extra.at[w] if s else mine(w, ou, v), spot(w, s), to_z, ("z", w, s), group=("w", w))

    numbers = {}

    def send_c(w, s, kind):
        if (w, s) not in numbers:
            numbers[w, s] = group_number(("w", w))
        number = numbers[w, s]
        name = ("e" if kind else "l", w, s)

        @pl.when(is_inner == kind)
        def _():
            describe(spot(w, 1) if s else own(w), spot(w, s), to_c, name, number).start()

    def send_b(w, s):
        send(extra.at[w] if s else mine(w, ou, v), spot(w, s), to_b, ("e", w, s), group="inside")

    def relay(w, s):
        send(spot(w, 2 + s), spot(w, 2 + s), to_c, ("l", w, s), group="inside")

    def send_y(w, j):
        send(own(w) if j == 0 else spot(w, j), spot(w, j), to_y, yname(w, j), group=("w", w))

    def wait_x(w, s):
        if s:
            arrive(extra.at[w], to_x, ("xo", w))
        else:
            arrive(spot(w, 1), to_x, ("xu", w))

    def wait_z(w, s):
        arrive(spot(w, 2 + s), to_z, ("z", w, s))

    def wait_e(w, s):
        arrive(spot(w, 4 + s), to_c, ("e", w, s))

    def wait_l(w, s):
        arrive(spot(w, 6 + s), to_c, ("l", w, s))

    def yname(w, j):
        return ("y", w, j // 4 if w == 2 else 0)

    def wait_y(w, part):
        count = 4 if w == 2 else 8
        at = pl.ds(0, count * depth)
        ref = down_full.at[:, at] if w == 2 else joined.at[pl.ds(w * pitch, slab), at]
        arrive(ref, to_y, ("y", w, part))

    barrier = pltpu.get_barrier_semaphore()
    others_sp = []
    for k in range(1, n):
        to = lax.rem(me + k, n)
        there = (lax.div(to, 4 * nm), lax.rem(lax.div(to, 2 * nm), 2),
                 lax.rem(lax.div(to, 2), nm), lax.rem(to, 2), core)
        others_sp.append(there)
        pl.semaphore_signal(barrier, inc=1, device_id=there, device_id_type=MESH)
    pl.semaphore_signal(barrier, inc=1, device_id=to_t, device_id_type=MESH)
    pairs = ((gate_hbm, raw.at[0]), (up_hbm, raw.at[1]), (decay_re, dr_ref), (decay_im, di_ref),
             (log_step, ls_ref), (x_hbm, x_raw), (in_re, inr_ref), (in_im, ini_ref),
             (out_re, outr_ref), (out_im, outi_ref), (down_hbm, down_ref), (skip_hbm, k_ref),
             (wo_hbm, wo_ref), (residual_hbm, res_ref), (gain_hbm, gain_ref))
    loads = [pltpu.make_async_copy(a, b, load_sem.at[i]) for i, (a, b) in enumerate(pairs)]
    for copy in loads:
        copy.start()
    exact = lax.Precision.HIGHEST

    def flip_weights(w):
        for i in range(raw.shape[2] // depth):
            turned[w, i * depth:(i + 1) * depth, :] = raw[w, :, i * depth:(i + 1) * depth].T

    with jax.named_scope("A_flip"):
        loads[0].wait()
        flip_weights(0)
    with jax.named_scope("A_barrier"):
        pl.semaphore_wait(barrier, n)
    loads[10].wait()
    if pitch > slab:
        for w in range(2):
            joined[w * pitch + slab:(w + 1) * pitch, :] = jnp.zeros(
                (pitch - slab, joined.shape[1]), BF16)

    def send_inner(w, s):
        @pl.when(inner)
        def _():
            send_b(w, s)

    send_x(0, 1)
    send_z(0, 0)
    send_y(0, 0)
    send_inner(0, 0)
    send_c(0, 0, 1)
    with jax.named_scope("A_param"):
        for copy in loads[2:5]:
            copy.wait()
        states = sb // GATHER
        spread = (lax.rem(iota((states, sb), 1), states) == iota((states, sb), 0)).astype(F32)
        chosen = lax.div(iota((GATHER, sb), 1), states) == iota((GATHER, sb), 0)
        for b in range(blocks):
            def lanes(ref):
                wide = jnp.dot(ref[b * GATHER:(b + 1) * GATHER, :], spread, precision=exact,
                               preferred_element_type=F32)
                return jnp.sum(jnp.where(chosen, wide, 0.0), axis=0, keepdims=True)

            groups = ls_ref.shape[1]
            group = (lax.div(iota((groups, sb), 1), states) + b * GATHER
                     == iota((groups, sb), 0)).astype(F32)
            step_size = jnp.exp(jnp.dot(ls_ref[...], group, precision=exact,
                                        preferred_element_type=F32))
            re, im = lanes(dr_ref), lanes(di_ref)
            magnitude = jnp.exp(re * step_size)
            angle = im * step_size
            power_re = magnitude * jnp.cos(angle)
            power_im = magnitude * jnp.sin(angle)
            denom = re * re + im * im
            a_ref[b, 0:1, :] = power_re
            a_ref[b, 1:2, :] = power_im
            ratio[b, 0:1, :] = ((power_re - 1.0) * re + power_im * im) / denom
            ratio[b, 1:2, :] = (power_im * re - (power_re - 1.0) * im) / denom
    with jax.named_scope("A_x"):
        square = (rows, rows)
        source = lax.rem(iota(square, 0), span) * CHUNKS + lax.div(iota(square, 0), span)
        turn[...] = (iota(square, 1) == source).astype(BF16)
        loads[5].wait()
        for b in range(blocks):
            x_ref[b] = lax.dot_general(
                turn[...], x_raw[:, b * cb:(b + 1) * cb], (((0,), (0,)), ((), ())),
                preferred_element_type=F32,
            ).astype(BF16)
    with jax.named_scope("A_flip1"):
        loads[1].wait()
        flip_weights(1)
        for copy in loads[6:10]:
            copy.wait()

    local = []
    for w in range(3):
        copy = pltpu.make_async_copy(own(w), spot(w, 0), local_sem.at[w])
        copy.start()
        local.append(copy)

    def scan(b, start, keep):
        work[...] = jnp.dot(x_ref[b], read_in[b], preferred_element_type=F32)
        br = jnp.broadcast_to(a_ref[b, 0:1, :], (CHUNKS, sb))
        bi = jnp.broadcast_to(a_ref[b, 1:2, :], (CHUNKS, sb))

        def step(i, state):
            at = pl.ds(pl.multiple_of(i * CHUNKS, CHUNKS), CHUNKS)
            nr, ni = cmul(br, bi, *state)
            nr, ni = nr + work[at, :sb], ni + work[at, sb:]
            if keep:
                work[at, :sb] = nr
                work[at, sb:] = ni
            return nr, ni

        return lax.fori_loop(0, span, step, start, unroll=8)

    size = cb // GATHER
    spread_narrow = spread.astype(BF16)
    with jax.named_scope("B_scan1"):
        @pl.loop(0, blocks)
        def _(b):
            keep = lax.div(iota((cb, sb), 0), size) == lax.div(iota((cb, sb), 1), states)
            at = pl.ds(pl.multiple_of(b * cb, cb), cb)
            def widen(ref):
                high = ref[at, :].astype(BF16)
                low = (ref[at, :] - high.astype(F32)).astype(BF16)
                return (jnp.dot(high, spread_narrow, preferred_element_type=F32)
                        + jnp.dot(low, spread_narrow, preferred_element_type=F32))

            vr, vi = widen(inr_ref), widen(ini_ref)
            cr, ci = ratio[b, 0:1, :], ratio[b, 1:2, :]
            read_in[b, :, :sb] = jnp.where(keep, cr * vr - ci * vi, 0.0).astype(BF16)
            read_in[b, :, sb:] = jnp.where(keep, cr * vi + ci * vr, 0.0).astype(BF16)
            zero = jnp.zeros((CHUNKS, sb), F32)
            sr, si = scan(b, (zero, zero), False)
            ends[b, :, :sb] = sr
            ends[b, :, sb:] = si
            lr, li = cpow(a_ref[b, 0:1, :], a_ref[b, 1:2, :], span)
            er, ei = sr[0:1], si[0:1]
            for chunk in range(1, CHUNKS):
                er, ei = cmul(lr, li, er, ei)
                er, ei = er + sr[chunk:chunk + 1], ei + si[chunk:chunk + 1]
            total[b, :, :sb] = er
            total[b, :, sb:] = ei

    def pass_z(w, s):
        with jax.named_scope(f"z{w}{s}"):
            wait_z(w, s)

        @pl.when(inner)
        def _():
            relay(w, s)

        send_y(w, 2 + s)

    def pass_e(w, s):
        with jax.named_scope(f"e{w}{s}"):
            wait_e(w, s)
        send_y(w, 4 + s)

    def pass_l(w, s):
        with jax.named_scope(f"l{w}{s}"):
            wait_l(w, s)
        send_y(w, 6 + s)

    here = m * 2 + v
    level = h * 2 + u
    for k, there in enumerate((to_x, to_y, (h, u, om, ov, core))):
        send(total, gathered.at[here], there, ("s", k))
    gathered[here] = total[...]
    send_x(0, 0)
    for w in (1, 2):
        for s in (1, 0):
            send_x(w, s)
    send_y(1, 0)
    send_y(2, 0)
    with jax.named_scope("C_readout"):
        @pl.loop(0, blocks)
        def _(b):
            high = (lax.rem(iota((sb, states), 0), states) == iota((sb, states), 1)).astype(BF16)
            keep = lax.div(iota((sb, cb), 0), states) == lax.div(iota((sb, cb), 1), size)
            at = pl.ds(pl.multiple_of(b * cb, cb), cb)
            for place_in, ref, sign in ((0, outr_ref, 1.0), (1, outi_ref, -1.0)):
                wide = lax.dot_general(high, (sign * ref[at, :]).astype(BF16), across,
                                       preferred_element_type=F32)
                read_out[b, place_in * sb:(place_in + 1) * sb, :] = jnp.where(
                    keep, wide, 0.0).astype(BF16)

    with jax.named_scope("C_states1"):
        for k, (a, b) in enumerate(((m, ov), (om, v), (om, ov))):
            arrive(gathered.at[a * 2 + b], to_x, ("s", k))

    def power_of(b, count):
        return cpow(a_ref[b, 0:1, :], a_ref[b, 1:2, :], count)

    @pl.loop(0, blocks)
    def _(b):
        tr, ti = power_of(b, span * CHUNKS)
        hr = jnp.zeros((1, sb), F32)
        hi, pr, pi = hr, hr, hr
        for device in range(4):
            gr, gi = gathered[device, b, :, :sb], gathered[device, b, :, sb:]
            nr, ni = cmul(tr, ti, hr, hi)
            hr = jnp.where(device < here, nr + gr, hr)
            hi = jnp.where(device < here, ni + gi, hi)
            nr, ni = cmul(tr, ti, pr, pi)
            pr, pi = nr + gr, ni + gi
        prefix[b, :, :sb] = hr
        prefix[b, :, sb:] = hi
        plane_total[b, :, :sb] = pr
        plane_total[b, :, sb:] = pi

    for k, (a, b) in enumerate(((h, ou), (oh, u), (oh, ou))):
        send(plane_total, planes.at[level], (a, b, m, v, core), ("plane", k))
    planes[level] = plane_total[...]
    with jax.named_scope("C_x01"):
        wait_x(0, 1)
    send_z(0, 1)
    send_inner(0, 1)
    send_c(0, 0, 0)
    for copy in loads[11:]:
        copy.wait()
    pass_z(0, 0)
    with jax.named_scope("C_states2"):
        for k, (a, b) in enumerate(((h, ou), (oh, u), (oh, ou))):
            arrive(planes.at[a * 2 + b], to_x, ("plane", k))
    with jax.named_scope("C_x00"):
        wait_x(0, 0)
    send_c(0, 1, 0)
    send_c(0, 1, 1)
    send_y(0, 1)
    send_z(1, 0)
    send_inner(1, 0)

    def second(b):
        lr, li = power_of(b, span)
        tr, ti = cpow(lr, li, CHUNKS)
        qr, qi = cpow(tr, ti, 4)
        hr = jnp.zeros((1, sb), F32)
        hi = hr
        for other in range(3):
            nr, ni = cmul(qr, qi, hr, hi)
            hr = jnp.where(other < level, nr + planes[other, b, :, :sb], hr)
            hi = jnp.where(other < level, ni + planes[other, b, :, sb:], hi)
        for device in range(3):
            nr, ni = cmul(tr, ti, hr, hi)
            hr, hi = jnp.where(device < here, nr, hr), jnp.where(device < here, ni, hi)
        hr, hi = hr + prefix[b, :, :sb], hi + prefix[b, :, sb:]
        starts_r, starts_i = [hr], [hi]
        for chunk in range(CHUNKS - 1):
            nr, ni = cmul(lr, li, hr, hi)
            hr = nr + ends[b, chunk:chunk + 1, :sb]
            hi = ni + ends[b, chunk:chunk + 1, sb:]
            starts_r.append(hr)
            starts_i.append(hi)
        scan(b, (jnp.concatenate(starts_r, axis=0), jnp.concatenate(starts_i, axis=0)), True)
        mixed = jnp.dot(work[...].astype(BF16), read_out[b], preferred_element_type=F32)
        at = pl.ds(pl.multiple_of(b * cb, cb), cb)
        mixed = mixed + k_ref[:, at] * x_ref[b].astype(F32)
        mixed = jax.nn.gelu(mixed).astype(BF16)
        act[:, at] = jnp.dot(
            turn[...], mixed, preferred_element_type=F32
        ).astype(BF16)

    with jax.named_scope("D_scan2a"):
        @pl.loop(0, blocks // 2)
        def _(b):
            second(b)

    pass_z(0, 1)
    with jax.named_scope("D_x11"):
        wait_x(1, 1)
    send_z(1, 1)
    send_inner(1, 1)
    with jax.named_scope("D_scan2b"):
        @pl.loop(blocks // 2, blocks)
        def _(b):
            second(b)

    with jax.named_scope("D_x10"):
        wait_x(1, 0)
    send_y(1, 1)
    send_c(1, 0, 1)
    send_c(1, 1, 1)

    tile = min(512, width)
    with jax.named_scope("E_outproj"):
        for t in (1, 0):
            to = core if t == 0 else 1 - core

            @pl.loop(0, width // tile)
            def _(j):
                at = pl.ds(pl.multiple_of(j * tile, tile), tile)
                share[t, :, at] = jnp.dot(
                    act[pl.ds(pl.multiple_of(to * keep_rows, keep_rows), keep_rows), :],
                    wo_ref[:, at], preferred_element_type=F32,
                ).astype(BF16)

            if t:
                send(share.at[1], others, to_t, ("mix",))

    with jax.named_scope("G_mix"):
        arrive(others, to_t, ("mix",))
    line = min(32, keep_rows)
    with jax.named_scope("H_norm"):
        @pl.loop(0, keep_rows // line)
        def _(i):
            at = pl.ds(pl.multiple_of(i * line, line), line)
            mixed = share[0, at, :].astype(F32) + others[at, :].astype(F32)
            carried = res_ref[at, :].astype(F32) + mixed.astype(BF16).astype(F32)
            scale = lax.rsqrt(jnp.mean(carried * carried, axis=-1, keepdims=True) + 1e-06)
            carried_ref[at, :] = carried
            rows_ref[0, 0, at, :] = (carried * scale * gain_ref[...]).astype(BF16)

    send(rows_ref.at[0, 0], rows_ref.at[0, 1], to_x, ("r", 1), moves)
    piece = keep_rows // PIECES
    for part in range(PIECES):
        at = pl.ds(part * piece, piece)
        send(rows_ref.at[0, 0, at], rows_ref.at[0, 2, at], to_z, ("r", 2, part), moves)
    send(rows_ref.at[0, 0], rows_ref.at[1, 0], to_t, ("t", 0), moves)

    def share_core(k):
        send(rows_ref.at[0, k], rows_ref.at[1, k], to_t, ("t", k), moves)

    def wait_core(k):
        arrive(rows_ref.at[1, k], to_t, ("t", k))

    def product(k, at):
        block = rows_ref[:, k].reshape(2 * keep_rows, width)
        return lax.dot_general(block, joined[at, :], across, preferred_element_type=F32)

    def keep_hidden(k, gate, up):
        result = (jax.nn.silu(gate) * up).astype(BF16)
        for t in range(2):
            hidden[pl.ds((4 * t + k) * keep_rows, keep_rows), :] = (
                result[t * keep_rows:(t + 1) * keep_rows])

    def gate_part(k):
        with jax.named_scope(f"gate{k}"):
            gates[k] = product(k, pl.ds(0, slab))

    def up_part(k):
        with jax.named_scope(f"up{k}"):
            keep_hidden(k, gates[k], product(k, pl.ds(pitch, slab)))

    def both_parts(k):
        with jax.named_scope(f"both{k}"):
            result = product(k, pl.ds(0, 2 * pitch))
            keep_hidden(k, result[:, :slab], result[:, pitch:pitch + slab])

    def first_rows():
        with jax.named_scope("r1"):
            arrive(rows_ref.at[0, 1], to_x, ("r", 1))
        share_core(1)

    def relay_rows(part):
        at = pl.ds(part * piece, piece)
        with jax.named_scope(f"r2{part}"):
            arrive(rows_ref.at[0, 2, at], to_z, ("r", 2, part))
        send(rows_ref.at[0, 2, at], rows_ref.at[0, 3, at], to_x, ("r", 3, part), moves)
        if part == PIECES - 1:
            share_core(2)

    def last_rows():
        with jax.named_scope("r3"):
            for part in range(PIECES):
                at = pl.ds(part * piece, piece)
                arrive(rows_ref.at[0, 3, at], to_x, ("r", 3, part))
        share_core(3)

    def second_weights():
        send_inner(2, 0)
        wait_x(2, 1)
        send_inner(2, 1)
        send_z(2, 0)
        send_z(2, 1)
        wait_x(2, 0)
        send_y(2, 1)
        send_c(2, 0, 0)
        send_c(2, 1, 0)

    def delayed_weights():
        send_c(2, 0, 1)
        send_c(2, 1, 1)

    def whole(w):
        with jax.named_scope(f"y{w}"):
            wait_y(w, 0)

    def core_rows(k):
        with jax.named_scope(f"t{k}"):
            wait_core(k)

    for s in range(2):
        send_c(1, s, 0)
    pass_e(0, 0)
    pass_e(0, 1)
    pass_z(1, 0)
    pass_z(1, 1)
    pass_l(0, 0)
    pass_l(0, 1)
    pass_e(1, 0)
    for copy in local:
        copy.wait()
    whole(0)
    core_rows(0)
    gate_part(0)
    first_rows()
    second_weights()
    relay_rows(0)
    pass_e(1, 1)
    relay_rows(1)
    core_rows(1)
    gate_part(1)
    pass_l(1, 0)
    pass_l(1, 1)
    delayed_weights()
    relay_rows(2)
    whole(1)
    up_part(0)
    relay_rows(3)
    up_part(1)
    core_rows(2)
    pass_z(2, 0)
    both_parts(2)
    last_rows()
    pass_z(2, 1)
    core_rows(3)
    both_parts(3)
    pass_e(2, 0)
    with jax.named_scope("moves"):
        for copy in moves:
            copy.wait_send()

    across_u = width // 8
    chunks = [(h, h, m), (h, oh, m), (h, h, om), (h, oh, om), (oh, h, m), (oh, oh, m),
              (oh, h, om), (oh, oh, om)]

    def columns(j):
        a, b, c = chunks[j]
        return pl.ds(pl.multiple_of(index(a, b, c, 0) * depth, across_u), across_u)

    def down(j):
        pair_of = (2 * j, 2 * j + 1)
        right = jnp.concatenate([down_full[:, columns(i)] for i in pair_of], axis=1)
        for t in (1, 0):
            result = jnp.dot(
                hidden[4 * t * keep_rows:4 * (t + 1) * keep_rows, :], right,
                preferred_element_type=F32,
            ).astype(BF16)
            for side, i in enumerate(pair_of):
                for k in range(4):
                    rows_ref[t, k, :, columns(i)] = result[
                        k * keep_rows:(k + 1) * keep_rows, side * across_u:(side + 1) * across_u]
                if t:
                    send(rows_ref.at[1, :, :, columns(i)], partners.at[i], to_t, ("p", i), group="p")

    def add(target, j, other):
        at = columns(j)

        @pl.loop(0, keep_rows // line)
        def _(i):
            lines = pl.ds(pl.multiple_of(i * line, line), line)
            rows_ref[0, target, lines, at] = (
                rows_ref[0, target, lines, at].astype(F32) + other[lines, :].astype(F32)
            ).astype(BF16)

    def pair(j):
        at = columns(j)
        near, far = (1, 2) if X_FIRST[j] else (2, 1)
        device = to_x if X_FIRST[j] else to_z
        arrive(partners.at[j], to_t, ("p", j))
        for place_in, k in enumerate((3, near)):
            add(k, j, partners.at[j, k])
            send(rows_ref.at[0, k, :, at], firsts.at[j, place_in], device, ("f", j, place_in), group="f")
        add(far, j, partners.at[j, far])
        add(0, j, partners.at[j, 0])

    def combine(j):
        at = columns(j)
        far = 2 if X_FIRST[j] else 1
        device, other = (to_x, to_z) if X_FIRST[j] else (to_z, to_x)
        arrive(firsts.at[j, 0], device, ("f", j, 0))
        add(far, j, firsts.at[j, 0])
        send(rows_ref.at[0, far, :, at], seconds.at[j], other, ("g", j), group="g")
        arrive(firsts.at[j, 1], device, ("f", j, 1))
        add(0, j, firsts.at[j, 1])

    stored = []

    def finish(j):
        at = columns(j)
        arrive(seconds.at[j], to_z if X_FIRST[j] else to_x, ("g", j))

        @pl.loop(0, keep_rows // line)
        def _(i):
            lines = pl.ds(pl.multiple_of(i * line, line), line)
            summed = rows_ref[0, 0, lines, at].astype(F32) + seconds[j, lines, :].astype(F32)
            summed = summed.astype(BF16).astype(F32)
            out_ref[lines, at] = (carried_ref[lines, at] + 0.5 * summed).astype(BF16)

        copy = pltpu.make_async_copy(out_ref.at[:, at], out_hbm.at[:, at], out_sem.at[j])
        copy.start()
        stored.append(copy)

    order = ORDER
    stages = {"d": down, "p": pair, "c": combine, "f": finish}
    for word in order:
        if word == "e":
            pass_e(2, 1)
            continue
        if word == "l":
            pass_l(2, 0)
            pass_l(2, 1)
            continue
        j = int(word[1])
        if word in ("d1", "d3"):
            with jax.named_scope("y2" + word):
                wait_y(2, j // 2)
        with jax.named_scope({"d": "down", "p": "pair", "c": "comb", "f": "fin"}[word[0]] + word[1]):
            stages[word[0]](j)
    def drain(group, ref):
        describe(ref, ref, to_x, ("mix",), fixed[group]).wait_send()

    with jax.named_scope("end_sends"):
        for copy in everywhere:
            copy.wait_send()
        for w in range(3):
            drain(("w", w), down_full.at[:, pl.ds(0, groups_of["w", w] * depth)])
        drain("p", partners)
        drain("f", firsts)
        drain("g", seconds)

        @pl.when(inner)
        def _():
            drain("inside", down_full.at[:, pl.ds(0, groups_of["inside"] * depth)])

    with jax.named_scope("end_store"):
        for copy in stored:
            copy.wait()


def shift(value, axis, count, by):
    return lax.ppermute(value, axis, [(i, (i + by) % count) for i in range(count)])


def flip(value, axes, count, k):
    return lax.ppermute(value, axes, [(i, i ^ k) for i in range(count)])


def on_device(sizes, mixer_in, residual, decay_real, decay_imag, log_step, in_real, in_imag,
              output_real, output_imaginary, skip, out_proj, norm_gain, w_gate, w_up, w_down):
    tp, nh, nm = sizes["tp"], sizes["h"], sizes["m"]
    n = nh * 4 * nm
    rows, channels = mixer_in.shape
    keep_rows, width = residual.shape
    depth, hidden_units = w_gate.shape
    part = hidden_units // 4
    groups, states = decay_real.shape
    blocks = groups // GATHER
    cb, sb = channels // blocks, GATHER * states
    vmem = pl.BlockSpec(memory_space=pltpu.VMEM)
    if depth % 128 == 0 and (tp, nh, nm) == (2, 2, 2):
        cut = width // 8
        pitch = -(-part // 128) * 128
        return pl.pallas_call(
            functools.partial(streamed, sizes),
            in_specs=[pl.BlockSpec(memory_space=pl.ANY)] * 15,
            out_specs=pl.BlockSpec(memory_space=pl.ANY),
            out_shape=jax.ShapeDtypeStruct((keep_rows, width), BF16),
            scratch_shapes=[
                pltpu.VMEM((keep_rows, width), BF16),
                pltpu.SemaphoreType.DMA((8,)),
                pltpu.VMEM((2 * pitch, n * depth), BF16),
                pltpu.VMEM((part, n * depth), BF16),
                pltpu.VMEM((3, part, depth), BF16),
                pltpu.VMEM((2, 4, keep_rows, width), BF16),
                pltpu.VMEM((keep_rows, width), F32),
                pltpu.VMEM((4, 2 * keep_rows, part), F32),
                pltpu.VMEM((8 * keep_rows, part), BF16),
                pltpu.VMEM((8, 4, keep_rows, cut), BF16),
                pltpu.VMEM((8, 2, keep_rows, cut), BF16),
                pltpu.VMEM((8, keep_rows, cut), BF16),
                pltpu.VMEM((rows, 2 * sb), F32),
                pltpu.VMEM((blocks, cb, 2 * sb), BF16),
                pltpu.VMEM((blocks, 2 * sb, cb), BF16),
                pltpu.VMEM((blocks, CHUNKS, 2 * sb), F32),
                pltpu.VMEM((blocks, 1, 2 * sb), F32),
                pltpu.VMEM((4, blocks, 1, 2 * sb), F32),
                pltpu.VMEM((blocks, 1, 2 * sb), F32),
                pltpu.VMEM((blocks, 1, 2 * sb), F32),
                pltpu.VMEM((4, blocks, 1, 2 * sb), F32),
                pltpu.VMEM((rows, rows), BF16),
                pltpu.VMEM((rows, channels), BF16),
                pltpu.VMEM((2, keep_rows, width), BF16),
                pltpu.VMEM((keep_rows, width), BF16),
                pltpu.VMEM((rows, channels), BF16),
                pltpu.VMEM((blocks, rows, cb), BF16),
                pltpu.VMEM((keep_rows, width), BF16),
                *[pltpu.VMEM((groups, states), F32)] * 2,
                pltpu.VMEM((1, groups), F32),
                *[pltpu.VMEM((channels, states), F32)] * 4,
                pltpu.VMEM((1, channels), F32),
                pltpu.VMEM((channels, width), BF16),
                pltpu.VMEM((1, width), F32),
                pltpu.VMEM((2, depth, hidden_units), BF16),
                pltpu.VMEM((2, hidden_units, depth), BF16),
                pltpu.VMEM((hidden_units, depth), BF16),
                pltpu.VMEM((blocks, 2, sb), F32),
                pltpu.VMEM((blocks, 2, sb), F32),
                pltpu.SemaphoreType.DMA((27,)),
                pltpu.SemaphoreType.DMA((80,)),
                pltpu.SemaphoreType.DMA((3,)),
                pltpu.SemaphoreType.DMA((15,)),
            ],
            compiler_params=pltpu.CompilerParams(
                collective_id=0, has_side_effects=True, vmem_limit_bytes=62 * 2**20
            ),
            name="streamed",
        )(mixer_in, residual, decay_real, decay_imag, log_step.reshape(1, groups),
          in_real.transpose(0, 2, 1).reshape(channels, states),
          in_imag.transpose(0, 2, 1).reshape(channels, states),
          output_real.reshape(channels, states), output_imaginary.reshape(channels, states),
          skip.reshape(1, channels), out_proj, norm_gain.reshape(1, width), w_gate, w_up, w_down)
    power_re, power_im, bar_re, bar_im = discrete(
        decay_real, decay_imag, log_step, in_real, in_imag
    )
    rows_first = lambda t: jnp.transpose(t, (0, 2, 1)).reshape(blocks, -1, t.shape[1])
    read_in = jnp.stack([rows_first(bar_re), rows_first(bar_im)], axis=1).astype(BF16)
    read_out = jnp.stack(
        [rows_first(output_real), -rows_first(output_imaginary)], axis=1
    ).astype(BF16)
    power = jnp.stack([power_re.reshape(blocks, sb), power_im.reshape(blocks, sb)], axis=1)
    x = mixer_in.reshape(CHUNKS, rows // CHUNKS, blocks, cb).transpose(2, 1, 0, 3)
    x = x.reshape(blocks, rows, cb)
    operands = (x, read_in, read_out, power, skip.reshape(blocks, 1, cb), out_proj, residual,
                norm_gain.reshape(1, width), w_gate.T.reshape(4, part, depth),
                w_up.T.reshape(4, part, depth), w_down.reshape(4, part, depth))
    copies = 3 * (3 + 4 * (nh - 1) + 4 * nh * (nm - 1)) + (n - 1) + (tp - 1) + 3 + 4 * (tp - 1)
    laid = (part, n * depth) if depth % 128 == 0 else (n, part, depth)
    between = [(laid, BF16)] * 3 + [
        ((tp, 4, keep_rows, width), BF16), ((keep_rows, width), F32),
    ]
    fused = depth % 128 == 0
    if fused:
        copies += 4 * (tp - 1) + 3
        out_shape = [jax.ShapeDtypeStruct((keep_rows, width), BF16)]
        extra = [
            pltpu.VMEM((4 * tp, keep_rows, part), BF16),
            pltpu.VMEM((4, tp - 1, keep_rows, width), BF16),
            pltpu.VMEM((3, keep_rows, width), BF16),
            *(pltpu.VMEM(*item) for item in between),
        ]
    else:
        out_shape = [jax.ShapeDtypeStruct(*item) for item in between]
        extra = []
    results = pl.pallas_call(
        functools.partial(layer, sizes, fused),
        in_specs=[vmem] * 11,
        out_specs=[vmem] * len(out_shape),
        out_shape=out_shape,
        scratch_shapes=[
            *extra,
            pltpu.VMEM((rows, 2 * sb), F32),
            pltpu.VMEM((blocks, cb, 2 * sb), BF16),
            pltpu.VMEM((blocks, 2 * sb, cb), BF16),
            pltpu.VMEM((blocks, CHUNKS, 2 * sb), F32),
            pltpu.VMEM((blocks, 1, 2 * sb), F32),
            pltpu.VMEM((n, blocks, 1, 2 * sb), F32),
            pltpu.VMEM((rows, channels), BF16),
            pltpu.VMEM((tp, keep_rows, width), BF16),
            pltpu.VMEM((tp - 1, keep_rows, width), BF16),
            pltpu.SemaphoreType.DMA((copies,)),
            pltpu.SemaphoreType.DMA((copies,)),
            pltpu.SemaphoreType.DMA((3,)),
        ],
        compiler_params=pltpu.CompilerParams(
            collective_id=0, has_side_effects=True, vmem_limit_bytes=62 * 2**20
        ),
        name="layer",
    )(*operands)
    if fused:
        return results[0]
    full_gate, full_up, full_down, rows_all, carried = results
    if len(laid) == 3:
        full_gate, full_up, full_down = (
            t.transpose(1, 0, 2).reshape(part, width) for t in (full_gate, full_up, full_down)
        )

    flat = rows_all.reshape(-1, width)
    across = (((1,), (1,)), ((), ()))
    gate = lax.dot_general(flat, full_gate, across, preferred_element_type=F32)
    up = lax.dot_general(flat, full_up, across, preferred_element_type=F32)
    hidden = (jax.nn.silu(gate) * up).astype(BF16)
    down = jnp.dot(hidden, full_down, preferred_element_type=F32).astype(BF16)
    down = down.reshape(rows_all.shape)
    summed = down[0].astype(F32)
    for t in range(1, tp):
        summed = summed + shift(down[t], "tp", tp, -t).astype(F32)
    summed = summed.astype(BF16)
    total = summed[0].astype(F32)
    for k in range(1, 4):
        total = total + flip(summed[k], PEERS, 4, k).astype(F32)
    total = total.astype(BF16)
    return (carried + 0.5 * total.astype(F32)).astype(BF16)


def solution(mesh):
    sp, tp = mesh.shape["sp"], mesh.shape["tp"]
    sizes = {"h": sp // 8, "u": 2, "m": 2, "v": 2, "tp": tp}
    cut = Mesh(mesh.devices.reshape(tuple(sizes.values())), tuple(sizes))
    return jax.shard_map(
        functools.partial(on_device, sizes),
        mesh=cut,
        in_specs=(
            P(SP, "tp"),
            P((*SP, "tp"), None),
            P("tp", None),
            P("tp", None),
            P("tp"),
            P("tp", None, None),
            P("tp", None, None),
            P("tp", None, None),
            P("tp", None, None),
            P("tp"),
            P("tp", None),
            P(),
            P(SP, "tp"),
            P(SP, "tp"),
            P("tp", SP),
        ),
        out_specs=P((*SP, "tp"), None),
        check_vma=False,
    )
```
